128 devices in a mesh: sp: 16 (over z, x), tp: 8 (over y, core).
Axes of the slice: x: 4, y: 4, z: 4, core: 2. Of those that a mesh axis runs over, the one named last changes fastest.
Arguments:
- tokens: bfloat16 [2048, 1024], P('sp', 'tp'), may hold values from -6 to 6
- norm_gain: float32 [3, 1024], replicated, may hold values from 0.1 to 1.9
- w_query: bfloat16 [3, 1024, 1024], P(None, 'sp', 'tp'), may hold values from -0.1875 to 0.1875
- w_key: bfloat16 [3, 1024, 1024], P(None, 'sp', 'tp'), may hold values from -0.1875 to 0.1875
- w_value: bfloat16 [3, 1024, 1024], P(None, 'sp', 'tp'), may hold values from -0.1875 to 0.1875
- w_out: bfloat16 [3, 1024, 1024], P(None, 'tp', 'sp'), may hold values from -0.5625 to 0.5625
- offset_bias: float32 [3, 16, 8, 16], P(None, 'tp'), may hold values from -3 to 3
- documents: int32 [2048], P('sp'), may hold values from 0 to 15, never falling along the last dimension, each value on 1 to 256 neighbouring positions
Outputs:
- mixed: bfloat16 [2048, 1024], P('sp', 'tp')
The draws below stay inside these ranges and needn't reach their ends.
Inputs may be any that keep to these rules, and one draw needn't show every extreme that they name: `documents`: document numbers never fall along the token order, start at 0, and each document has 1 to 256 tokens.
All inputs are finite; a program needn't handle non-finite values.
Results may differ from the reference program's by a relative error of at most 0.02.
Values may be sent and summed in bfloat16 or wider, within the bound.
No kernel may reach another device: no remote copies, remote signals or barrier semaphores. Data moves between devices by JAX's collectives and lax.ppermute only.
A program may use at most 64 MiB of HBM per device.

```python
import math
import jax
import jax.numpy as jnp
import numpy as np
from jax import lax

HEADS = 16
HEAD_DIM = 64
D = 1024
WIN_ROWS = 8
WIN_COLS = 16
LAYERS = 3
ROWS_DEV = 4
GRID_W = 32
TOKENS = 2048


def level_of(own_key, dims, pieces, low, largest):
    factor_of = 1.0
    for dim, blocks in pieces:
        heights = jax.random.uniform(jax.random.fold_in(jax.random.fold_in(own_key, 6), dim), (blocks,), jnp.float32, low / len(pieces), largest / len(pieces))
        factor_of = factor_of * jnp.repeat(jnp.exp(heights), dims[dim] // blocks).reshape((-1,) + (1,) * (len(dims) - 1 - dim))
    return factor_of


def length_profile(number_of, total, most, slope):
    weights = [(1 << 20) // math.isqrt(grade ** slope) + 1 for grade in range(2, number_of + 1)]
    spare, given = total - most - (number_of - 1), [1] * (number_of - 1)
    while spare > 0:
        movable = [i for i in range(number_of - 1) if given[i] < most]
        whole, left = sum([weights[i] for i in movable]), spare
        for i in movable:
            more = min(most - given[i], max(1, left * weights[i] // whole), spare)
            given[i] = given[i] + more
            spare = spare - more
    return np.array([most] + given)


def uneven_parts(own_key, count, total, most, skew):
    if count == 2:
        one = jax.random.randint(own_key, (), max(1, total - most), min(most, total - 1) + 1)
        return jnp.stack([one, total - one])
    lengths = jnp.asarray(length_profile(count, total, most, skew), jnp.int32)
    pairs = (count - 1) // 2
    giver, sink = lengths[1:1 + 2 * pairs:2], lengths[2:2 + 2 * pairs:2]
    margin = jnp.minimum(giver - 1, most - sink)
    shifted = jax.random.randint(jax.random.fold_in(own_key, 1), (pairs,), 0, 1 << 20) % (margin + 1)
    lengths = lengths.at[1:1 + 2 * pairs:2].set(giver - shifted).at[2:2 + 2 * pairs:2].set(sink + shifted)
    return lengths[jax.random.permutation(jax.random.fold_in(own_key, 2), count)]


def centred(stream_key, shape, deviation, bound, split=(), held_as=jnp.bfloat16):
    result = deviation * jax.random.normal(stream_key, shape, jnp.float32)
    if split:
        result = result * level_of(stream_key, shape, split, -0.22, 0.18)
    return jnp.clip(result, -bound, bound).astype(held_as)


def setup_inputs(seed: int = 0) -> dict:
    keys = jax.random.split(jax.random.key(seed), 9)
    return {
        "tokens": centred(keys[0], (TOKENS, D), 1.0, 6.0, ((0, 16), (1, 8))),
        "norm_gain": jnp.clip(1.0 + 0.18 * jax.random.normal(keys[1], (LAYERS, D), jnp.float32), 0.1, 1.9),
        "w_query": centred(keys[2], (LAYERS, D, D), D ** -0.5, 0.1875, ((1, 16), (2, 8))),
        "w_key": centred(keys[3], (LAYERS, D, D), D ** -0.5, 0.1875, ((1, 16), (2, 8))),
        "w_value": centred(keys[4], (LAYERS, D, D), D ** -0.5, 0.1875, ((1, 16), (2, 8))),
        "w_out": centred(keys[5], (LAYERS, D, D), (3.0 / D ** 0.5), 0.5625, ((1, 8), (2, 16))),
        "offset_bias": centred(keys[6], (LAYERS, HEADS, WIN_ROWS, WIN_COLS), 0.5, 3.0, ((1, 8),), jnp.float32),
        "documents": jnp.searchsorted(jnp.cumsum(uneven_parts(keys[7], TOKENS // (ROWS_DEV * GRID_W), TOKENS, 2 * ROWS_DEV * GRID_W, 2)), jnp.arange(TOKENS), side="right").astype(jnp.int32),
    }


EPS = 1e-06

def rms_rows(stream, gain_row):
    values = stream.astype(jnp.float32)
    mean_sq = lax.optimization_barrier(jnp.mean(values * values, axis=-1, keepdims=True))
    return (values * lax.rsqrt(mean_sq + EPS) * gain_row).astype(jnp.bfloat16)

def head_norm(heads_raw):
    values = heads_raw.astype(jnp.float32)
    mean_sq = lax.optimization_barrier(jnp.mean(values * values, axis=-1, keepdims=True))
    return (values * lax.rsqrt(mean_sq + EPS)).astype(jnp.bfloat16)

def attend(queries, fringe, seg_own, seg_fringe, bias_layer):
    row_count, grid_width, head_count, head_width = queries.shape
    key_rows = jnp.stack([fringe[row_lag:row_lag + row_count] for row_lag in range(WIN_ROWS)], axis=1)
    seg_rows = jnp.stack([seg_fringe[row_lag:row_lag + row_count] for row_lag in range(WIN_ROWS)], axis=1)
    key_part = key_rows[..., :head_width].astype(jnp.float32)
    value_part = key_rows[..., head_width:].astype(jnp.float32)
    scores = jnp.einsum('rchd,rjkhd->rhcjk', queries.astype(jnp.float32), key_part) * head_width ** (-0.5)
    column = jnp.arange(grid_width)
    col_offset = column[None, :] - column[:, None] + WIN_COLS // 2
    inside = (col_offset >= 0) & (col_offset < WIN_COLS)
    bias_table = bias_layer[:, :, jnp.clip(col_offset, 0, WIN_COLS - 1)]
    scores = scores + jnp.transpose(bias_table, (0, 2, 1, 3))[None]
    same_doc = seg_rows[:, None, None, :, :] == seg_own[:, None, :, None, None]
    allowed = same_doc & inside[None, None, :, None, :]
    scores = jnp.where(allowed, scores, -1e+30)
    flat = scores.reshape(row_count, head_count, grid_width, WIN_ROWS * grid_width)
    attn_probs = jax.nn.softmax(flat, axis=-1).astype(jnp.bfloat16)
    attn_probs = attn_probs.reshape(row_count, head_count, grid_width, WIN_ROWS, grid_width)
    mixed_heads = jnp.einsum('rhcjk,rjkhd->rchd', attn_probs.astype(jnp.float32), value_part)
    return mixed_heads.astype(jnp.bfloat16)

def reference(tokens, norm_gain, w_query, w_key, w_value, w_out, offset_bias, documents):
    row_count = TOKENS // GRID_W
    reach_rows = WIN_ROWS // 2
    seg_own = (documents + 1).reshape(row_count, GRID_W)
    seg_fringe = jnp.pad(seg_own, ((reach_rows, reach_rows), (0, 0)))
    stream = tokens
    for layer_index in range(LAYERS):
        normed = rms_rows(stream, norm_gain[layer_index])
        query_raw = jnp.dot(normed, w_query[layer_index], preferred_element_type=jnp.float32).astype(jnp.bfloat16)
        key_raw = jnp.dot(normed, w_key[layer_index], preferred_element_type=jnp.float32).astype(jnp.bfloat16)
        value_heads = jnp.dot(normed, w_value[layer_index], preferred_element_type=jnp.float32).astype(jnp.bfloat16)
        query_heads = head_norm(query_raw.reshape(row_count, GRID_W, HEADS, HEAD_DIM))
        key_heads = head_norm(key_raw.reshape(row_count, GRID_W, HEADS, HEAD_DIM))
        value_heads = value_heads.reshape(row_count, GRID_W, HEADS, HEAD_DIM)
        key_value = jnp.concatenate([key_heads, value_heads], axis=-1)
        fringe = jnp.pad(key_value, ((reach_rows, reach_rows), (0, 0), (0, 0), (0, 0)))
        attended = attend(query_heads, fringe, seg_own, seg_fringe, offset_bias[layer_index])
        attended = attended.reshape(TOKENS, HEADS * HEAD_DIM)
        stream = jnp.dot(attended, w_out[layer_index], preferred_element_type=jnp.float32).astype(jnp.bfloat16)
    return stream
```

```python
import jax
import jax.numpy as jnp
from jax import lax
from jax.experimental import pallas as pl
from jax.experimental.pallas import tpu as pltpu
from jax.sharding import Mesh
from jax.sharding import PartitionSpec as P

HEAD_DIM = 64
WIN_ROWS = 8
WIN_COLS = 16
LAYERS = 3
GRID_W = 32
SP = ("z", "x")
TP = ("y", "c")
EPS = 1e-06
F32 = jnp.float32
BF16 = jnp.bfloat16
NT = (((1,), (1,)), ((), ()))


def turn(k):
    return [(i, (i + k) % 4) for i in range(4)]


def spread(a, axis):
    return [lax.ppermute(a, axis, turn(k)) for k in (1, 3, 2)]


def in_order(a, three):
    return [a, three[0], three[2], three[1]]


def swap(a):
    return lax.ppermute(a, "c", [(0, 1), (1, 0)])


def from_before(a):
    return lax.ppermute(a, SP, [(i, i + 1) for i in range(15)])


def from_after(a):
    return lax.ppermute(a, SP, [(i + 1, i) for i in range(15)])


def behind(axis, k):
    return (lax.axis_index(axis) + (4 - k)) & 3


def ahead(axis, k):
    return (lax.axis_index(axis) + k) & 3


def call(body, outs, *args, scratch=(), name=None):
    return pl.pallas_call(
        body,
        out_shape=outs,
        scratch_shapes=list(scratch),
        name=name,
        compiler_params=pltpu.CompilerParams(vmem_limit_bytes=24 * 1024 * 1024),
    )(*args)


def shaped(*shape, dtype=BF16):
    return jax.ShapeDtypeStruct(shape, dtype)


def pack_body(wq, wk, wv, wo, tokens, docs, first, rest, payload):
    for layer in range(LAYERS):
        into = first if layer == 0 else rest.at[layer - 1]
        into[:, 0:128] = wq[layer]
        into[:, 128:256] = wk[layer]
        into[:, 256:384] = wv[layer]
        into[:, 384:512] = wo[layer].astype(F32).T.astype(BF16)
    payload[0:128, :] = tokens[...]
    payload[128:144, :] = jnp.broadcast_to((docs[...] + 1).astype(F32).astype(BF16), (16, 128))


def table_body(rows, before, own, after, table):
    own_docs = own[128:144, :].astype(F32)[0:1]
    query_docs = jnp.broadcast_to(own_docs, (128, 128)).T
    key_docs = jnp.concatenate(
        [before[128:144, :].astype(F32)[0:1], own_docs, after[128:144, :].astype(F32)[0:1]], axis=1
    )
    same = jnp.concatenate([query_docs] * 3, axis=1) == key_docs
    r = lax.broadcasted_iota(jnp.int32, (128, 384), 0)
    m = lax.broadcasted_iota(jnp.int32, (128, 384), 1)
    lag = (m >> 5) - (r >> 5)
    off = (m & 31) - (r & 31) + WIN_COLS // 2
    allowed = same & (lag >= 0) & (lag < WIN_ROWS) & (off >= 0) & (off < WIN_COLS)
    for n in range(2 * LAYERS):
        line = jnp.broadcast_to(rows[n : n + 1, :], (GRID_W, 256))
        line = pltpu.roll(line, 256 - WIN_COLS // 2, 1, stride=1, stride_axis=0)
        line = jnp.concatenate([line, jnp.zeros((GRID_W, 128), F32)], axis=1)
        block = jnp.concatenate(
            [line] + [pltpu.roll(line, 32 * q, 1) for q in range(1, 4)], axis=0
        )
        table[n] = jnp.where(allowed, block, -1e30)


def normed_heads(raw):
    values = raw.astype(BF16).astype(F32)
    squares = values * values
    low = lax.broadcasted_iota(jnp.int32, values.shape, 1) < HEAD_DIM
    first = jnp.sum(jnp.where(low, squares, 0.0), axis=1, keepdims=True)
    second = jnp.sum(jnp.where(low, 0.0, squares), axis=1, keepdims=True)
    scale = jnp.where(
        low,
        lax.rsqrt(first * (1.0 / HEAD_DIM) + EPS),
        lax.rsqrt(second * (1.0 / HEAD_DIM) + EPS),
    )
    return (values * scale).astype(BF16)


def fill_weights(parts, weights, lo, hi):
    for kz in range(4):
        for kx in range(4):
            block = behind("z", kz) * 4 + behind("x", kx)
            weights[pl.ds(pl.multiple_of(block * 64, 64), 64), :] = parts[kz][kx, :, lo:hi]


def finish_heads(acc, q, kv):
    q[...] = normed_heads(acc[:, 0:128])
    kv[:, 0:128] = normed_heads(acc[:, 128:256])
    kv[:, 128:256] = acc[:, 256:384].astype(BF16)


def heads_first_body(own, partner, gain, w0, w1, w2, w3, q, kv, weights):
    fill_weights((w0, w1, w2, w3), weights, 0, 384)
    c = lax.axis_index("c")
    total = jnp.zeros((384, 128), F32)
    for k in range(4):
        for part in (own, partner):
            values = part[k].astype(F32)
            total = total + values * values
    scale = lax.rsqrt(jnp.sum(total, axis=1, keepdims=True) * (1.0 / 1024) + EPS)
    acc = jnp.zeros((384, 384), F32)
    for k in range(4):
        for part, core in ((own, c), (partner, 1 - c)):
            block = behind("y", k) * 2 + core
            gains = gain[pl.ds(block, 1), :]
            normed = (part[k].astype(F32) * scale * gains).astype(BF16)
            rows = weights[pl.ds(pl.multiple_of(block * 128, 128), 128), :]
            acc = acc + jnp.dot(normed, rows, preferred_element_type=F32)
    q[...] = normed_heads(acc[128:256, 0:128])
    kv[:, 0:128] = normed_heads(acc[:, 128:256])
    kv[:, 128:256] = acc[:, 256:384].astype(BF16)


def heads_pieces_body(x0, x1, x2, x3, gain, w0, w1, w2, w3, q, kv, weights):
    fill_weights((w0, w1, w2, w3), weights, 0, 384)
    pieces = [x[...].astype(F32) for x in (x0, x1, x2, x3)]
    total = sum(p * p for p in pieces)
    scale = lax.rsqrt(jnp.sum(total, axis=1, keepdims=True) * (1.0 / 1024) + EPS)
    acc = jnp.zeros((128, 384), F32)
    for k in range(4):
        block = behind("y", k)
        normed = (pieces[k] * scale * gain[block]).astype(BF16)
        rows = weights[pl.ds(pl.multiple_of(block * 256, 256), 256), :]
        acc = acc + jnp.dot(normed, rows, preferred_element_type=F32)
    finish_heads(acc, q, kv)


def heads_whole_body(mine, theirs, gain, w0, w1, w2, w3, q, kv, weights):
    fill_weights((w0, w1, w2, w3), weights, 0, 384)
    stream = (mine[...].astype(F32) + theirs[...].astype(F32)).astype(BF16).astype(F32)
    scale = lax.rsqrt(jnp.sum(stream * stream, axis=1, keepdims=True) * (1.0 / 1024) + EPS)
    normed = (stream * scale * gain[...]).astype(BF16)
    acc = jnp.dot(normed, weights[...], preferred_element_type=F32)
    finish_heads(acc, q, kv)


def attend(q, keys_values, table):
    queries = q[...]
    low = lax.broadcasted_iota(jnp.int32, (128, 128), 1) < HEAD_DIM
    results = []
    for h in range(2):
        mine = jnp.where(low if h == 0 else ~low, queries, jnp.zeros_like(queries))
        weights, total = [], 0.0
        for b, (keys, _) in enumerate(keys_values):
            scores = lax.dot_general(mine, keys, NT, preferred_element_type=F32)
            scores = scores * HEAD_DIM**-0.5 + table[h, :, b * 128 : (b + 1) * 128]
            grown = jnp.exp(scores)
            weights.append(grown)
            total = total + jnp.sum(grown, axis=1, keepdims=True)
        share = 1.0 / total
        out = 0.0
        for grown, (_, values) in zip(weights, keys_values):
            probs = (grown * share).astype(BF16)
            out = out + jnp.dot(probs, values, preferred_element_type=F32)
        results.append(out)
    return jnp.where(low, results[0], results[1]).astype(BF16)


def attend_scatter_body(q, before, own, after, table, w0, w1, w2, w3, kept, s1, s2, s3, weights):
    fill_weights((w0, w1, w2, w3), weights, 384, 512)
    parts = [(p[:, 0:128], p[:, 128:256]) for p in (before, own, after)]
    attended = attend(q, parts, table)
    for k, into in enumerate((kept, s1, s2, s3)):
        rows = weights[pl.ds(pl.multiple_of(ahead("y", k) * 256, 256), 256), :]
        share = lax.dot_general(attended, rows, NT, preferred_element_type=F32)
        into[...] = share.astype(into.dtype)


def attend_first_body(q, kv, table, *rest):
    attend_scatter_body(q, kv.at[0:128], kv.at[128:256], kv.at[256:384], table, *rest)


def attend_body(q, before, own, after, table, out):
    parts = [(p[:, 0:128], p[:, 128:256]) for p in (before, own, after)]
    out[...] = attend(q, parts, table)


def extract_body(w0, w1, w2, w3, out):
    fill_weights((w0, w1, w2, w3), out, 384, 512)


def project_body(a0, a1, a2, a3, w0, w1, w2, w3, out):
    acc = 0.0
    for a, w in ((a0, w0), (a1, w1), (a2, w2), (a3, w3)):
        acc = acc + lax.dot_general(a[...], w[...], NT, preferred_element_type=F32)
    out[...] = acc.astype(BF16)


def sum_body(kept, r1, r2, r3, out):
    out[...] = kept[...] + r1[...].astype(F32) + r2[...].astype(F32) + r3[...].astype(F32)


def pair_sum_body(mine, theirs, out):
    out[...] = (mine[...] + theirs[...]).astype(BF16)


def split_body(kept, r1, r2, r3, mine, theirs):
    c = lax.axis_index("c")
    for into, core in ((mine, c), (theirs, 1 - c)):
        at = pl.ds(pl.multiple_of(core * 128, 128), 128)
        into[...] = (
            kept[:, at] + r1[:, at].astype(F32) + r2[:, at].astype(F32) + r3[:, at].astype(F32)
        )


def scattered(q_and_kv, body, table, weights):
    outs = [shaped(128, 256, dtype=F32)] + [shaped(128, 256)] * 3
    kept, s1, s2, s3 = call(
        body, outs, *q_and_kv, table, *weights,
        scratch=[pltpu.VMEM((1024, 128), BF16)], name="attend_scatter",
    )
    r3 = lax.ppermute(s3, "y", turn(3))
    r1 = lax.ppermute(s1, "y", turn(1))
    r2 = lax.ppermute(s2, "y", turn(2))
    return kept, r1, r2, r3


def local(tokens, norm_gain, w_query, w_key, w_value, w_out, offset_bias, documents):
    first, rest, payload = call(
        pack_body,
        [shaped(64, 512), shaped(2, 64, 512), shaped(144, 128)],
        w_query, w_key, w_value, w_out, tokens, documents.reshape(1, 128), name="pack",
    )
    heads_scratch = [pltpu.VMEM((1024, 384), BF16)]
    first_x = jnp.stack(in_order(first, spread(first, "x")))
    before = from_before(payload)
    after = from_after(payload)
    weights0 = in_order(first_x, spread(first_x, "z"))

    near = jnp.concatenate([before[0:128], tokens, after[0:128]], axis=0)
    near_y = jnp.stack(in_order(near, spread(near, "y")))
    near_partner = swap(near_y)

    rest_x = in_order(rest, spread(rest, "x"))
    layer1_x = jnp.stack([r[0] for r in rest_x])
    layer2_x = jnp.stack([r[1] for r in rest_x])

    rows = jnp.pad(offset_bias, ((0, 0), (0, 0), (0, 0), (0, 16))).reshape(6, 256)
    table = call(
        table_body, shaped(6, 128, 384, dtype=F32), rows, before, payload, after, name="table"
    )

    q, kv = call(
        heads_first_body, [shaped(128, 128), shaped(384, 256)],
        near_y, near_partner, norm_gain[0].reshape(8, 128), *weights0,
        scratch=heads_scratch, name="heads0",
    )
    weights1 = in_order(layer1_x, spread(layer1_x, "z"))
    kept, r1, r2, r3 = scattered((q, kv), attend_first_body, table[0:2], weights0)
    half = call(sum_body, shaped(128, 256, dtype=F32), kept, r1, r2, r3, name="sum0")
    stream = call(pair_sum_body, shaped(128, 256), half, swap(half), name="pair0")
    pieces = in_order(stream, spread(stream, "y"))

    q, kv = call(
        heads_pieces_body, [shaped(128, 128), shaped(128, 256)],
        *pieces, norm_gain[1].reshape(4, 1, 256), *weights1,
        scratch=heads_scratch, name="heads1",
    )
    out1 = call(extract_body, shaped(1024, 128), *weights1, name="extract1")
    out1_y = in_order(out1, spread(out1, "y"))
    weights2 = in_order(layer2_x, spread(layer2_x, "z"))
    attended = call(
        attend_body, shaped(128, 128), q, from_before(kv), kv, from_after(kv), table[2:4],
        name="attend1",
    )
    attended_y = in_order(attended, spread(attended, "y"))
    share = call(project_body, shaped(128, 1024), *attended_y, *out1_y, name="project1")
    q, kv = call(
        heads_whole_body, [shaped(128, 128), shaped(128, 256)],
        share, swap(share), norm_gain[2].reshape(1, 1024), *weights2,
        scratch=heads_scratch, name="heads2",
    )
    kept, r1, r2, r3 = scattered(
        (q, from_before(kv), kv, from_after(kv)), attend_scatter_body, table[4:6], weights2
    )
    mine, theirs = call(
        split_body, [shaped(128, 128, dtype=F32)] * 2, kept, r1, r2, r3, name="split2"
    )
    return call(pair_sum_body, shaped(128, 128), mine, swap(theirs), name="pair2")


def solution(mesh):
    torus = Mesh(mesh.devices.reshape(4, 4, 4, 2), ("z", "x", "y", "c"))
    return jax.shard_map(
        local,
        mesh=torus,
        in_specs=(
            P(SP, TP),
            P(),
            P(None, SP, TP),
            P(None, SP, TP),
            P(None, SP, TP),
            P(None, TP, SP),
            P(None, TP, None, None),
            P(SP),
        ),
        out_specs=P(SP, TP),
        check_vma=False,
    )
```

```python
import jax
import jax.numpy as jnp
from jax import lax
from jax.experimental import pallas as pl
from jax.experimental.pallas import tpu as pltpu
from jax.sharding import Mesh
from jax.sharding import PartitionSpec as P

HEAD_DIM = 64
WIN_ROWS = 8
WIN_COLS = 16
LAYERS = 3
GRID_W = 32
SP = ("z", "x")
TP = ("y", "c")
EPS = 1e-06
F32 = jnp.float32
BF16 = jnp.bfloat16
NT = (((1,), (1,)), ((), ()))


def turn(k):
    return [(i, (i + k) % 4) for i in range(4)]


def spread(a, axis):
    return [lax.ppermute(a, axis, turn(k)) for k in (1, 3, 2)]


def in_order(a, three):
    return [a, three[0], three[2], three[1]]


def gather_rows(a):
    many = a if a.ndim == 3 else jnp.broadcast_to(a[None], (16,) + a.shape)
    return lax.all_to_all(many, SP, 0, 0, tiled=True).reshape(1024, 512)


def after_this(a, done):
    return lax.optimization_barrier((a, done))[0]


def swap(a):
    return lax.ppermute(a, "c", [(0, 1), (1, 0)])


def from_before(a):
    return lax.ppermute(a, SP, [(i, i + 1) for i in range(15)])


def from_after(a):
    return lax.ppermute(a, SP, [(i + 1, i) for i in range(15)])


def behind(axis, k):
    return (lax.axis_index(axis) + (4 - k)) & 3


def ahead(axis, k):
    return (lax.axis_index(axis) + k) & 3


def call(body, outs, *args, scratch=(), name=None, **specs):
    return pl.pallas_call(
        body,
        out_shape=outs,
        **specs,
        scratch_shapes=list(scratch),
        name=name,
        compiler_params=pltpu.CompilerParams(vmem_limit_bytes=24 * 1024 * 1024),
    )(*args)


def shaped(*shape, dtype=BF16):
    return jax.ShapeDtypeStruct(shape, dtype)


def pack_body(
    wq, wk, wv, wo, tokens, docs, first, rest, payload, wq_in, wk_in, wv_in, wo_in, docs_in, sems
):
    pairs = ((wq, wq_in), (wk, wk_in), (wv, wv_in), (wo, wo_in), (docs, docs_in))
    pairs = pairs + ((tokens, payload.at[0:128]),)
    copies = [pltpu.make_async_copy(a, b, sems.at[n]) for n, (a, b) in enumerate(pairs)]
    for copy in copies:
        copy.start()
    for copy in copies:
        copy.wait()
    whole = jnp.concatenate([wq_in[0], wk_in[0], wv_in[0], wo_in[0]], axis=1)
    for n in range(16):
        first[n] = whole
    for layer in (1, 2):
        for n, part in enumerate((wq_in, wk_in, wv_in, wo_in)):
            rest[layer - 1, :, n * 128 : n * 128 + 128] = part[layer]
    payload[128:144, :] = jnp.broadcast_to((docs_in[...] + 1).astype(F32).astype(BF16), (16, 128))


def table_body(bias, before, own, after, table, wide):
    own_docs = own[128:144, :].astype(F32)[0:1]
    query_docs = jnp.broadcast_to(own_docs, (128, 128)).T
    key_docs = jnp.concatenate(
        [before[128:144, :].astype(F32)[0:1], own_docs, after[128:144, :].astype(F32)[0:1]], axis=1
    )
    same = jnp.concatenate([query_docs] * 3, axis=1) == key_docs
    r = lax.broadcasted_iota(jnp.int32, (128, 384), 0)
    m = lax.broadcasted_iota(jnp.int32, (128, 384), 1)
    lag = (m >> 5) - (r >> 5)
    off = (m & 31) - (r & 31) + WIN_COLS // 2
    allowed = same & (lag >= 0) & (lag < WIN_ROWS) & (off >= 0) & (off < WIN_COLS)
    wide[...] = jnp.zeros((8, 256), F32)
    for n in range(2 * LAYERS):
        for lag_row in range(WIN_ROWS):
            at = lag_row * GRID_W
            wide[n : n + 1, at : at + WIN_COLS] = bias[n // 2, n % 2, lag_row : lag_row + 1, :]
    for n in range(2 * LAYERS):
        line = jnp.broadcast_to(wide[n : n + 1, :], (GRID_W, 256))
        line = pltpu.roll(line, 256 - WIN_COLS // 2, 1, stride=1, stride_axis=0)
        line = jnp.concatenate([line, jnp.zeros((GRID_W, 128), F32)], axis=1)
        block = jnp.concatenate(
            [line] + [pltpu.roll(line, 32 * q, 1) for q in range(1, 4)], axis=0
        )
        table[n] = jnp.where(allowed, block, -1e30)


def normed_heads(raw):
    values = raw.astype(BF16).astype(F32)
    squares = values * values
    low = lax.broadcasted_iota(jnp.int32, values.shape, 1) < HEAD_DIM
    first = jnp.sum(jnp.where(low, squares, 0.0), axis=1, keepdims=True)
    second = jnp.sum(jnp.where(low, 0.0, squares), axis=1, keepdims=True)
    scale = jnp.where(
        low,
        lax.rsqrt(first * (1.0 / HEAD_DIM) + EPS),
        lax.rsqrt(second * (1.0 / HEAD_DIM) + EPS),
    )
    return (values * scale).astype(BF16)


def finish_heads(acc, q, kv):
    q[...] = normed_heads(acc[:, 0:128])
    kv[:, 0:128] = normed_heads(acc[:, 128:256])
    kv[:, 128:256] = acc[:, 256:384].astype(BF16)


def heads_first_body(own, partner, gain, weights, q, kv):
    c = lax.axis_index("c")
    total = jnp.zeros((384, 128), F32)
    for k in range(4):
        for part in (own, partner):
            values = part[k].astype(F32)
            total = total + values * values
    scale = lax.rsqrt(jnp.sum(total, axis=1, keepdims=True) * (1.0 / 1024) + EPS)
    acc = jnp.zeros((384, 384), F32)
    for k in range(4):
        for part, core in ((own, c), (partner, 1 - c)):
            block = behind("y", k) * 2 + core
            gains = gain[0:1, pl.ds(pl.multiple_of(block * 128, 128), 128)]
            normed = (part[k].astype(F32) * scale * gains).astype(BF16)
            rows = weights[pl.ds(pl.multiple_of(block * 128, 128), 128), 0:384]
            acc = acc + jnp.dot(normed, rows, preferred_element_type=F32)
    q[...] = normed_heads(acc[128:256, 0:128])
    kv[:, 0:128] = normed_heads(acc[:, 128:256])
    kv[:, 128:256] = acc[:, 256:384].astype(BF16)


def heads_pieces_body(x0, x1, x2, x3, gain, weights, q, kv):
    pieces = [x[...].astype(F32) for x in (x0, x1, x2, x3)]
    total = sum(p * p for p in pieces)
    scale = lax.rsqrt(jnp.sum(total, axis=1, keepdims=True) * (1.0 / 1024) + EPS)
    acc = jnp.zeros((128, 384), F32)
    for k in range(4):
        block = behind("y", k)
        at = pl.ds(pl.multiple_of(block * 256, 256), 256)
        normed = (pieces[k] * scale * gain[1:2, at]).astype(BF16)
        rows = weights[at, 0:384]
        acc = acc + jnp.dot(normed, rows, preferred_element_type=F32)
    finish_heads(acc, q, kv)


def heads_whole_body(mine, theirs, gain, weights, q, kv):
    stream = (mine[...].astype(F32) + theirs[...].astype(F32)).astype(BF16).astype(F32)
    scale = lax.rsqrt(jnp.sum(stream * stream, axis=1, keepdims=True) * (1.0 / 1024) + EPS)
    normed = (stream * scale * gain[2:3, :]).astype(BF16)
    acc = jnp.dot(normed, weights[:, 0:384], preferred_element_type=F32)
    finish_heads(acc, q, kv)


def attend(q, keys_values, table):
    queries = q[...]
    low = lax.broadcasted_iota(jnp.int32, (128, 128), 1) < HEAD_DIM
    results = []
    for h in range(2):
        mine = jnp.where(low if h == 0 else ~low, queries, jnp.zeros_like(queries))
        weights, total = [], 0.0
        for b, (keys, _) in enumerate(keys_values):
            scores = lax.dot_general(mine, keys, NT, preferred_element_type=F32)
            scores = scores * HEAD_DIM**-0.5 + table[h, :, b * 128 : (b + 1) * 128]
            grown = jnp.exp(scores)
            weights.append(grown)
            total = total + jnp.sum(grown, axis=1, keepdims=True)
        share = 1.0 / total
        out = 0.0
        for grown, (_, values) in zip(weights, keys_values):
            probs = (grown * share).astype(BF16)
            out = out + jnp.dot(probs, values, preferred_element_type=F32)
        results.append(out)
    return jnp.where(low, results[0], results[1]).astype(BF16)


def attend_scatter_body(q, before, own, after, table, weights, kept, s1, s2, s3, *, layer):
    parts = [(p[:, 0:128], p[:, 128:256]) for p in (before, own, after)]
    attended = attend(q, parts, table.at[2 * layer : 2 * layer + 2])
    for k, into in enumerate((kept, s1, s2, s3)):
        rows = weights[pl.ds(pl.multiple_of(ahead("y", k) * 256, 256), 256), 384:512]
        share = lax.dot_general(attended, rows, NT, preferred_element_type=F32)
        into[...] = share.astype(into.dtype)


def attend_first_body(q, kv, *rest):
    attend_scatter_body(q, kv.at[0:128], kv.at[128:256], kv.at[256:384], *rest, layer=0)


def attend_last_body(*refs):
    attend_scatter_body(*refs, layer=2)


def attend_body(q, before, own, after, table, out):
    parts = [(p[:, 0:128], p[:, 128:256]) for p in (before, own, after)]
    out[...] = attend(q, parts, table.at[2:4])


def project_body(a0, a1, a2, a3, w, out):
    acc = 0.0
    for k, a in enumerate((a0, a1, a2, a3)):
        acc = acc + lax.dot_general(a[...], w[behind("y", k)], NT, preferred_element_type=F32)
    out[...] = acc.astype(BF16)


def sum_body(kept, r1, r2, r3, out):
    out[...] = kept[...] + r1[...].astype(F32) + r2[...].astype(F32) + r3[...].astype(F32)


def pair_sum_body(mine, theirs, out):
    out[...] = (mine[...] + theirs[...]).astype(BF16)


def split_body(kept, r1, r2, r3, mine, theirs):
    c = lax.axis_index("c")
    for into, core in ((mine, c), (theirs, 1 - c)):
        at = pl.ds(pl.multiple_of(core * 128, 128), 128)
        into[...] = (
            kept[:, at] + r1[:, at].astype(F32) + r2[:, at].astype(F32) + r3[:, at].astype(F32)
        )


def scattered(body, *args):
    outs = [shaped(128, 256, dtype=F32)] + [shaped(128, 256)] * 3
    kept, s1, s2, s3 = call(body, outs, *args, name="attend_scatter")
    r1 = lax.ppermute(s1, "y", turn(1))
    r3 = lax.ppermute(s3, "y", turn(3))
    r2 = lax.ppermute(s2, "y", turn(2))
    return kept, r1, r2, r3


def local(tokens, norm_gain, w_query, w_key, w_value, w_out, offset_bias, documents):
    hbm = pl.BlockSpec(memory_space=pltpu.HBM)
    first, rest, payload = call(
        pack_body,
        [shaped(16, 64, 512), shaped(2, 64, 512), shaped(144, 128)],
        *[
            pltpu.with_memory_space_constraint(a, pltpu.HBM)
            for a in (
                w_query,
                w_key,
                w_value,
                jnp.swapaxes(w_out, 1, 2),
                tokens,
                documents.reshape(1, 128),
            )
        ],
        name="pack",
        in_specs=[hbm] * 6,
        scratch=[pltpu.VMEM((3, 64, 128), BF16)] * 4
        + [pltpu.VMEM((1, 128), jnp.int32), pltpu.SemaphoreType.DMA((6,))],
    )
    weights0 = gather_rows(first)
    before = from_before(payload)
    after = from_after(payload)
    near = jnp.concatenate([before[0:128], payload[0:128], after[0:128]], axis=0)
    near_y = jnp.stack(in_order(near, spread(near, "y")))
    table = call(
        table_body, shaped(6, 128, 384, dtype=F32), offset_bias, before, payload, after,
        scratch=[pltpu.VMEM((8, 256), F32)], name="table",
    )
    near_partner = swap(after_this(near_y, table))

    q, kv = call(
        heads_first_body, [shaped(128, 128), shaped(384, 256)],
        near_y, near_partner, norm_gain, weights0, name="heads0",
    )
    weights1 = gather_rows(after_this(rest[0], q))
    kept, r1, r2, r3 = scattered(attend_first_body, q, kv, table, weights0)
    half = call(sum_body, shaped(128, 256, dtype=F32), kept, r1, r2, r3, name="sum0")
    stream = call(pair_sum_body, shaped(128, 256), half, swap(half), name="pair0")
    pieces = in_order(stream, spread(stream, "y"))

    q, kv = call(
        heads_pieces_body, [shaped(128, 128), shaped(128, 256)],
        *pieces, norm_gain, weights1, name="heads1",
    )
    out1 = jnp.broadcast_to(after_this(weights1, q)[None, :, 384:512], (4, 1024, 128))
    out1_y = lax.all_to_all(out1, "y", 0, 0, tiled=True)
    before, after = from_before(kv), from_after(kv)
    weights2 = gather_rows(after_this(rest[1], (before, after)))
    attended = call(attend_body, shaped(128, 128), q, before, kv, after, table, name="attend1")
    attended_y = in_order(attended, spread(attended, "y"))
    share = call(project_body, shaped(128, 1024), *attended_y, out1_y, name="project1")
    q, kv = call(
        heads_whole_body, [shaped(128, 128), shaped(128, 256)],
        share, swap(share), norm_gain, weights2, name="heads2",
    )
    before, after = from_before(kv), from_after(kv)
    kept, r1, r2, r3 = scattered(attend_last_body, q, before, kv, after, table, weights2)
    mine, theirs = call(
        split_body, [shaped(128, 128, dtype=F32)] * 2, kept, r1, r2, r3, name="split2"
    )
    return call(pair_sum_body, shaped(128, 128), mine, swap(theirs), name="pair2")


def solution(mesh):
    torus = Mesh(mesh.devices.reshape(4, 4, 4, 2), ("z", "x", "y", "c"))
    return jax.shard_map(
        local,
        mesh=torus,
        in_specs=(
            P(SP, TP),
            P(),
            P(None, SP, TP),
            P(None, SP, TP),
            P(None, SP, TP),
            P(None, TP, SP),
            P(None, TP, None, None),
            P(SP),
        ),
        out_specs=P(SP, TP),
        check_vma=False,
    )
```

```python
import functools

import jax
import jax.numpy as jnp
from jax import lax
from jax.experimental import pallas as pl
from jax.experimental.pallas import tpu as pltpu
from jax.sharding import Mesh
from jax.sharding import PartitionSpec as P

HEAD_DIM = 64
WIN_ROWS = 8
WIN_COLS = 16
LAYERS = 3
GRID_W = 32
SP = ("z", "x")
TP = ("y", "c")
EPS = 1e-06
F32 = jnp.float32
BF16 = jnp.bfloat16
NT = (((1,), (1,)), ((), ()))


def turn(k):
    return [(i, (i + k) % 4) for i in range(4)]


def spread(a, axis):
    return [lax.ppermute(a, axis, turn(k)) for k in (1, 3, 2)]


def in_order(a, three):
    return [a, three[0], three[2], three[1]]


def gather_rows(a):
    return lax.all_to_all(a, SP, 0, 0, tiled=True).reshape(1024, 512)


def after_this(a, done):
    return lax.optimization_barrier((a, done))[0]


def swap(a):
    return lax.ppermute(a, "c", [(0, 1), (1, 0)])


def from_before(a):
    return lax.ppermute(a, SP, [(i, i + 1) for i in range(15)])


def from_after(a):
    return lax.ppermute(a, SP, [(i + 1, i) for i in range(15)])


def behind(axis, k):
    return (lax.axis_index(axis) + (4 - k)) & 3


def ahead(axis, k):
    return (lax.axis_index(axis) + k) & 3


def call(body, outs, *args, scratch=(), name=None, **specs):
    return pl.pallas_call(
        body,
        out_shape=outs,
        **specs,
        scratch_shapes=list(scratch),
        name=name,
        compiler_params=pltpu.CompilerParams(vmem_limit_bytes=24 * 1024 * 1024),
    )(*args)


def shaped(*shape, dtype=BF16):
    return jax.ShapeDtypeStruct(shape, dtype)


def pack_body(
    wq, wk, wv, wo, tokens, docs, first, rest, payload, wq_in, wk_in, wv_in, wo_in, docs_in, sems
):
    pairs = ((wq, wq_in), (wk, wk_in), (wv, wv_in), (wo, wo_in), (docs, docs_in))
    pairs = pairs + ((tokens, payload.at[0:128]),)
    copies = [pltpu.make_async_copy(a, b, sems.at[n]) for n, (a, b) in enumerate(pairs)]
    for copy in copies:
        copy.start()
    for copy in copies:
        copy.wait()
    whole = jnp.concatenate([wq_in[0], wk_in[0], wv_in[0], wo_in[0]], axis=1)
    for n in range(16):
        first[n] = whole
    for layer in (1, 2):
        for n, part in enumerate((wq_in, wk_in, wv_in, wo_in)):
            rest[layer - 1, :, n * 128 : n * 128 + 128] = part[layer]
    payload[128:144, :] = jnp.broadcast_to((docs_in[...] + 1).astype(F32).astype(BF16), (16, 128))


def table_body(bias, before, own, after, rest, table, many1, many2, wide):
    for n in range(16):
        many1[n] = rest[0]
        many2[n] = rest[1]
    own_docs = own[128:144, :].astype(F32)[0:1]
    query_docs = jnp.broadcast_to(own_docs, (128, 128)).T
    key_docs = jnp.concatenate(
        [before[128:144, :].astype(F32)[0:1], own_docs, after[128:144, :].astype(F32)[0:1]], axis=1
    )
    same = jnp.concatenate([query_docs] * 3, axis=1) == key_docs
    r = lax.broadcasted_iota(jnp.int32, (128, 384), 0)
    m = lax.broadcasted_iota(jnp.int32, (128, 384), 1)
    lag = (m >> 5) - (r >> 5)
    off = (m & 31) - (r & 31) + WIN_COLS // 2
    allowed = same & (lag >= 0) & (lag < WIN_ROWS) & (off >= 0) & (off < WIN_COLS)
    wide[...] = jnp.zeros((8, 256), F32)
    for n in range(2 * LAYERS):
        for lag_row in range(WIN_ROWS):
            at = lag_row * GRID_W
            wide[n : n + 1, at : at + WIN_COLS] = bias[n // 2, n % 2, lag_row : lag_row + 1, :]
    for n in range(2 * LAYERS):
        line = jnp.broadcast_to(wide[n : n + 1, :], (GRID_W, 256))
        line = pltpu.roll(line, 256 - WIN_COLS // 2, 1, stride=1, stride_axis=0)
        line = jnp.concatenate([line, jnp.zeros((GRID_W, 128), F32)], axis=1)
        block = jnp.concatenate(
            [line] + [pltpu.roll(line, 32 * q, 1) for q in range(1, 4)], axis=0
        )
        table[n] = jnp.where(allowed, block, -1e30)


def normed_heads(raw):
    values = raw.astype(BF16).astype(F32)
    squares = values * values
    low = lax.broadcasted_iota(jnp.int32, values.shape, 1) < HEAD_DIM
    first = jnp.sum(jnp.where(low, squares, 0.0), axis=1, keepdims=True)
    second = jnp.sum(jnp.where(low, 0.0, squares), axis=1, keepdims=True)
    scale = jnp.where(
        low,
        lax.rsqrt(first * (1.0 / HEAD_DIM) + EPS),
        lax.rsqrt(second * (1.0 / HEAD_DIM) + EPS),
    )
    return (values * scale).astype(BF16)


def finish_heads(acc, q, kv):
    q[...] = normed_heads(acc[:, 0:128])
    kv[:, 0:128] = normed_heads(acc[:, 128:256])
    kv[:, 128:256] = acc[:, 256:384].astype(BF16)


def heads_first_body(own, partner, gain, weights, q, kv):
    c = lax.axis_index("c")
    total = jnp.zeros((384, 128), F32)
    for k in range(4):
        for part in (own, partner):
            values = part[k].astype(F32)
            total = total + values * values
    scale = lax.rsqrt(jnp.sum(total, axis=1, keepdims=True) * (1.0 / 1024) + EPS)
    acc = jnp.zeros((384, 384), F32)
    for k in range(4):
        for part, core in ((own, c), (partner, 1 - c)):
            block = behind("y", k) * 2 + core
            gains = gain[0:1, pl.ds(pl.multiple_of(block * 128, 128), 128)]
            normed = (part[k].astype(F32) * scale * gains).astype(BF16)
            rows = weights[pl.ds(pl.multiple_of(block * 128, 128), 128), 0:384]
            acc = acc + jnp.dot(normed, rows, preferred_element_type=F32)
    q[...] = normed_heads(acc[128:256, 0:128])
    kv[:, 0:128] = normed_heads(acc[:, 128:256])
    kv[:, 128:256] = acc[:, 256:384].astype(BF16)


def heads_pieces_body(x0, x1, x2, x3, gain, weights, q, kv, *, layer):
    pieces = [x[...].astype(F32) for x in (x0, x1, x2, x3)]
    total = sum(p * p for p in pieces)
    scale = lax.rsqrt(jnp.sum(total, axis=1, keepdims=True) * (1.0 / 1024) + EPS)
    acc = jnp.zeros((128, 384), F32)
    for k in range(4):
        block = behind("y", k)
        at = pl.ds(pl.multiple_of(block * 256, 256), 256)
        normed = (pieces[k] * scale * gain[layer : layer + 1, at]).astype(BF16)
        rows = weights[at, 0:384]
        acc = acc + jnp.dot(normed, rows, preferred_element_type=F32)
    finish_heads(acc, q, kv)


def attend(q, keys_values, table):
    queries = q[...]
    low = lax.broadcasted_iota(jnp.int32, (128, 128), 1) < HEAD_DIM
    results = []
    for h in range(2):
        mine = jnp.where(low if h == 0 else ~low, queries, jnp.zeros_like(queries))
        weights, total = [], 0.0
        for b, (keys, _) in enumerate(keys_values):
            scores = lax.dot_general(mine, keys, NT, preferred_element_type=F32)
            scores = scores * HEAD_DIM**-0.5 + table[h, :, b * 128 : (b + 1) * 128]
            grown = jnp.exp(scores)
            weights.append(grown)
            total = total + jnp.sum(grown, axis=1, keepdims=True)
        share = 1.0 / total
        out = 0.0
        for grown, (_, values) in zip(weights, keys_values):
            probs = (grown * share).astype(BF16)
            out = out + jnp.dot(probs, values, preferred_element_type=F32)
        results.append(out)
    return jnp.where(low, results[0], results[1]).astype(BF16)


def attend_scatter_body(q, before, own, after, table, weights, kept, s1, s2, s3, *, layer):
    parts = [(p[:, 0:128], p[:, 128:256]) for p in (before, own, after)]
    attended = attend(q, parts, table.at[2 * layer : 2 * layer + 2])
    for k, into in enumerate((kept, s1, s2, s3)):
        rows = weights[pl.ds(pl.multiple_of(ahead("y", k) * 256, 256), 256), 384:512]
        share = lax.dot_general(attended, rows, NT, preferred_element_type=F32)
        into[...] = share.astype(into.dtype)


def attend_first_body(q, kv, *rest):
    attend_scatter_body(q, kv.at[0:128], kv.at[128:256], kv.at[256:384], *rest, layer=0)


def sum_body(kept, r1, r2, r3, out):
    out[...] = kept[...] + r1[...].astype(F32) + r2[...].astype(F32) + r3[...].astype(F32)


def pair_sum_body(mine, theirs, out):
    out[...] = (mine[...] + theirs[...]).astype(BF16)


def split_body(kept, r1, r2, r3, mine, theirs):
    c = lax.axis_index("c")
    for into, core in ((mine, c), (theirs, 1 - c)):
        at = pl.ds(pl.multiple_of(core * 128, 128), 128)
        into[...] = (
            kept[:, at] + r1[:, at].astype(F32) + r2[:, at].astype(F32) + r3[:, at].astype(F32)
        )


def scattered(body, *args):
    outs = [shaped(128, 256, dtype=F32)] + [shaped(128, 256)] * 3
    kept, s1, s2, s3 = call(body, outs, *args, name="attend_scatter")
    r1 = lax.ppermute(s1, "y", turn(1))
    r3 = lax.ppermute(s3, "y", turn(3))
    r2 = lax.ppermute(s2, "y", turn(2))
    return kept, r1, r2, r3


def local(tokens, norm_gain, w_query, w_key, w_value, w_out, offset_bias, documents):
    hbm = pl.BlockSpec(memory_space=pltpu.HBM)
    first, rest, payload = call(
        pack_body,
        [shaped(16, 64, 512), shaped(2, 64, 512), shaped(144, 128)],
        *[
            pltpu.with_memory_space_constraint(a, pltpu.HBM)
            for a in (
                w_query,
                w_key,
                w_value,
                jnp.swapaxes(w_out, 1, 2),
                tokens,
                documents.reshape(1, 128),
            )
        ],
        name="pack",
        in_specs=[hbm] * 6,
        scratch=[pltpu.VMEM((3, 64, 128), BF16)] * 4
        + [pltpu.VMEM((1, 128), jnp.int32), pltpu.SemaphoreType.DMA((6,))],
    )
    before = from_before(payload)
    after = from_after(payload)
    weights0 = gather_rows(after_this(first, (before, after)))
    near = jnp.concatenate([before[0:128], payload[0:128], after[0:128]], axis=0)
    near_y = jnp.stack(in_order(near, spread(near, "y")))
    table, many1, many2 = call(
        table_body, [shaped(6, 128, 384, dtype=F32)] + [shaped(16, 64, 512)] * 2,
        offset_bias, before, payload, after, rest,
        scratch=[pltpu.VMEM((8, 256), F32)], name="table",
    )
    near_partner = swap(after_this(near_y, table))

    q, kv = call(
        heads_first_body, [shaped(128, 128), shaped(384, 256)],
        near_y, near_partner, norm_gain, weights0, name="heads0",
    )
    weights = weights0
    body, args = attend_first_body, (q, kv)
    for layer, many in ((1, many1), (2, many2)):
        kept, r1, r2, r3 = scattered(body, *args, table, weights)
        weights = gather_rows(after_this(many, kept))
        half = call(sum_body, shaped(128, 256, dtype=F32), kept, r1, r2, r3, name="sum")
        stream = call(pair_sum_body, shaped(128, 256), half, swap(half), name="pair")
        pieces = in_order(stream, spread(stream, "y"))
        q, kv = call(
            functools.partial(heads_pieces_body, layer=layer),
            [shaped(128, 128), shaped(128, 256)],
            *pieces, norm_gain, weights, name="heads",
        )
        body = functools.partial(attend_scatter_body, layer=layer)
        args = (q, from_before(kv), kv, from_after(kv))
    kept, r1, r2, r3 = scattered(body, *args, table, weights)
    mine, theirs = call(
        split_body, [shaped(128, 128, dtype=F32)] * 2, kept, r1, r2, r3, name="split"
    )
    return call(pair_sum_body, shaped(128, 128), mine, swap(theirs), name="pair_last")


def solution(mesh):
    torus = Mesh(mesh.devices.reshape(4, 4, 4, 2), ("z", "x", "y", "c"))
    return jax.shard_map(
        local,
        mesh=torus,
        in_specs=(
            P(SP, TP),
            P(),
            P(None, SP, TP),
            P(None, SP, TP),
            P(None, SP, TP),
            P(None, TP, SP),
            P(None, TP, None, None),
            P(SP),
        ),
        out_specs=P(SP, TP),
        check_vma=False,
    )
```

```python
import functools

import jax
import jax.numpy as jnp
from jax import lax
from jax.experimental import pallas as pl
from jax.experimental.pallas import tpu as pltpu
from jax.sharding import Mesh
from jax.sharding import PartitionSpec as P

HEAD_DIM = 64
WIN_ROWS = 8
WIN_COLS = 16
LAYERS = 3
GRID_W = 32
SP = ("z", "x")
TP = ("y", "c")
EPS = 1e-06
F32 = jnp.float32
BF16 = jnp.bfloat16
NT = (((1,), (1,)), ((), ()))


def turn(k):
    return [(i, (i + k) % 4) for i in range(4)]


def spread(a, axis):
    return [lax.ppermute(a, axis, turn(k)) for k in (1, 3, 2)]


def in_order(a, three):
    return [a, three[0], three[2], three[1]]


def gather_rows(a):
    return lax.all_gather(a, SP, axis=0, tiled=True)


def after_this(a, done):
    return lax.optimization_barrier((a, done))[0]


def swap(a):
    return lax.ppermute(a, "c", [(0, 1), (1, 0)])


def from_before(a):
    return lax.ppermute(a, SP, [(i, i + 1) for i in range(15)])


def from_after(a):
    return lax.ppermute(a, SP, [(i + 1, i) for i in range(15)])


def behind(axis, k):
    return (lax.axis_index(axis) + (4 - k)) & 3


def ahead(axis, k):
    return (lax.axis_index(axis) + k) & 3


def call(body, outs, *args, scratch=(), name=None, **specs):
    return pl.pallas_call(
        body,
        out_shape=outs,
        **specs,
        scratch_shapes=list(scratch),
        name=name,
        compiler_params=pltpu.CompilerParams(vmem_limit_bytes=24 * 1024 * 1024),
    )(*args)


def shaped(*shape, dtype=BF16):
    return jax.ShapeDtypeStruct(shape, dtype)


def pack_body(
    wq, wk, wv, wo, tokens, docs, first, second, third, payload,
    wq_in, wk_in, wv_in, wo_in, docs_in, sems
):
    pairs = ((wq, wq_in), (wk, wk_in), (wv, wv_in), (wo, wo_in), (docs, docs_in))
    pairs = pairs + ((tokens, payload.at[0:128]),)
    copies = [pltpu.make_async_copy(a, b, sems.at[n]) for n, (a, b) in enumerate(pairs)]
    for copy in copies:
        copy.start()
    for copy in copies:
        copy.wait()
    for layer, into in enumerate((first, second, third)):
        for n, part in enumerate((wq_in, wk_in, wv_in, wo_in)):
            into[:, n * 128 : n * 128 + 128] = part[layer]
    payload[128:144, :] = jnp.broadcast_to((docs_in[...] + 1).astype(F32).astype(BF16), (16, 128))


def table_body(bias, before, own, after, table, wide):
    own_docs = own[128:144, :].astype(F32)[0:1]
    query_docs = jnp.broadcast_to(own_docs, (128, 128)).T
    key_docs = jnp.concatenate(
        [before[128:144, :].astype(F32)[0:1], own_docs, after[128:144, :].astype(F32)[0:1]], axis=1
    )
    same = jnp.concatenate([query_docs] * 3, axis=1) == key_docs
    r = lax.broadcasted_iota(jnp.int32, (128, 384), 0)
    m = lax.broadcasted_iota(jnp.int32, (128, 384), 1)
    lag = (m >> 5) - (r >> 5)
    off = (m & 31) - (r & 31) + WIN_COLS // 2
    allowed = same & (lag >= 0) & (lag < WIN_ROWS) & (off >= 0) & (off < WIN_COLS)
    wide[...] = jnp.zeros((8, 256), F32)
    for n in range(2 * LAYERS):
        for lag_row in range(WIN_ROWS):
            at = lag_row * GRID_W
            wide[n : n + 1, at : at + WIN_COLS] = bias[n // 2, n % 2, lag_row : lag_row + 1, :]
    for n in range(2 * LAYERS):
        line = jnp.broadcast_to(wide[n : n + 1, :], (GRID_W, 256))
        line = pltpu.roll(line, 256 - WIN_COLS // 2, 1, stride=1, stride_axis=0)
        line = jnp.concatenate([line, jnp.zeros((GRID_W, 128), F32)], axis=1)
        block = jnp.concatenate(
            [line] + [pltpu.roll(line, 32 * q, 1) for q in range(1, 4)], axis=0
        )
        table[n] = jnp.where(allowed, block, -1e30)


def normed_heads(raw):
    values = raw.astype(BF16).astype(F32)
    squares = values * values
    low = lax.broadcasted_iota(jnp.int32, values.shape, 1) < HEAD_DIM
    first = jnp.sum(jnp.where(low, squares, 0.0), axis=1, keepdims=True)
    second = jnp.sum(jnp.where(low, 0.0, squares), axis=1, keepdims=True)
    scale = jnp.where(
        low,
        lax.rsqrt(first * (1.0 / HEAD_DIM) + EPS),
        lax.rsqrt(second * (1.0 / HEAD_DIM) + EPS),
    )
    return (values * scale).astype(BF16)


def finish_heads(acc, q, kv):
    q[...] = normed_heads(acc[:, 0:128])
    kv[:, 0:128] = normed_heads(acc[:, 128:256])
    kv[:, 128:256] = acc[:, 256:384].astype(BF16)


def heads_first_body(own, partner, gain, weights, q, kv):
    c = lax.axis_index("c")
    total = jnp.zeros((384, 128), F32)
    for k in range(4):
        for part in (own, partner):
            values = part[k].astype(F32)
            total = total + values * values
    scale = lax.rsqrt(jnp.sum(total, axis=1, keepdims=True) * (1.0 / 1024) + EPS)
    acc = jnp.zeros((384, 384), F32)
    for k in range(4):
        for part, core in ((own, c), (partner, 1 - c)):
            block = behind("y", k) * 2 + core
            gains = gain[0:1, pl.ds(pl.multiple_of(block * 128, 128), 128)]
            normed = (part[k].astype(F32) * scale * gains).astype(BF16)
            rows = weights[pl.ds(pl.multiple_of(block * 128, 128), 128), 0:384]
            acc = acc + jnp.dot(normed, rows, preferred_element_type=F32)
    q[...] = normed_heads(acc[128:256, 0:128])
    kv[:, 0:128] = normed_heads(acc[:, 128:256])
    kv[:, 128:256] = acc[:, 256:384].astype(BF16)


def heads_pieces_body(x0, x1, x2, x3, gain, weights, q, kv, *, layer):
    pieces = [x[...].astype(F32) for x in (x0, x1, x2, x3)]
    total = sum(p * p for p in pieces)
    scale = lax.rsqrt(jnp.sum(total, axis=1, keepdims=True) * (1.0 / 1024) + EPS)
    acc = jnp.zeros((128, 384), F32)
    for k in range(4):
        block = behind("y", k)
        at = pl.ds(pl.multiple_of(block * 256, 256), 256)
        normed = (pieces[k] * scale * gain[layer : layer + 1, at]).astype(BF16)
        rows = weights[at, 0:384]
        acc = acc + jnp.dot(normed, rows, preferred_element_type=F32)
    finish_heads(acc, q, kv)


def attend(q, keys_values, table):
    queries = q[...]
    low = lax.broadcasted_iota(jnp.int32, (128, 128), 1) < HEAD_DIM
    results = []
    for h in range(2):
        mine = jnp.where(low if h == 0 else ~low, queries, jnp.zeros_like(queries))
        weights, total = [], 0.0
        for b, (keys, _) in enumerate(keys_values):
            scores = lax.dot_general(mine, keys, NT, preferred_element_type=F32)
            scores = scores * HEAD_DIM**-0.5 + table[h, :, b * 128 : (b + 1) * 128]
            grown = jnp.exp(scores)
            weights.append(grown)
            total = total + jnp.sum(grown, axis=1, keepdims=True)
        share = 1.0 / total
        out = 0.0
        for grown, (_, values) in zip(weights, keys_values):
            probs = (grown * share).astype(BF16)
            out = out + jnp.dot(probs, values, preferred_element_type=F32)
        results.append(out)
    return jnp.where(low, results[0], results[1]).astype(BF16)


def attend_scatter_body(q, before, own, after, table, weights, kept, s1, s2, s3, *, layer):
    parts = [(p[:, 0:128], p[:, 128:256]) for p in (before, own, after)]
    attended = attend(q, parts, table.at[2 * layer : 2 * layer + 2])
    for k, into in enumerate((kept, s1, s2, s3)):
        rows = weights[pl.ds(pl.multiple_of(ahead("y", k) * 256, 256), 256), 384:512]
        share = lax.dot_general(attended, rows, NT, preferred_element_type=F32)
        into[...] = share.astype(into.dtype)


def attend_first_body(q, kv, *rest):
    attend_scatter_body(q, kv.at[0:128], kv.at[128:256], kv.at[256:384], *rest, layer=0)


def sum_body(kept, r1, r2, r3, out):
    out[...] = kept[...] + r1[...].astype(F32) + r2[...].astype(F32) + r3[...].astype(F32)


def pair_sum_body(mine, theirs, out):
    out[...] = (mine[...] + theirs[...]).astype(BF16)


def split_body(kept, r1, r2, r3, mine, theirs):
    c = lax.axis_index("c")
    for into, core in ((mine, c), (theirs, 1 - c)):
        at = pl.ds(pl.multiple_of(core * 128, 128), 128)
        into[...] = (
            kept[:, at] + r1[:, at].astype(F32) + r2[:, at].astype(F32) + r3[:, at].astype(F32)
        )


def scattered(body, *args):
    outs = [shaped(128, 256, dtype=F32)] + [shaped(128, 256)] * 3
    kept, s1, s2, s3 = call(body, outs, *args, name="attend_scatter")
    r1 = lax.ppermute(s1, "y", turn(1))
    r3 = lax.ppermute(s3, "y", turn(3))
    r2 = lax.ppermute(s2, "y", turn(2))
    return kept, r1, r2, r3


def local(tokens, norm_gain, w_query, w_key, w_value, w_out, offset_bias, documents):
    hbm = pl.BlockSpec(memory_space=pltpu.HBM)
    first, second, third, payload = call(
        pack_body,
        [shaped(64, 512)] * 3 + [shaped(144, 128)],
        *[
            pltpu.with_memory_space_constraint(a, pltpu.HBM)
            for a in (
                w_query,
                w_key,
                w_value,
                jnp.swapaxes(w_out, 1, 2),
                tokens,
                documents.reshape(1, 128),
            )
        ],
        name="pack",
        in_specs=[hbm] * 6,
        scratch=[pltpu.VMEM((3, 64, 128), BF16)] * 4
        + [pltpu.VMEM((1, 128), jnp.int32), pltpu.SemaphoreType.DMA((6,))],
    )
    before = from_before(payload)
    after = from_after(payload)
    weights0, weights1, weights2 = [gather_rows(a) for a in (first, second, third)]
    near = jnp.concatenate([before[0:128], payload[0:128], after[0:128]], axis=0)
    near_y = jnp.stack(in_order(near, spread(near, "y")))
    table = call(
        table_body, shaped(6, 128, 384, dtype=F32), offset_bias, before, payload, after,
        scratch=[pltpu.VMEM((8, 256), F32)], name="table",
    )
    near_partner = swap(after_this(near_y, table))

    q, kv = call(
        heads_first_body, [shaped(128, 128), shaped(384, 256)],
        near_y, near_partner, norm_gain, weights0, name="heads0",
    )
    weights = weights0
    body, args = attend_first_body, (q, kv)
    for layer, next_weights in ((1, weights1), (2, weights2)):
        kept, r1, r2, r3 = scattered(body, *args, table, weights)
        weights = next_weights
        half = call(sum_body, shaped(128, 256, dtype=F32), kept, r1, r2, r3, name="sum")
        stream = call(pair_sum_body, shaped(128, 256), half, swap(half), name="pair")
        pieces = in_order(stream, spread(stream, "y"))
        q, kv = call(
            functools.partial(heads_pieces_body, layer=layer),
            [shaped(128, 128), shaped(128, 256)],
            *pieces, norm_gain, weights, name="heads",
        )
        body = functools.partial(attend_scatter_body, layer=layer)
        args = (q, from_before(kv), kv, from_after(kv))
    kept, r1, r2, r3 = scattered(body, *args, table, weights)
    mine, theirs = call(
        split_body, [shaped(128, 128, dtype=F32)] * 2, kept, r1, r2, r3, name="split"
    )
    return call(pair_sum_body, shaped(128, 128), mine, swap(theirs), name="pair_last")


def solution(mesh):
    torus = Mesh(mesh.devices.reshape(4, 4, 4, 2), ("z", "x", "y", "c"))
    return jax.shard_map(
        local,
        mesh=torus,
        in_specs=(
            P(SP, TP),
            P(),
            P(None, SP, TP),
            P(None, SP, TP),
            P(None, SP, TP),
            P(None, TP, SP),
            P(None, TP, None, None),
            P(SP),
        ),
        out_specs=P(SP, TP),
        check_vma=False,
    )
```

```python
import functools

import jax
import jax.numpy as jnp
from jax import lax
from jax.experimental import pallas as pl
from jax.experimental.pallas import tpu as pltpu
from jax.sharding import Mesh
from jax.sharding import PartitionSpec as P


HEAD_DIM = 64
WIN_ROWS = 8
WIN_COLS = 16
LAYERS = 3
GRID_W = 32
SP = ("z", "x")
TP = ("y", "c")
EPS = 1e-06
F32 = jnp.float32
BF16 = jnp.bfloat16
NT = (((1,), (1,)), ((), ()))


def turn(k):
    return [(i, (i + k) % 4) for i in range(4)]


def spread(a, axis):
    return [lax.ppermute(a, axis, turn(k)) for k in (1, 3, 2)]


def in_order(a, three):
    return [a, three[0], three[2], three[1]]


def gather_rows(a):
    return lax.all_to_all(a, SP, 0, 0, tiled=True).reshape(1024, 512)


def after_this(a, done):
    return lax.optimization_barrier((a, done))[0]


def swap(a):
    return lax.ppermute(a, "c", [(0, 1), (1, 0)])


def from_before(a):
    return lax.ppermute(a, SP, [(i, i + 1) for i in range(15)])


def from_after(a):
    return lax.ppermute(a, SP, [(i + 1, i) for i in range(15)])


def behind(axis, k):
    return (lax.axis_index(axis) + (4 - k)) & 3


def ahead(axis, k):
    return (lax.axis_index(axis) + k) & 3


def call(body, outs, *args, scratch=(), **specs):
    return pl.pallas_call(
        body,
        out_shape=outs,
        **specs,
        scratch_shapes=list(scratch),
        compiler_params=pltpu.CompilerParams(vmem_limit_bytes=24 * 1024 * 1024),
    )(*args)


def shaped(*shape, dtype=BF16):
    return jax.ShapeDtypeStruct(shape, dtype)


def pack_body(
    wq, wk, wv, wo, first, rest, wq_in, wk_in, wv_in, wo_in, sems
):
    pairs = ((wq, wq_in), (wk, wk_in), (wv, wv_in), (wo, wo_in))
    copies = [pltpu.make_async_copy(a, b, sems.at[n]) for n, (a, b) in enumerate(pairs)]
    for copy in copies:
        copy.start()
    for copy in copies:
        copy.wait()
    whole = jnp.concatenate([wq_in[0], wk_in[0], wv_in[0], wo_in[0]], axis=1)
    for n in range(16):
        first[n] = whole
    for layer in (1, 2):
        for n, part in enumerate((wq_in, wk_in, wv_in, wo_in)):
            rest[layer - 1, :, n * 128 : n * 128 + 128] = part[layer]


def many_body(rest, many1, many2):
    for n in range(16):
        many1[n] = rest[0]
        many2[n] = rest[1]


def table_body(bias, before, own, after, table, wide):
    own_docs = own[128:144, 0:128].astype(F32)[0:1]
    query_docs = jnp.broadcast_to(own_docs, (128, 128)).T
    key_docs = jnp.concatenate(
        [before[128:144, 0:128].astype(F32)[0:1], own_docs, after[128:144, 0:128].astype(F32)[0:1]], axis=1
    )
    same = jnp.concatenate([query_docs] * 3, axis=1) == key_docs
    r = lax.broadcasted_iota(jnp.int32, (128, 384), 0)
    m = lax.broadcasted_iota(jnp.int32, (128, 384), 1)
    lag = (m >> 5) - (r >> 5)
    off = (m & 31) - (r & 31) + WIN_COLS // 2
    allowed = same & (lag >= 0) & (lag < WIN_ROWS) & (off >= 0) & (off < WIN_COLS)
    wide[...] = jnp.zeros((8, 256), F32)
    for n in range(2 * LAYERS):
        for lag_row in range(WIN_ROWS):
            at = lag_row * GRID_W
            wide[n : n + 1, at : at + WIN_COLS] = bias[n // 2, n % 2, lag_row : lag_row + 1, :]
    for n in range(2 * LAYERS):
        line = jnp.broadcast_to(wide[n : n + 1, :], (GRID_W, 256))
        line = pltpu.roll(line, 256 - WIN_COLS // 2, 1, stride=1, stride_axis=0)
        line = jnp.concatenate([line, jnp.zeros((GRID_W, 128), F32)], axis=1)
        block = jnp.concatenate(
            [line] + [pltpu.roll(line, 32 * q, 1) for q in range(1, 4)], axis=0
        )
        table[n] = jnp.where(allowed, block, -1e30)


def normed_heads(raw):
    values = raw.astype(BF16).astype(F32)
    squares = values * values
    low = lax.broadcasted_iota(jnp.int32, values.shape, 1) < HEAD_DIM
    first = jnp.sum(jnp.where(low, squares, 0.0), axis=1, keepdims=True)
    second = jnp.sum(jnp.where(low, 0.0, squares), axis=1, keepdims=True)
    scale = jnp.where(
        low,
        lax.rsqrt(first * (1.0 / HEAD_DIM) + EPS),
        lax.rsqrt(second * (1.0 / HEAD_DIM) + EPS),
    )
    return (values * scale).astype(BF16)


def finish_heads(acc, q, kv):
    q[...] = normed_heads(acc[:, 0:128])
    kv[:, 0:128] = normed_heads(acc[:, 128:256])
    kv[:, 128:256] = acc[:, 256:384].astype(BF16)


def heads_first_body(own, partner, gain, docs, weights, q, kv):
    c = lax.axis_index("c")
    total = jnp.zeros((128, 128), F32)
    for k in range(4):
        for part in (own, partner):
            values = part[k].astype(F32)
            total = total + values * values
    scale = lax.rsqrt(jnp.sum(total, axis=1, keepdims=True) * (1.0 / 1024) + EPS)
    acc = jnp.zeros((128, 384), F32)
    for k in range(4):
        for part, core in ((own, c), (partner, 1 - c)):
            block = behind("y", k) * 2 + core
            gains = gain[0:1, pl.ds(pl.multiple_of(block * 128, 128), 128)]
            normed = (part[k].astype(F32) * scale * gains).astype(BF16)
            rows = weights[pl.ds(pl.multiple_of(block * 128, 128), 128), 0:384]
            acc = acc + jnp.dot(normed, rows, preferred_element_type=F32)
    finish_heads(acc, q, kv.at[0:128])
    line = (docs[...] + 1).astype(F32).astype(BF16)
    kv[128:144, :] = jnp.broadcast_to(jnp.concatenate([line, line], axis=1), (16, 256))


def heads_pieces_body(x0, x1, x2, x3, gain, weights, q, kv, *, layer):
    pieces = [x[...].astype(F32) for x in (x0, x1, x2, x3)]
    total = sum(p * p for p in pieces)
    scale = lax.rsqrt(jnp.sum(total, axis=1, keepdims=True) * (1.0 / 1024) + EPS)
    acc = jnp.zeros((128, 384), F32)
    for k in range(4):
        block = behind("y", k)
        at = pl.ds(pl.multiple_of(block * 256, 256), 256)
        normed = (pieces[k] * scale * gain[layer : layer + 1, at]).astype(BF16)
        rows = weights[at, 0:384]
        acc = acc + jnp.dot(normed, rows, preferred_element_type=F32)
    finish_heads(acc, q, kv)


def attend(q, keys_values, table):
    queries = q[...]
    low = lax.broadcasted_iota(jnp.int32, (128, 128), 1) < HEAD_DIM
    results = []
    for h in range(2):
        mine = jnp.where(low if h == 0 else ~low, queries, jnp.zeros_like(queries))
        weights, total = [], 0.0
        for b, (keys, _) in enumerate(keys_values):
            scores = lax.dot_general(mine, keys, NT, preferred_element_type=F32)
            scores = scores * HEAD_DIM**-0.5 + table[h, :, b * 128 : (b + 1) * 128]
            grown = jnp.exp(scores)
            weights.append(grown)
            total = total + jnp.sum(grown, axis=1, keepdims=True)
        share = 1.0 / total
        out = 0.0
        for grown, (_, values) in zip(weights, keys_values):
            probs = (grown * share).astype(BF16)
            out = out + jnp.dot(probs, values, preferred_element_type=F32)
        results.append(out)
    return jnp.where(low, results[0], results[1]).astype(BF16)


def attend_scatter_body(q, before, own, after, table, weights, kept, s1, s2, s3, *, layer):
    parts = [(p[0:128, 0:128], p[0:128, 128:256]) for p in (before, own, after)]
    attended = attend(q, parts, table.at[2 * layer : 2 * layer + 2])
    for k, into in enumerate((kept, s1, s2, s3)):
        rows = weights[pl.ds(pl.multiple_of(ahead("y", k) * 256, 256), 256), 384:512]
        share = lax.dot_general(attended, rows, NT, preferred_element_type=F32)
        into[...] = share.astype(into.dtype)


def sum_body(kept, r1, r2, r3, out):
    out[...] = kept[...] + r1[...].astype(F32) + r2[...].astype(F32) + r3[...].astype(F32)


def pair_sum_body(mine, theirs, out):
    out[...] = (mine[...] + theirs[...]).astype(BF16)


def split_body(kept, r1, r2, r3, mine, theirs):
    c = lax.axis_index("c")
    for into, core in ((mine, c), (theirs, 1 - c)):
        at = pl.ds(pl.multiple_of(core * 128, 128), 128)
        into[...] = (
            kept[:, at] + r1[:, at].astype(F32) + r2[:, at].astype(F32) + r3[:, at].astype(F32)
        )


def scattered(body, *args):
    outs = [shaped(128, 256, dtype=F32)] + [shaped(128, 256)] * 3
    kept, s1, s2, s3 = call(body, outs, *args)
    r1 = lax.ppermute(s1, "y", turn(1))
    r3 = lax.ppermute(s3, "y", turn(3))
    r2 = lax.ppermute(s2, "y", turn(2))
    return kept, r1, r2, r3


def local(tokens, norm_gain, w_query, w_key, w_value, w_out, offset_bias, documents):
    hbm = pl.BlockSpec(memory_space=pltpu.HBM)
    first, rest = call(
        pack_body,
        [shaped(16, 64, 512), shaped(2, 64, 512)],
        *[
            pltpu.with_memory_space_constraint(a, pltpu.HBM)
            for a in (w_query, w_key, w_value, jnp.swapaxes(w_out, 1, 2))
        ],
        in_specs=[hbm] * 4,
        scratch=[pltpu.VMEM((3, 64, 128), BF16)] * 4 + [pltpu.SemaphoreType.DMA((4,))],
    )
    weights = gather_rows(first)
    near_y = jnp.stack(in_order(tokens, spread(tokens, "y")))
    many1, many2 = call(many_body, [shaped(16, 64, 512)] * 2, rest)
    near_partner = swap(after_this(near_y, many1))

    q, kv = call(
        heads_first_body, [shaped(128, 128), shaped(144, 256)],
        near_y, near_partner, norm_gain, documents.reshape(1, 128), weights,
    )
    args = (q, from_before(kv), kv, from_after(kv))
    table = call(
        table_body, shaped(6, 128, 384, dtype=F32), offset_bias, *args[1:],
        scratch=[pltpu.VMEM((8, 256), F32)],
    )
    body = functools.partial(attend_scatter_body, layer=0)
    for layer, many in ((1, many1), (2, many2)):
        kept, r1, r2, r3 = scattered(body, *args, table, weights)
        weights = gather_rows(after_this(many, kept))
        half = call(sum_body, shaped(128, 256, dtype=F32), kept, r1, r2, r3)
        stream = call(pair_sum_body, shaped(128, 256), half, swap(half))
        pieces = in_order(stream, spread(stream, "y"))
        q, kv = call(
            functools.partial(heads_pieces_body, layer=layer),
            [shaped(128, 128), shaped(128, 256)],
            *pieces, norm_gain, weights,
        )
        body = functools.partial(attend_scatter_body, layer=layer)
        args = (q, from_before(kv), kv, from_after(kv))
    kept, r1, r2, r3 = scattered(body, *args, table, weights)
    mine, theirs = call(split_body, [shaped(128, 128, dtype=F32)] * 2, kept, r1, r2, r3)
    return call(pair_sum_body, shaped(128, 128), mine, swap(theirs))


def solution(mesh):
    torus = Mesh(mesh.devices.reshape(4, 4, 4, 2), ("z", "x", "y", "c"))
    return jax.shard_map(
        local,
        mesh=torus,
        in_specs=(
            P(SP, TP),
            P(),
            P(None, SP, TP),
            P(None, SP, TP),
            P(None, SP, TP),
            P(None, TP, SP),
            P(None, TP, None, None),
            P(SP),
        ),
        out_specs=P(SP, TP),
        check_vma=False,
    )
```

```python
import functools

import jax
import jax.numpy as jnp
from jax import lax
from jax.experimental import pallas as pl
from jax.experimental.pallas import tpu as pltpu
from jax.sharding import Mesh
from jax.sharding import PartitionSpec as P


HEAD_DIM = 64
WIN_ROWS = 8
WIN_COLS = 16
LAYERS = 3
GRID_W = 32
SP = ("z", "x")
TP = ("y", "c")
EPS = 1e-06
F32 = jnp.float32
BF16 = jnp.bfloat16
NT = (((1,), (1,)), ((), ()))


def turn(k):
    return [(i, (i + k) % 4) for i in range(4)]


def spread(a, axis):
    sent = []
    for k in (1, 3, 2):
        sent.append(lax.ppermute(a, axis, turn(k)))
    return sent


def in_order(a, three):
    return [a, three[0], three[2], three[1]]


def gather_rows(a):
    return lax.all_to_all(a, SP, 0, 0, tiled=True).reshape(1024, 512)


def after_this(a, done):
    return lax.optimization_barrier((a, done))[0]


def swap(a):
    return lax.ppermute(a, "c", [(0, 1), (1, 0)])


def from_before(a):
    return lax.ppermute(a, SP, [(i, i + 1) for i in range(15)])


def from_after(a):
    return lax.ppermute(a, SP, [(i + 1, i) for i in range(15)])


def behind(axis, k):
    return (lax.axis_index(axis) + (4 - k)) & 3


def ahead(axis, k):
    return (lax.axis_index(axis) + k) & 3


def call(body, outs, *args, scratch=(), **specs):
    return pl.pallas_call(
        body,
        out_shape=outs,
        **specs,
        scratch_shapes=list(scratch),
        compiler_params=pltpu.CompilerParams(vmem_limit_bytes=24 * 1024 * 1024),
    )(*args)


def shaped(*shape, dtype=BF16):
    return jax.ShapeDtypeStruct(shape, dtype)


def fetch(pairs, sems):
    copies = [pltpu.make_async_copy(a, b, sems.at[n]) for n, (a, b) in enumerate(pairs)]
    for copy in copies:
        copy.start()
    for copy in copies:
        copy.wait()


def pack_body(wq, wk, wv, wo, first, parts, sems):
    fetch([(w.at[0], parts.at[n]) for n, w in enumerate((wq, wk, wv, wo))], sems)
    whole = jnp.concatenate([parts[n] for n in range(4)], axis=1)
    for n in range(16):
        first[n] = whole


def many_body(wq, wk, wv, wo, many1, many2, parts, sems):
    pairs = [(w.at[1:3], parts.at[n]) for n, w in enumerate((wq, wk, wv, wo))]
    fetch(pairs, sems)
    for layer, many in enumerate((many1, many2)):
        whole = jnp.concatenate([parts[n, layer] for n in range(4)], axis=1)
        for n in range(16):
            many[n] = whole


def table_body(bias, before, own, after, table, wide):
    own_docs = own[128:144, 0:128].astype(F32)[0:1]
    query_docs = jnp.broadcast_to(own_docs, (128, 128)).T
    key_docs = jnp.concatenate(
        [before[128:144, 0:128].astype(F32)[0:1], own_docs, after[128:144, 0:128].astype(F32)[0:1]], axis=1
    )
    same = jnp.concatenate([query_docs] * 3, axis=1) == key_docs
    r = lax.broadcasted_iota(jnp.int32, (128, 384), 0)
    m = lax.broadcasted_iota(jnp.int32, (128, 384), 1)
    lag = (m >> 5) - (r >> 5)
    off = (m & 31) - (r & 31) + WIN_COLS // 2
    allowed = same & (lag >= 0) & (lag < WIN_ROWS) & (off >= 0) & (off < WIN_COLS)
    wide[...] = jnp.zeros((8, 256), F32)
    for n in range(2 * LAYERS):
        for lag_row in range(WIN_ROWS):
            at = lag_row * GRID_W
            wide[n : n + 1, at : at + WIN_COLS] = bias[n // 2, n % 2, lag_row : lag_row + 1, :]
    for n in range(2 * LAYERS):
        line = jnp.broadcast_to(wide[n : n + 1, :], (GRID_W, 256))
        line = pltpu.roll(line, 256 - WIN_COLS // 2, 1, stride=1, stride_axis=0)
        line = jnp.concatenate([line, jnp.zeros((GRID_W, 128), F32)], axis=1)
        block = jnp.concatenate(
            [line] + [pltpu.roll(line, 32 * q, 1) for q in range(1, 4)], axis=0
        )
        table[n] = jnp.where(allowed, block, -1e30)


def normed_heads(raw):
    values = raw.astype(BF16).astype(F32)
    squares = values * values
    low = lax.broadcasted_iota(jnp.int32, values.shape, 1) < HEAD_DIM
    first = jnp.sum(jnp.where(low, squares, 0.0), axis=1, keepdims=True)
    second = jnp.sum(jnp.where(low, 0.0, squares), axis=1, keepdims=True)
    scale = jnp.where(
        low,
        lax.rsqrt(first * (1.0 / HEAD_DIM) + EPS),
        lax.rsqrt(second * (1.0 / HEAD_DIM) + EPS),
    )
    return (values * scale).astype(BF16)


def finish_heads(acc, q, kv):
    q[...] = normed_heads(acc[:, 0:128])
    kv[:, 0:128] = normed_heads(acc[:, 128:256])
    kv[:, 128:256] = acc[:, 256:384].astype(BF16)


def heads_first_body(own, partner, gain, docs, weights, q, kv):
    c = lax.axis_index("c")
    total = jnp.zeros((128, 128), F32)
    for k in range(4):
        for part in (own, partner):
            values = part[k].astype(F32)
            total = total + values * values
    scale = lax.rsqrt(jnp.sum(total, axis=1, keepdims=True) * (1.0 / 1024) + EPS)
    acc = jnp.zeros((128, 384), F32)
    for k in range(4):
        for part, core in ((own, c), (partner, 1 - c)):
            block = behind("y", k) * 2 + core
            gains = gain[0:1, pl.ds(pl.multiple_of(block * 128, 128), 128)]
            normed = (part[k].astype(F32) * scale * gains).astype(BF16)
            rows = weights[pl.ds(pl.multiple_of(block * 128, 128), 128), 0:384]
            acc = acc + jnp.dot(normed, rows, preferred_element_type=F32)
    finish_heads(acc, q, kv.at[0:128])
    line = (docs[...] + 1).astype(F32).astype(BF16)
    kv[128:144, :] = jnp.broadcast_to(jnp.concatenate([line, line], axis=1), (16, 256))


def heads_pieces_body(x0, x1, x2, x3, gain, weights, q, kv, *, layer):
    pieces = [x[...].astype(F32) for x in (x0, x1, x2, x3)]
    total = sum(p * p for p in pieces)
    scale = lax.rsqrt(jnp.sum(total, axis=1, keepdims=True) * (1.0 / 1024) + EPS)
    acc = jnp.zeros((128, 384), F32)
    for k in range(4):
        block = behind("y", k)
        at = pl.ds(pl.multiple_of(block * 256, 256), 256)
        normed = (pieces[k] * scale * gain[layer : layer + 1, at]).astype(BF16)
        rows = weights[at, 0:384]
        acc = acc + jnp.dot(normed, rows, preferred_element_type=F32)
    finish_heads(acc, q, kv)


def attend(q, keys_values, table):
    queries = q[...]
    low = lax.broadcasted_iota(jnp.int32, (128, 128), 1) < HEAD_DIM
    results = []
    for h in range(2):
        mine = jnp.where(low if h == 0 else ~low, queries, jnp.zeros_like(queries))
        weights, total = [], 0.0
        for b, (keys, _) in enumerate(keys_values):
            scores = lax.dot_general(mine, keys, NT, preferred_element_type=F32)
            scores = scores * HEAD_DIM**-0.5 + table[h, :, b * 128 : (b + 1) * 128]
            grown = jnp.exp(scores)
            weights.append(grown)
            total = total + jnp.sum(grown, axis=1, keepdims=True)
        share = 1.0 / total
        out = 0.0
        for grown, (_, values) in zip(weights, keys_values):
            probs = (grown * share).astype(BF16)
            out = out + jnp.dot(probs, values, preferred_element_type=F32)
        results.append(out)
    return jnp.where(low, results[0], results[1]).astype(BF16)


def attend_scatter_body(q, before, own, after, table, weights, kept, s1, s2, s3, *, layer):
    parts = [(p[0:128, 0:128], p[0:128, 128:256]) for p in (before, own, after)]
    attended = attend(q, parts, table.at[2 * layer : 2 * layer + 2])
    for k, into in enumerate((kept, s1, s2, s3)):
        rows = weights[pl.ds(pl.multiple_of(ahead("y", k) * 256, 256), 256), 384:512]
        share = lax.dot_general(attended, rows, NT, preferred_element_type=F32)
        into[...] = share.astype(into.dtype)


def sum_body(kept, r1, r2, r3, out):
    out[...] = kept[...] + r1[...].astype(F32) + r2[...].astype(F32) + r3[...].astype(F32)


def pair_sum_body(mine, theirs, out):
    out[...] = (mine[...] + theirs[...]).astype(BF16)


def split_body(kept, r1, r2, r3, mine, theirs):
    c = lax.axis_index("c")
    for into, core in ((mine, c), (theirs, 1 - c)):
        at = pl.ds(pl.multiple_of(core * 128, 128), 128)
        into[...] = (
            kept[:, at] + r1[:, at].astype(F32) + r2[:, at].astype(F32) + r3[:, at].astype(F32)
        )


def scattered(body, *args):
    outs = [shaped(128, 256, dtype=F32)] + [shaped(128, 256)] * 3
    kept, s1, s2, s3 = call(body, outs, *args)
    r1 = lax.ppermute(s1, "y", turn(1))
    r3 = lax.ppermute(s3, "y", turn(3))
    r2 = lax.ppermute(s2, "y", turn(2))
    return kept, r1, r2, r3


def local(tokens, norm_gain, w_query, w_key, w_value, w_out, offset_bias, documents):
    hbm = pl.BlockSpec(memory_space=pltpu.HBM)
    held = [
        pltpu.with_memory_space_constraint(a, pltpu.HBM)
        for a in (w_query, w_key, w_value, jnp.swapaxes(w_out, 1, 2))
    ]
    first = call(
        pack_body, shaped(16, 64, 512), *held, in_specs=[hbm] * 4,
        scratch=[pltpu.VMEM((4, 64, 128), BF16), pltpu.SemaphoreType.DMA((4,))],
    )
    weights = gather_rows(first)
    near_y = jnp.stack(in_order(tokens, spread(tokens, "y")))
    many1, many2 = call(
        many_body, [shaped(16, 64, 512)] * 2, *held, in_specs=[hbm] * 4,
        scratch=[pltpu.VMEM((4, 2, 64, 128), BF16), pltpu.SemaphoreType.DMA((4,))],
    )
    near_partner = swap(after_this(near_y, many1))

    q, kv = call(
        heads_first_body, [shaped(128, 128), shaped(144, 256)],
        near_y, near_partner, norm_gain, documents.reshape(1, 128), weights,
    )
    args = (q, from_before(kv), kv, from_after(kv))
    table = call(
        table_body, shaped(6, 128, 384, dtype=F32), offset_bias, *args[1:],
        scratch=[pltpu.VMEM((8, 256), F32)],
    )
    body = functools.partial(attend_scatter_body, layer=0)
    for layer, many in ((1, many1), (2, many2)):
        kept, r1, r2, r3 = scattered(body, *args, table, weights)
        weights = gather_rows(after_this(many, kept))
        half = call(sum_body, shaped(128, 256, dtype=F32), kept, r1, r2, r3)
        stream = call(pair_sum_body, shaped(128, 256), half, swap(half))
        pieces = in_order(stream, spread(stream, "y"))
        q, kv = call(
            functools.partial(heads_pieces_body, layer=layer),
            [shaped(128, 128), shaped(128, 256)],
            *pieces, norm_gain, weights,
        )
        body = functools.partial(attend_scatter_body, layer=layer)
        args = (q, from_before(kv), kv, from_after(kv))
    kept, r1, r2, r3 = scattered(body, *args, table, weights)
    mine, theirs = call(split_body, [shaped(128, 128, dtype=F32)] * 2, kept, r1, r2, r3)
    return call(pair_sum_body, shaped(128, 128), mine, swap(theirs))


def solution(mesh):
    torus = Mesh(mesh.devices.reshape(4, 4, 4, 2), ("z", "x", "y", "c"))
    return jax.shard_map(
        local,
        mesh=torus,
        in_specs=(
            P(SP, TP),
            P(),
            P(None, SP, TP),
            P(None, SP, TP),
            P(None, SP, TP),
            P(None, TP, SP),
            P(None, TP, None, None),
            P(SP),
        ),
        out_specs=P(SP, TP),
        check_vma=False,
    )
```

```python
import functools

import jax
import jax.numpy as jnp
from jax import lax
from jax.experimental import pallas as pl
from jax.experimental.pallas import tpu as pltpu
from jax.sharding import Mesh
from jax.sharding import PartitionSpec as P


HEAD_DIM = 64
WIN_ROWS = 8
WIN_COLS = 16
LAYERS = 3
GRID_W = 32
SP = ("z", "x")
TP = ("y", "c")
EPS = 1e-06
F32 = jnp.float32
BF16 = jnp.bfloat16
NT = (((1,), (1,)), ((), ()))


def turn(k):
    return [(i, (i + k) % 4) for i in range(4)]


def spread(a, axis):
    return [lax.ppermute(a, axis, turn(k)) for k in (1, 3, 2)]


def in_order(a, three):
    return [a, three[0], three[2], three[1]]


def gather_rows(a):
    return lax.all_to_all(a, SP, 0, 0, tiled=True).reshape(1024, 512)


def after_this(a, done):
    return lax.optimization_barrier((a, done))[0]


def swap(a):
    return lax.ppermute(a, "c", [(0, 1), (1, 0)])


def from_before(a):
    return lax.ppermute(a, SP, [(i, i + 1) for i in range(15)])


def from_after(a):
    return lax.ppermute(a, SP, [(i + 1, i) for i in range(15)])


def behind(axis, k):
    return (lax.axis_index(axis) + (4 - k)) & 3


def ahead(axis, k):
    return (lax.axis_index(axis) + k) & 3


def call(body, outs, *args, scratch=(), **specs):
    return pl.pallas_call(
        body,
        out_shape=outs,
        **specs,
        scratch_shapes=list(scratch),
        compiler_params=pltpu.CompilerParams(vmem_limit_bytes=24 * 1024 * 1024),
    )(*args)


def shaped(*shape, dtype=BF16):
    return jax.ShapeDtypeStruct(shape, dtype)


def fetch(pairs, sems):
    copies = [pltpu.make_async_copy(a, b, sems.at[n]) for n, (a, b) in enumerate(pairs)]
    for copy in copies:
        copy.start()
    for copy in copies:
        copy.wait()


def pack_body(wq, wk, wv, wo, first, parts, sems):
    fetch([(w.at[0], parts.at[n]) for n, w in enumerate((wq, wk, wv, wo))], sems)
    whole = jnp.concatenate([parts[n] for n in range(4)], axis=1)
    for n in range(16):
        first[n] = whole


def many_body(wq, wk, wv, wo, bias, many1, many2, wide, parts, sems):
    pairs = [(w.at[1:3], parts.at[n]) for n, w in enumerate((wq, wk, wv, wo))]
    fetch(pairs, sems)
    for layer, many in enumerate((many1, many2)):
        whole = jnp.concatenate([parts[n, layer] for n in range(4)], axis=1)
        for n in range(16):
            many[n] = whole
    wide[...] = jnp.zeros((8, 256), F32)
    for n in range(2 * LAYERS):
        for lag_row in range(WIN_ROWS):
            at = lag_row * GRID_W
            wide[n : n + 1, at : at + WIN_COLS] = bias[n // 2, n % 2, lag_row : lag_row + 1, :]


def table_body(wide, before, own, after, table):
    own_docs = own[128:144, 0:128].astype(F32)[0:1]
    query_docs = jnp.broadcast_to(own_docs, (128, 128)).T
    key_docs = jnp.concatenate(
        [before[128:144, 0:128].astype(F32)[0:1], own_docs, after[128:144, 0:128].astype(F32)[0:1]], axis=1
    )
    same = jnp.concatenate([query_docs] * 3, axis=1) == key_docs
    r = lax.broadcasted_iota(jnp.int32, (128, 384), 0)
    m = lax.broadcasted_iota(jnp.int32, (128, 384), 1)
    lag = (m >> 5) - (r >> 5)
    off = (m & 31) - (r & 31) + WIN_COLS // 2
    allowed = same & (lag >= 0) & (lag < WIN_ROWS) & (off >= 0) & (off < WIN_COLS)
    for n in range(2 * LAYERS):
        line = jnp.broadcast_to(wide[n : n + 1, :], (GRID_W, 256))
        line = pltpu.roll(line, 256 - WIN_COLS // 2, 1, stride=1, stride_axis=0)
        line = jnp.concatenate([line, jnp.zeros((GRID_W, 128), F32)], axis=1)
        block = jnp.concatenate(
            [line] + [pltpu.roll(line, 32 * q, 1) for q in range(1, 4)], axis=0
        )
        table[n] = jnp.where(allowed, block, -1e30)


def normed_heads(raw):
    values = raw.astype(BF16).astype(F32)
    squares = values * values
    low = lax.broadcasted_iota(jnp.int32, values.shape, 1) < HEAD_DIM
    first = jnp.sum(jnp.where(low, squares, 0.0), axis=1, keepdims=True)
    second = jnp.sum(jnp.where(low, 0.0, squares), axis=1, keepdims=True)
    scale = jnp.where(
        low,
        lax.rsqrt(first * (1.0 / HEAD_DIM) + EPS),
        lax.rsqrt(second * (1.0 / HEAD_DIM) + EPS),
    )
    return (values * scale).astype(BF16)


def finish_heads(acc, q, kv):
    q[...] = normed_heads(acc[:, 0:128])
    kv[:, 0:128] = normed_heads(acc[:, 128:256])
    kv[:, 128:256] = acc[:, 256:384].astype(BF16)


def heads_first_body(own, partner, gain, docs, weights, q, kv):
    c = lax.axis_index("c")
    total = jnp.zeros((128, 128), F32)
    for k in range(4):
        for part in (own, partner):
            values = part[k].astype(F32)
            total = total + values * values
    scale = lax.rsqrt(jnp.sum(total, axis=1, keepdims=True) * (1.0 / 1024) + EPS)
    acc = jnp.zeros((128, 384), F32)
    for k in range(4):
        for part, core in ((own, c), (partner, 1 - c)):
            block = behind("y", k) * 2 + core
            gains = gain[0:1, pl.ds(pl.multiple_of(block * 128, 128), 128)]
            normed = (part[k].astype(F32) * scale * gains).astype(BF16)
            rows = weights[pl.ds(pl.multiple_of(block * 128, 128), 128), 0:384]
            acc = acc + jnp.dot(normed, rows, preferred_element_type=F32)
    finish_heads(acc, q, kv.at[0:128])
    line = (docs[...] + 1).astype(F32).astype(BF16)
    kv[128:144, :] = jnp.broadcast_to(jnp.concatenate([line, line], axis=1), (16, 256))


def heads_pieces_body(x0, x1, x2, x3, gain, weights, q, kv, *, layer):
    pieces = [x[...].astype(F32) for x in (x0, x1, x2, x3)]
    total = sum(p * p for p in pieces)
    scale = lax.rsqrt(jnp.sum(total, axis=1, keepdims=True) * (1.0 / 1024) + EPS)
    acc = jnp.zeros((128, 384), F32)
    for k in range(4):
        block = behind("y", k)
        at = pl.ds(pl.multiple_of(block * 256, 256), 256)
        normed = (pieces[k] * scale * gain[layer : layer + 1, at]).astype(BF16)
        rows = weights[at, 0:384]
        acc = acc + jnp.dot(normed, rows, preferred_element_type=F32)
    finish_heads(acc, q, kv)


def attend(q, keys_values, table):
    queries = q[...]
    low = lax.broadcasted_iota(jnp.int32, (128, 128), 1) < HEAD_DIM
    results = []
    for h in range(2):
        mine = jnp.where(low if h == 0 else ~low, queries, jnp.zeros_like(queries))
        weights, total = [], 0.0
        for b, (keys, _) in enumerate(keys_values):
            scores = lax.dot_general(mine, keys, NT, preferred_element_type=F32)
            scores = scores * HEAD_DIM**-0.5 + table[h, :, b * 128 : (b + 1) * 128]
            grown = jnp.exp(scores)
            weights.append(grown)
            total = total + jnp.sum(grown, axis=1, keepdims=True)
        share = 1.0 / total
        out = 0.0
        for grown, (_, values) in zip(weights, keys_values):
            probs = (grown * share).astype(BF16)
            out = out + jnp.dot(probs, values, preferred_element_type=F32)
        results.append(out)
    return jnp.where(low, results[0], results[1]).astype(BF16)


def attend_scatter_body(q, before, own, after, table, weights, kept, s1, s2, s3, *, layer):
    parts = [(p[0:128, 0:128], p[0:128, 128:256]) for p in (before, own, after)]
    attended = attend(q, parts, table.at[2 * layer : 2 * layer + 2])
    for k, into in enumerate((kept, s1, s2, s3)):
        rows = weights[pl.ds(pl.multiple_of(ahead("y", k) * 256, 256), 256), 384:512]
        share = lax.dot_general(attended, rows, NT, preferred_element_type=F32)
        into[...] = share.astype(into.dtype)


def sum_body(kept, r1, r2, r3, out):
    out[...] = kept[...] + r1[...].astype(F32) + r2[...].astype(F32) + r3[...].astype(F32)


def pair_sum_body(mine, theirs, out):
    out[...] = (mine[...] + theirs[...]).astype(BF16)


def split_body(kept, r1, r2, r3, mine, theirs):
    c = lax.axis_index("c")
    for into, core in ((mine, c), (theirs, 1 - c)):
        at = pl.ds(pl.multiple_of(core * 128, 128), 128)
        into[...] = (
            kept[:, at] + r1[:, at].astype(F32) + r2[:, at].astype(F32) + r3[:, at].astype(F32)
        )


def scattered(body, *args):
    outs = [shaped(128, 256, dtype=F32)] + [shaped(128, 256)] * 3
    kept, s1, s2, s3 = call(body, outs, *args)
    r1 = lax.ppermute(s1, "y", turn(1))
    r3 = lax.ppermute(s3, "y", turn(3))
    r2 = lax.ppermute(s2, "y", turn(2))
    return kept, r1, r2, r3


def local(tokens, norm_gain, w_query, w_key, w_value, w_out, offset_bias, documents):
    hbm = pl.BlockSpec(memory_space=pltpu.HBM)
    held = [
        pltpu.with_memory_space_constraint(a, pltpu.HBM)
        for a in (w_query, w_key, w_value, jnp.swapaxes(w_out, 1, 2))
    ]
    first = call(
        pack_body, shaped(16, 64, 512), *held, in_specs=[hbm] * 4,
        scratch=[pltpu.VMEM((4, 64, 128), BF16), pltpu.SemaphoreType.DMA((4,))],
    )
    weights = gather_rows(first)
    near_y = jnp.stack(in_order(tokens, spread(tokens, "y")))
    many1, many2, wide = call(
        many_body, [shaped(16, 64, 512)] * 2 + [shaped(8, 256, dtype=F32)],
        *held, offset_bias, in_specs=[hbm] * 4 + [pl.BlockSpec()],
        scratch=[pltpu.VMEM((4, 2, 64, 128), BF16), pltpu.SemaphoreType.DMA((4,))],
    )
    near_partner = swap(after_this(near_y, many1))

    q, kv = call(
        heads_first_body, [shaped(128, 128), shaped(144, 256)],
        near_y, near_partner, norm_gain, documents.reshape(1, 128), weights,
    )
    for layer in range(LAYERS):
        after = from_after(kv)
        before = from_before(kv)
        if layer < 2:
            next_weights = gather_rows(after_this((many1, many2)[layer], kv))
        if layer == 0:
            table = call(table_body, shaped(6, 128, 384, dtype=F32), wide, before, kv, after)
        kept, r1, r2, r3 = scattered(
            functools.partial(attend_scatter_body, layer=layer),
            q, before, kv, after, table, weights,
        )
        if layer == 2:
            break
        half = call(sum_body, shaped(128, 256, dtype=F32), kept, r1, r2, r3)
        stream = call(pair_sum_body, shaped(128, 256), half, swap(half))
        weights = next_weights
        q, kv = call(
            functools.partial(heads_pieces_body, layer=layer + 1),
            [shaped(128, 128), shaped(128, 256)],
            *in_order(stream, spread(stream, "y")), norm_gain, weights,
        )
    mine, theirs = call(split_body, [shaped(128, 128, dtype=F32)] * 2, kept, r1, r2, r3)
    return call(pair_sum_body, shaped(128, 128), mine, swap(theirs))


def solution(mesh):
    torus = Mesh(mesh.devices.reshape(4, 4, 4, 2), ("z", "x", "y", "c"))
    return jax.shard_map(
        local,
        mesh=torus,
        in_specs=(
            P(SP, TP),
            P(),
            P(None, SP, TP),
            P(None, SP, TP),
            P(None, SP, TP),
            P(None, TP, SP),
            P(None, TP, None, None),
            P(SP),
        ),
        out_specs=P(SP, TP),
        check_vma=False,
    )
```

```python
import functools

import jax
import jax.numpy as jnp
from jax import lax
from jax.experimental import pallas as pl
from jax.experimental.pallas import tpu as pltpu
from jax.sharding import Mesh
from jax.sharding import PartitionSpec as P


HEAD_DIM = 64
WIN_ROWS = 8
WIN_COLS = 16
LAYERS = 3
GRID_W = 32
SP = ("z", "x")
TP = ("y", "c")
EPS = 1e-06
F32 = jnp.float32
BF16 = jnp.bfloat16
NT = (((1,), (1,)), ((), ()))


def turn(k):
    return [(i, (i + k) % 4) for i in range(4)]


def spread(a, axis):
    return [lax.ppermute(a, axis, turn(k)) for k in (1, 3, 2)]


def in_order(a, three):
    return [a, three[0], three[2], three[1]]


def gather_rows(a, axes):
    return lax.all_to_all(a, axes, 0, 0, tiled=True).reshape(1024, 512)


def after_this(a, done):
    return lax.optimization_barrier((a, done))[0]


def swap(a):
    return lax.ppermute(a, "c", [(0, 1), (1, 0)])


def from_before(a):
    return lax.ppermute(a, SP, [(i, i + 1) for i in range(15)])


def from_after(a):
    return lax.ppermute(a, SP, [(i + 1, i) for i in range(15)])


def behind(axis, k):
    return (lax.axis_index(axis) + (4 - k)) & 3


def ahead(axis, k):
    return (lax.axis_index(axis) + k) & 3


def call(body, outs, *args, scratch=(), **specs):
    return pl.pallas_call(
        body,
        out_shape=outs,
        **specs,
        scratch_shapes=list(scratch),
        compiler_params=pltpu.CompilerParams(vmem_limit_bytes=24 * 1024 * 1024),
    )(*args)


def shaped(*shape, dtype=BF16):
    return jax.ShapeDtypeStruct(shape, dtype)


def fetch(pairs, sems):
    copies = [pltpu.make_async_copy(a, b, sems.at[n]) for n, (a, b) in enumerate(pairs)]
    for copy in copies:
        copy.start()
    for copy in copies:
        copy.wait()


def pack_body(wq, wk, wv, wo, first, parts, sems):
    fetch([(w.at[0], parts.at[n]) for n, w in enumerate((wq, wk, wv, wo))], sems)
    whole = jnp.concatenate([parts[n] for n in range(4)], axis=1)
    for n in range(16):
        first[n] = whole


def many_body(wq, wk, wv, wo, bias, many, third, wide, parts, sems):
    pairs = [(w.at[1:3], parts.at[n]) for n, w in enumerate((wq, wk, wv, wo))]
    fetch(pairs, sems)
    third[...] = jnp.concatenate([parts[n, 1] for n in range(4)], axis=1)
    whole = jnp.concatenate([parts[n, 0] for n in range(4)], axis=1)
    for n in range(16):
        many[n] = whole
    wide[...] = jnp.zeros((8, 256), F32)
    for n in range(2 * LAYERS):
        for lag_row in range(WIN_ROWS):
            at = lag_row * GRID_W
            wide[n : n + 1, at : at + WIN_COLS] = bias[n // 2, n % 2, lag_row : lag_row + 1, :]


def line_body(p0, p1, p2, p3, many):
    for k, part in enumerate((p0, p1, p2, p3)):
        at = behind("x", k)
        for n in range(4):
            many[n, at] = part[...]


def table_body(wide, before, own, after, table):
    own_docs = own[128:144, 0:128].astype(F32)[0:1]
    query_docs = jnp.broadcast_to(own_docs, (128, 128)).T
    key_docs = jnp.concatenate(
        [before[128:144, 0:128].astype(F32)[0:1], own_docs, after[128:144, 0:128].astype(F32)[0:1]], axis=1
    )
    same = jnp.concatenate([query_docs] * 3, axis=1) == key_docs
    r = lax.broadcasted_iota(jnp.int32, (128, 384), 0)
    m = lax.broadcasted_iota(jnp.int32, (128, 384), 1)
    lag = (m >> 5) - (r >> 5)
    off = (m & 31) - (r & 31) + WIN_COLS // 2
    allowed = same & (lag >= 0) & (lag < WIN_ROWS) & (off >= 0) & (off < WIN_COLS)
    for n in range(2 * LAYERS):
        line = jnp.broadcast_to(wide[n : n + 1, :], (GRID_W, 256))
        line = pltpu.roll(line, 256 - WIN_COLS // 2, 1, stride=1, stride_axis=0)
        line = jnp.concatenate([line, jnp.zeros((GRID_W, 128), F32)], axis=1)
        block = jnp.concatenate(
            [line] + [pltpu.roll(line, 32 * q, 1) for q in range(1, 4)], axis=0
        )
        table[n] = jnp.where(allowed, block, -1e30)


def normed_heads(raw):
    values = raw.astype(BF16).astype(F32)
    squares = values * values
    low = lax.broadcasted_iota(jnp.int32, values.shape, 1) < HEAD_DIM
    first = jnp.sum(jnp.where(low, squares, 0.0), axis=1, keepdims=True)
    second = jnp.sum(jnp.where(low, 0.0, squares), axis=1, keepdims=True)
    scale = jnp.where(
        low,
        lax.rsqrt(first * (1.0 / HEAD_DIM) + EPS),
        lax.rsqrt(second * (1.0 / HEAD_DIM) + EPS),
    )
    return (values * scale).astype(BF16)


def finish_heads(acc, q, kv):
    q[...] = normed_heads(acc[:, 0:128])
    kv[:, 0:128] = normed_heads(acc[:, 128:256])
    kv[:, 128:256] = acc[:, 256:384].astype(BF16)


def heads_first_body(own, partner, gain, docs, weights, q, kv):
    c = lax.axis_index("c")
    total = jnp.zeros((128, 128), F32)
    for k in range(4):
        for part in (own, partner):
            values = part[k].astype(F32)
            total = total + values * values
    scale = lax.rsqrt(jnp.sum(total, axis=1, keepdims=True) * (1.0 / 1024) + EPS)
    acc = jnp.zeros((128, 384), F32)
    for k in range(4):
        for part, core in ((own, c), (partner, 1 - c)):
            block = behind("y", k) * 2 + core
            gains = gain[0:1, pl.ds(pl.multiple_of(block * 128, 128), 128)]
            normed = (part[k].astype(F32) * scale * gains).astype(BF16)
            rows = weights[pl.ds(pl.multiple_of(block * 128, 128), 128), 0:384]
            acc = acc + jnp.dot(normed, rows, preferred_element_type=F32)
    finish_heads(acc, q, kv.at[0:128])
    line = (docs[...] + 1).astype(F32).astype(BF16)
    kv[128:144, :] = jnp.broadcast_to(jnp.concatenate([line, line], axis=1), (16, 256))


def heads_pieces_body(x0, x1, x2, x3, gain, weights, q, kv, *, layer):
    pieces = [x[...].astype(F32) for x in (x0, x1, x2, x3)]
    total = sum(p * p for p in pieces)
    scale = lax.rsqrt(jnp.sum(total, axis=1, keepdims=True) * (1.0 / 1024) + EPS)
    acc = jnp.zeros((128, 384), F32)
    for k in range(4):
        block = behind("y", k)
        at = pl.ds(pl.multiple_of(block * 256, 256), 256)
        normed = (pieces[k] * scale * gain[layer : layer + 1, at]).astype(BF16)
        rows = weights[at, 0:384]
        acc = acc + jnp.dot(normed, rows, preferred_element_type=F32)
    finish_heads(acc, q, kv)


def attend(q, keys_values, table):
    queries = q[...]
    low = lax.broadcasted_iota(jnp.int32, (128, 128), 1) < HEAD_DIM
    results = []
    for h in range(2):
        mine = jnp.where(low if h == 0 else ~low, queries, jnp.zeros_like(queries))
        weights, total = [], 0.0
        for b, (keys, _) in enumerate(keys_values):
            scores = lax.dot_general(mine, keys, NT, preferred_element_type=F32)
            scores = scores * HEAD_DIM**-0.5 + table[h, :, b * 128 : (b + 1) * 128]
            grown = jnp.exp(scores)
            weights.append(grown)
            total = total + jnp.sum(grown, axis=1, keepdims=True)
        share = 1.0 / total
        out = 0.0
        for grown, (_, values) in zip(weights, keys_values):
            probs = (grown * share).astype(BF16)
            out = out + jnp.dot(probs, values, preferred_element_type=F32)
        results.append(out)
    return jnp.where(low, results[0], results[1]).astype(BF16)


def attend_scatter_body(q, before, own, after, table, weights, kept, s1, s2, s3, *, layer):
    parts = [(p[0:128, 0:128], p[0:128, 128:256]) for p in (before, own, after)]
    attended = attend(q, parts, table.at[2 * layer : 2 * layer + 2])
    for k, into in enumerate((kept, s1, s2, s3)):
        rows = weights[pl.ds(pl.multiple_of(ahead("y", k) * 256, 256), 256), 384:512]
        share = lax.dot_general(attended, rows, NT, preferred_element_type=F32)
        into[...] = share.astype(into.dtype)


def sum_body(kept, r1, r2, r3, out):
    out[...] = kept[...] + r1[...].astype(F32) + r2[...].astype(F32) + r3[...].astype(F32)


def pair_sum_body(mine, theirs, out):
    out[...] = (mine[...] + theirs[...]).astype(BF16)


def split_body(kept, r1, r2, r3, mine, theirs):
    c = lax.axis_index("c")
    for into, core in ((mine, c), (theirs, 1 - c)):
        at = pl.ds(pl.multiple_of(core * 128, 128), 128)
        into[...] = (
            kept[:, at] + r1[:, at].astype(F32) + r2[:, at].astype(F32) + r3[:, at].astype(F32)
        )


def scattered(body, *args):
    outs = [shaped(128, 256, dtype=F32)] + [shaped(128, 256)] * 3
    kept, s1, s2, s3 = call(body, outs, *args)
    r1 = lax.ppermute(s1, "y", turn(1))
    r3 = lax.ppermute(s3, "y", turn(3))
    r2 = lax.ppermute(s2, "y", turn(2))
    return kept, r1, r2, r3


def local(tokens, norm_gain, w_query, w_key, w_value, w_out, offset_bias, documents):
    hbm = pl.BlockSpec(memory_space=pltpu.HBM)
    held = [
        pltpu.with_memory_space_constraint(a, pltpu.HBM)
        for a in (w_query, w_key, w_value, jnp.swapaxes(w_out, 1, 2))
    ]
    first = call(
        pack_body, shaped(16, 64, 512), *held, in_specs=[hbm] * 4,
        scratch=[pltpu.VMEM((4, 64, 128), BF16), pltpu.SemaphoreType.DMA((4,))],
    )
    weights = gather_rows(first, SP)
    tokens_y = spread(tokens, "y")
    near_y = jnp.stack(in_order(tokens, tokens_y))
    many1, third, wide = call(
        many_body, [shaped(16, 64, 512), shaped(64, 512), shaped(8, 256, dtype=F32)],
        *held, offset_bias, in_specs=[hbm] * 4 + [pl.BlockSpec()],
        scratch=[pltpu.VMEM((4, 2, 64, 128), BF16), pltpu.SemaphoreType.DMA((4,))],
    )
    third_x = in_order(third, spread(third, "x"))
    near_partner = swap(after_this(near_y, many1))

    q, kv = call(
        heads_first_body, [shaped(128, 128), shaped(144, 256)],
        near_y, near_partner, norm_gain, documents.reshape(1, 128), weights,
    )
    many2 = call(line_body, shaped(4, 4, 64, 512), *third_x)
    for layer in range(LAYERS):
        after = from_after(kv)
        before = from_before(kv)
        if layer < 2:
            many, axes = ((many1, SP), (many2, "z"))[layer]
            next_weights = gather_rows(after_this(many, kv), axes)
        if layer == 0:
            table = call(table_body, shaped(6, 128, 384, dtype=F32), wide, before, kv, after)
        kept, r1, r2, r3 = scattered(
            functools.partial(attend_scatter_body, layer=layer),
            q, before, kv, after, table, weights,
        )
        if layer == 2:
            break
        if layer == 0:
            kept = after_this(kept, many2)
        half = call(sum_body, shaped(128, 256, dtype=F32), kept, r1, r2, r3)
        stream = call(pair_sum_body, shaped(128, 256), half, swap(half))
        weights = next_weights
        q, kv = call(
            functools.partial(heads_pieces_body, layer=layer + 1),
            [shaped(128, 128), shaped(128, 256)],
            *in_order(stream, spread(stream, "y")), norm_gain, weights,
        )
    mine, theirs = call(split_body, [shaped(128, 128, dtype=F32)] * 2, kept, r1, r2, r3)
    return call(pair_sum_body, shaped(128, 128), mine, swap(theirs))


def solution(mesh):
    torus = Mesh(mesh.devices.reshape(4, 4, 4, 2), ("z", "x", "y", "c"))
    return jax.shard_map(
        local,
        mesh=torus,
        in_specs=(
            P(SP, TP),
            P(),
            P(None, SP, TP),
            P(None, SP, TP),
            P(None, SP, TP),
            P(None, TP, SP),
            P(None, TP, None, None),
            P(SP),
        ),
        out_specs=P(SP, TP),
        check_vma=False,
    )
```

```python
import functools

import jax
import jax.numpy as jnp
from jax import lax
from jax.experimental import pallas as pl
from jax.experimental.pallas import tpu as pltpu
from jax.sharding import Mesh
from jax.sharding import PartitionSpec as P


HEAD_DIM = 64
WIN_ROWS = 8
WIN_COLS = 16
LAYERS = 3
GRID_W = 32
SP = ("z", "x")
TP = ("y", "c")
EPS = 1e-06
F32 = jnp.float32
BF16 = jnp.bfloat16
NT = (((1,), (1,)), ((), ()))


def turn(k):
    return [(i, (i + k) % 4) for i in range(4)]


def spread(a, axis):
    return [lax.ppermute(a, axis, turn(k)) for k in (1, 3, 2)]


def in_order(a, three):
    return [a, three[0], three[2], three[1]]


def gather_rows(a, axes):
    return lax.all_to_all(a, axes, 0, 0, tiled=True).reshape(1024, 512)


def after_this(a, done):
    return lax.optimization_barrier((a, done))[0]


def swap(a):
    return lax.ppermute(a, "c", [(0, 1), (1, 0)])


def from_before(a):
    return lax.ppermute(a, SP, [(i, i + 1) for i in range(15)])


def from_after(a):
    return lax.ppermute(a, SP, [(i + 1, i) for i in range(15)])


def behind(axis, k):
    return (lax.axis_index(axis) + (4 - k)) & 3


def ahead(axis, k):
    return (lax.axis_index(axis) + k) & 3


def call(body, outs, *args, scratch=(), **specs):
    return pl.pallas_call(
        body,
        out_shape=outs,
        **specs,
        scratch_shapes=list(scratch),
        compiler_params=pltpu.CompilerParams(vmem_limit_bytes=24 * 1024 * 1024),
    )(*args)


def shaped(*shape, dtype=BF16):
    return jax.ShapeDtypeStruct(shape, dtype)


def fetch(pairs, sems):
    copies = [pltpu.make_async_copy(a, b, sems.at[n]) for n, (a, b) in enumerate(pairs)]
    for copy in copies:
        copy.start()
    for copy in copies:
        copy.wait()


def pack_body(wq, wk, wv, wo, first, parts, sems):
    fetch([(w.at[0], parts.at[n]) for n, w in enumerate((wq, wk, wv, wo))], sems)
    whole = jnp.concatenate([parts[n] for n in range(4)], axis=1)
    for n in range(16):
        first[n] = whole


def many_body(wq, wk, wv, wo, bias, many, third, wide, parts, sems):
    pairs = [(w.at[1:3], parts.at[n]) for n, w in enumerate((wq, wk, wv, wo))]
    fetch(pairs, sems)
    third[...] = jnp.concatenate([parts[n, 1] for n in range(4)], axis=1)
    whole = jnp.concatenate([parts[n, 0] for n in range(4)], axis=1)
    for n in range(16):
        many[n] = whole
    wide[...] = jnp.zeros((8, 256), F32)
    for n in range(2 * LAYERS):
        for lag_row in range(WIN_ROWS):
            at = lag_row * GRID_W
            wide[n : n + 1, at : at + WIN_COLS] = bias[n // 2, n % 2, lag_row : lag_row + 1, :]


def line_body(p0, p1, p2, p3, many, sems):
    pairs = []
    for k, part in enumerate((p0, p1, p2, p3)):
        pairs += [(part, many.at[n, behind("x", k)]) for n in range(4)]
    fetch(pairs, sems)


def table_body(wide, table):
    r = lax.broadcasted_iota(jnp.int32, (128, 384), 0)
    m = lax.broadcasted_iota(jnp.int32, (128, 384), 1)
    lag = (m >> 5) - (r >> 5)
    off = (m & 31) - (r & 31) + WIN_COLS // 2
    allowed = (lag >= 0) & (lag < WIN_ROWS) & (off >= 0) & (off < WIN_COLS)
    for n in range(2 * LAYERS):
        line = jnp.broadcast_to(wide[n : n + 1, :], (GRID_W, 256))
        line = pltpu.roll(line, 256 - WIN_COLS // 2, 1, stride=1, stride_axis=0)
        line = jnp.concatenate([line, jnp.zeros((GRID_W, 128), F32)], axis=1)
        block = jnp.concatenate(
            [line] + [pltpu.roll(line, 32 * q, 1) for q in range(1, 4)], axis=0
        )
        table[n] = jnp.where(allowed, block, -1e30)


def normed_heads(raw):
    values = raw.astype(BF16).astype(F32)
    squares = values * values
    low = lax.broadcasted_iota(jnp.int32, values.shape, 1) < HEAD_DIM
    first = jnp.sum(jnp.where(low, squares, 0.0), axis=1, keepdims=True)
    second = jnp.sum(jnp.where(low, 0.0, squares), axis=1, keepdims=True)
    scale = jnp.where(
        low,
        lax.rsqrt(first * (1.0 / HEAD_DIM) + EPS),
        lax.rsqrt(second * (1.0 / HEAD_DIM) + EPS),
    )
    return (values * scale).astype(BF16)


def finish_heads(acc, q, kv):
    q[...] = normed_heads(acc[:, 0:128])
    kv[:, 0:128] = normed_heads(acc[:, 128:256])
    kv[:, 128:256] = acc[:, 256:384].astype(BF16)


def heads_first_body(own, partner, gain, docs, weights, q, kv):
    c = lax.axis_index("c")
    total = jnp.zeros((128, 128), F32)
    for k in range(4):
        for part in (own, partner):
            values = part[k].astype(F32)
            total = total + values * values
    scale = lax.rsqrt(jnp.sum(total, axis=1, keepdims=True) * (1.0 / 1024) + EPS)
    acc = jnp.zeros((128, 384), F32)
    for k in range(4):
        for part, core in ((own, c), (partner, 1 - c)):
            block = behind("y", k) * 2 + core
            gains = gain[0:1, pl.ds(pl.multiple_of(block * 128, 128), 128)]
            normed = (part[k].astype(F32) * scale * gains).astype(BF16)
            rows = weights[pl.ds(pl.multiple_of(block * 128, 128), 128), 0:384]
            acc = acc + jnp.dot(normed, rows, preferred_element_type=F32)
    finish_heads(acc, q, kv.at[0:128])
    line = (docs[...] + 1).astype(F32).astype(BF16)
    kv[128:144, :] = jnp.broadcast_to(jnp.concatenate([line, line], axis=1), (16, 256))


def heads_pieces_body(x0, x1, x2, x3, gain, weights, q, kv, *, layer):
    pieces = [x[...].astype(F32) for x in (x0, x1, x2, x3)]
    total = sum(p * p for p in pieces)
    scale = lax.rsqrt(jnp.sum(total, axis=1, keepdims=True) * (1.0 / 1024) + EPS)
    acc = jnp.zeros((128, 384), F32)
    for k in range(4):
        block = behind("y", k)
        at = pl.ds(pl.multiple_of(block * 256, 256), 256)
        normed = (pieces[k] * scale * gain[layer : layer + 1, at]).astype(BF16)
        rows = weights[at, 0:384]
        acc = acc + jnp.dot(normed, rows, preferred_element_type=F32)
    finish_heads(acc, q, kv)


def line_of(documents):
    return documents[128:144, 0:128].astype(F32)[0:1]


def attend(q, keys_values, table, documents):
    queries = q[...]
    query_docs = jnp.broadcast_to(line_of(documents[1]), (128, 128)).T
    same = [query_docs == line_of(d) for d in documents]
    low = lax.broadcasted_iota(jnp.int32, (128, 128), 1) < HEAD_DIM
    results = []
    for h in range(2):
        mine = jnp.where(low if h == 0 else ~low, queries, jnp.zeros_like(queries))
        weights, total = [], 0.0
        for b, (keys, _) in enumerate(keys_values):
            scores = lax.dot_general(mine, keys, NT, preferred_element_type=F32)
            scores = scores * HEAD_DIM**-0.5 + table[h, :, b * 128 : (b + 1) * 128]
            grown = jnp.where(same[b], jnp.exp(scores), 0.0)
            weights.append(grown)
            total = total + jnp.sum(grown, axis=1, keepdims=True)
        share = 1.0 / total
        out = 0.0
        for grown, (_, values) in zip(weights, keys_values):
            probs = (grown * share).astype(BF16)
            out = out + jnp.dot(probs, values, preferred_element_type=F32)
        results.append(out)
    return jnp.where(low, results[0], results[1]).astype(BF16)


def attend_scatter_body(
    q, before, own, after, doc_before, doc_own, doc_after, table, weights,
    kept, s1, s2, s3, *, layer,
):
    parts = [(p[0:128, 0:128], p[0:128, 128:256]) for p in (before, own, after)]
    table = table.at[2 * layer : 2 * layer + 2]
    attended = attend(q, parts, table, (doc_before, doc_own, doc_after))
    for k, into in enumerate((kept, s1, s2, s3)):
        rows = weights[pl.ds(pl.multiple_of(ahead("y", k) * 256, 256), 256), 384:512]
        share = lax.dot_general(attended, rows, NT, preferred_element_type=F32)
        into[...] = share.astype(into.dtype)


def sum_body(kept, r1, r2, r3, out):
    out[...] = kept[...] + r1[...].astype(F32) + r2[...].astype(F32) + r3[...].astype(F32)


def pair_sum_body(mine, theirs, out):
    out[...] = (mine[...] + theirs[...]).astype(BF16)


def split_body(kept, r1, r2, r3, mine, theirs):
    c = lax.axis_index("c")
    for into, core in ((mine, c), (theirs, 1 - c)):
        at = pl.ds(pl.multiple_of(core * 128, 128), 128)
        into[...] = (
            kept[:, at] + r1[:, at].astype(F32) + r2[:, at].astype(F32) + r3[:, at].astype(F32)
        )


def scattered(body, *args):
    outs = [shaped(128, 256, dtype=F32)] + [shaped(128, 256)] * 3
    kept, s1, s2, s3 = call(body, outs, *args)
    r1 = lax.ppermute(s1, "y", turn(1))
    r3 = lax.ppermute(s3, "y", turn(3))
    r2 = lax.ppermute(s2, "y", turn(2))
    return kept, r1, r2, r3


def local(tokens, norm_gain, w_query, w_key, w_value, w_out, offset_bias, documents):
    hbm = pl.BlockSpec(memory_space=pltpu.HBM)
    held = [
        pltpu.with_memory_space_constraint(a, pltpu.HBM)
        for a in (w_query, w_key, w_value, jnp.swapaxes(w_out, 1, 2))
    ]
    first = call(
        pack_body, shaped(16, 64, 512), *held, in_specs=[hbm] * 4,
        scratch=[pltpu.VMEM((4, 64, 128), BF16), pltpu.SemaphoreType.DMA((4,))],
    )
    weights = gather_rows(first, SP)
    tokens_y = spread(tokens, "y")
    near_y = jnp.stack(in_order(tokens, tokens_y))
    many1, third, wide = call(
        many_body, [shaped(16, 64, 512), shaped(64, 512), shaped(8, 256, dtype=F32)],
        *held, offset_bias, in_specs=[hbm] * 4 + [pl.BlockSpec()],
        scratch=[pltpu.VMEM((4, 2, 64, 128), BF16), pltpu.SemaphoreType.DMA((4,))],
    )
    third_x = in_order(third, spread(third, "x"))
    table = call(table_body, shaped(6, 128, 384, dtype=F32), wide)
    near_partner = swap(after_this(near_y, (many1, table)))

    q, kv = call(
        heads_first_body, [shaped(128, 128), shaped(144, 256)],
        near_y, near_partner, norm_gain, documents.reshape(1, 128), weights,
    )
    many2 = call(
        line_body, pltpu.HBM((4, 4, 64, 512), BF16), *third_x, out_specs=hbm,
        scratch=[pltpu.SemaphoreType.DMA((16,))],
    )
    for layer in range(LAYERS):
        after = from_after(kv)
        before = from_before(kv)
        if layer < 2:
            many, axes = ((many1, SP), (many2, "z"))[layer]
            next_weights = gather_rows(after_this(many, kv), axes)
        if layer == 0:
            docs = (before, kv, after)
        kept, r1, r2, r3 = scattered(
            functools.partial(attend_scatter_body, layer=layer),
            q, before, kv, after, *docs, table, weights,
        )
        if layer == 2:
            break
        if layer == 0:
            kept = after_this(kept, many2)
        half = call(sum_body, shaped(128, 256, dtype=F32), kept, r1, r2, r3)
        stream = call(pair_sum_body, shaped(128, 256), half, swap(half))
        weights = next_weights
        q, kv = call(
            functools.partial(heads_pieces_body, layer=layer + 1),
            [shaped(128, 128), shaped(128, 256)],
            *in_order(stream, spread(stream, "y")), norm_gain, weights,
        )
    mine, theirs = call(split_body, [shaped(128, 128, dtype=F32)] * 2, kept, r1, r2, r3)
    return call(pair_sum_body, shaped(128, 128), mine, swap(theirs))


def solution(mesh):
    torus = Mesh(mesh.devices.reshape(4, 4, 4, 2), ("z", "x", "y", "c"))
    return jax.shard_map(
        local,
        mesh=torus,
        in_specs=(
            P(SP, TP),
            P(),
            P(None, SP, TP),
            P(None, SP, TP),
            P(None, SP, TP),
            P(None, TP, SP),
            P(None, TP, None, None),
            P(SP),
        ),
        out_specs=P(SP, TP),
        check_vma=False,
    )
```

```python
import functools

import jax
import jax.numpy as jnp
from jax import lax
from jax.experimental import pallas as pl
from jax.experimental.pallas import tpu as pltpu
from jax.sharding import Mesh
from jax.sharding import PartitionSpec as P


HEAD_DIM = 64
WIN_ROWS = 8
WIN_COLS = 16
LAYERS = 3
GRID_W = 32
SP = ("z", "x")
TP = ("y", "c")
EPS = 1e-06
F32 = jnp.float32
BF16 = jnp.bfloat16
NT = (((1,), (1,)), ((), ()))


def turn(k):
    return [(i, (i + k) % 4) for i in range(4)]


def spread(a, axis):
    return [lax.ppermute(a, axis, turn(k)) for k in (1, 3, 2)]


def in_order(a, three):
    return [a, three[0], three[2], three[1]]


def gather_rows(a, axes):
    return lax.all_to_all(a, axes, 0, 0, tiled=True).reshape(1024, 512)


def after_this(a, done):
    return lax.optimization_barrier((a, done))[0]


def swap(a):
    return lax.ppermute(a, "c", [(0, 1), (1, 0)])


def from_before(a):
    return lax.ppermute(a, SP, [(i, i + 1) for i in range(15)])


def from_after(a):
    return lax.ppermute(a, SP, [(i + 1, i) for i in range(15)])


def behind(axis, k):
    return (lax.axis_index(axis) + (4 - k)) & 3


def ahead(axis, k):
    return (lax.axis_index(axis) + k) & 3


def call(body, outs, *args, scratch=(), **specs):
    return pl.pallas_call(
        body,
        out_shape=outs,
        **specs,
        scratch_shapes=list(scratch),
        compiler_params=pltpu.CompilerParams(vmem_limit_bytes=24 * 1024 * 1024),
    )(*args)


def shaped(*shape, dtype=BF16):
    return jax.ShapeDtypeStruct(shape, dtype)


def fetch(pairs, sems):
    copies = [pltpu.make_async_copy(a, b, sems.at[n]) for n, (a, b) in enumerate(pairs)]
    for copy in copies:
        copy.start()
    for copy in copies:
        copy.wait()


def pack_body(wq, wk, wv, wo, first, parts, sems):
    fetch([(w.at[0], parts.at[n]) for n, w in enumerate((wq, wk, wv, wo))], sems)
    whole = jnp.concatenate([parts[n] for n in range(4)], axis=1)
    for n in range(16):
        first[n] = whole


def many_body(wq, wk, wv, wo, bias, many, third, wide, parts, sems):
    pairs = [(w.at[1:3], parts.at[n]) for n, w in enumerate((wq, wk, wv, wo))]
    fetch(pairs, sems)
    third[...] = jnp.concatenate([parts[n, 1] for n in range(4)], axis=1)
    whole = jnp.concatenate([parts[n, 0] for n in range(4)], axis=1)
    for n in range(16):
        many[n] = whole
    wide[...] = jnp.zeros((8, 256), F32)
    for n in range(2 * LAYERS):
        for lag_row in range(WIN_ROWS):
            at = lag_row * GRID_W
            wide[n : n + 1, at : at + WIN_COLS] = bias[n // 2, n % 2, lag_row : lag_row + 1, :]


def line_body(p0, p1, p2, p3, many):
    for k, part in enumerate((p0, p1, p2, p3)):
        at = behind("x", k)
        for n in range(4):
            many[n, at] = part[...]


def table_body(wide, table):
    r = lax.broadcasted_iota(jnp.int32, (128, 384), 0)
    m = lax.broadcasted_iota(jnp.int32, (128, 384), 1)
    lag = (m >> 5) - (r >> 5)
    off = (m & 31) - (r & 31) + WIN_COLS // 2
    allowed = (lag >= 0) & (lag < WIN_ROWS) & (off >= 0) & (off < WIN_COLS)
    for n in range(2 * LAYERS):
        line = jnp.broadcast_to(wide[n : n + 1, :], (GRID_W, 256))
        line = pltpu.roll(line, 256 - WIN_COLS // 2, 1, stride=1, stride_axis=0)
        line = jnp.concatenate([line, jnp.zeros((GRID_W, 128), F32)], axis=1)
        block = jnp.concatenate(
            [line] + [pltpu.roll(line, 32 * q, 1) for q in range(1, 4)], axis=0
        )
        table[n] = jnp.where(allowed, block, -1e30)


def normed_heads(raw):
    values = raw.astype(BF16).astype(F32)
    squares = values * values
    low = lax.broadcasted_iota(jnp.int32, values.shape, 1) < HEAD_DIM
    first = jnp.sum(jnp.where(low, squares, 0.0), axis=1, keepdims=True)
    second = jnp.sum(jnp.where(low, 0.0, squares), axis=1, keepdims=True)
    scale = jnp.where(
        low,
        lax.rsqrt(first * (1.0 / HEAD_DIM) + EPS),
        lax.rsqrt(second * (1.0 / HEAD_DIM) + EPS),
    )
    return (values * scale).astype(BF16)


def finish_heads(acc, q, kv):
    q[...] = normed_heads(acc[:, 0:128])
    kv[:, 0:128] = normed_heads(acc[:, 128:256])
    kv[:, 128:256] = acc[:, 256:384].astype(BF16)


def heads_first_body(own, partner, gain, docs, weights, q, kv):
    c = lax.axis_index("c")
    total = jnp.zeros((128, 128), F32)
    for k in range(4):
        for part in (own, partner):
            values = part[k].astype(F32)
            total = total + values * values
    scale = lax.rsqrt(jnp.sum(total, axis=1, keepdims=True) * (1.0 / 1024) + EPS)
    acc = jnp.zeros((128, 384), F32)
    for k in range(4):
        for part, core in ((own, c), (partner, 1 - c)):
            block = behind("y", k) * 2 + core
            gains = gain[0:1, pl.ds(pl.multiple_of(block * 128, 128), 128)]
            normed = (part[k].astype(F32) * scale * gains).astype(BF16)
            rows = weights[pl.ds(pl.multiple_of(block * 128, 128), 128), 0:384]
            acc = acc + jnp.dot(normed, rows, preferred_element_type=F32)
    finish_heads(acc, q, kv.at[0:128])
    line = (docs[...] + 1).astype(F32).astype(BF16)
    kv[128:144, :] = jnp.broadcast_to(jnp.concatenate([line, line], axis=1), (16, 256))


def heads_pieces_body(x0, x1, x2, x3, gain, weights, q, kv, *, layer):
    pieces = [x[...].astype(F32) for x in (x0, x1, x2, x3)]
    total = sum(p * p for p in pieces)
    scale = lax.rsqrt(jnp.sum(total, axis=1, keepdims=True) * (1.0 / 1024) + EPS)
    acc = jnp.zeros((128, 384), F32)
    for k in range(4):
        block = behind("y", k)
        at = pl.ds(pl.multiple_of(block * 256, 256), 256)
        normed = (pieces[k] * scale * gain[layer : layer + 1, at]).astype(BF16)
        rows = weights[at, 0:384]
        acc = acc + jnp.dot(normed, rows, preferred_element_type=F32)
    finish_heads(acc, q, kv)


def line_of(documents):
    return documents[128:144, 0:128].astype(F32)[0:1]


def attend(q, keys_values, table, documents):
    queries = q[...]
    query_docs = jnp.broadcast_to(line_of(documents[1]), (128, 128)).T
    same = [query_docs == line_of(d) for d in documents]
    low = lax.broadcasted_iota(jnp.int32, (128, 128), 1) < HEAD_DIM
    results = []
    for h in range(2):
        mine = jnp.where(low if h == 0 else ~low, queries, jnp.zeros_like(queries))
        weights, total = [], 0.0
        for b, (keys, _) in enumerate(keys_values):
            scores = lax.dot_general(mine, keys, NT, preferred_element_type=F32)
            scores = scores * HEAD_DIM**-0.5 + table[h, :, b * 128 : (b + 1) * 128]
            grown = jnp.where(same[b], jnp.exp(scores), 0.0)
            weights.append(grown)
            total = total + jnp.sum(grown, axis=1, keepdims=True)
        share = 1.0 / total
        out = 0.0
        for grown, (_, values) in zip(weights, keys_values):
            probs = (grown * share).astype(BF16)
            out = out + jnp.dot(probs, values, preferred_element_type=F32)
        results.append(out)
    return jnp.where(low, results[0], results[1]).astype(BF16)


def attend_scatter_body(
    q, before, own, after, doc_before, doc_own, doc_after, table, weights,
    kept, s1, s2, s3, *, layer,
):
    parts = [(p[0:128, 0:128], p[0:128, 128:256]) for p in (before, own, after)]
    table = table.at[2 * layer : 2 * layer + 2]
    attended = attend(q, parts, table, (doc_before, doc_own, doc_after))
    for k, into in enumerate((kept, s1, s2, s3)):
        rows = weights[pl.ds(pl.multiple_of(ahead("y", k) * 256, 256), 256), 384:512]
        share = lax.dot_general(attended, rows, NT, preferred_element_type=F32)
        into[...] = share.astype(into.dtype)


def sum_body(kept, r1, r2, r3, out):
    out[...] = kept[...] + r1[...].astype(F32) + r2[...].astype(F32) + r3[...].astype(F32)


def pair_sum_body(mine, theirs, out):
    out[...] = (mine[...] + theirs[...]).astype(BF16)


def split_body(kept, r1, r2, r3, mine, theirs):
    c = lax.axis_index("c")
    for into, core in ((mine, c), (theirs, 1 - c)):
        at = pl.ds(pl.multiple_of(core * 128, 128), 128)
        into[...] = (
            kept[:, at] + r1[:, at].astype(F32) + r2[:, at].astype(F32) + r3[:, at].astype(F32)
        )


def scattered(body, *args):
    outs = [shaped(128, 256, dtype=F32)] + [shaped(128, 256)] * 3
    kept, s1, s2, s3 = call(body, outs, *args)
    r1 = lax.ppermute(s1, "y", turn(1))
    r3 = lax.ppermute(s3, "y", turn(3))
    r2 = lax.ppermute(s2, "y", turn(2))
    return kept, r1, r2, r3


def local(tokens, norm_gain, w_query, w_key, w_value, w_out, offset_bias, documents):
    hbm = pl.BlockSpec(memory_space=pltpu.HBM)
    held = [
        pltpu.with_memory_space_constraint(a, pltpu.HBM)
        for a in (w_query, w_key, w_value, jnp.swapaxes(w_out, 1, 2))
    ]
    first = call(
        pack_body, shaped(16, 64, 512), *held, in_specs=[hbm] * 4,
        scratch=[pltpu.VMEM((4, 64, 128), BF16), pltpu.SemaphoreType.DMA((4,))],
    )
    weights = gather_rows(first, SP)
    tokens_y = spread(tokens, "y")
    near_y = jnp.stack(in_order(tokens, tokens_y))
    many1, third, wide = call(
        many_body, [shaped(16, 64, 512), shaped(64, 512), shaped(8, 256, dtype=F32)],
        *held, offset_bias, in_specs=[hbm] * 4 + [pl.BlockSpec()],
        scratch=[pltpu.VMEM((4, 2, 64, 128), BF16), pltpu.SemaphoreType.DMA((4,))],
    )
    third_x = in_order(third, spread(third, "x"))
    table = call(table_body, shaped(6, 128, 384, dtype=F32), wide)
    near_partner = swap(after_this(near_y, (many1, table)))

    q, kv = call(
        heads_first_body, [shaped(128, 128), shaped(144, 256)],
        near_y, near_partner, norm_gain, documents.reshape(1, 128), weights,
    )
    many2 = call(line_body, shaped(4, 4, 64, 512), *third_x)
    for layer in range(LAYERS):
        after = from_after(kv)
        before = from_before(kv)
        if layer < 2:
            many, axes = ((many1, SP), (many2, "z"))[layer]
            next_weights = gather_rows(after_this(many, kv), axes)
        if layer == 0:
            docs = (before, kv, after)
        kept, r1, r2, r3 = scattered(
            functools.partial(attend_scatter_body, layer=layer),
            q, before, kv, after, *docs, table, weights,
        )
        if layer == 2:
            break
        if layer == 0:
            kept = after_this(kept, many2)
        half = call(sum_body, shaped(128, 256, dtype=F32), kept, r1, r2, r3)
        stream = call(pair_sum_body, shaped(128, 256), half, swap(half))
        weights = next_weights
        q, kv = call(
            functools.partial(heads_pieces_body, layer=layer + 1),
            [shaped(128, 128), shaped(128, 256)],
            *in_order(stream, spread(stream, "y")), norm_gain, weights,
        )
    mine, theirs = call(split_body, [shaped(128, 128, dtype=F32)] * 2, kept, r1, r2, r3)
    return call(pair_sum_body, shaped(128, 128), mine, swap(theirs))


def solution(mesh):
    torus = Mesh(mesh.devices.reshape(4, 4, 4, 2), ("z", "x", "y", "c"))
    return jax.shard_map(
        local,
        mesh=torus,
        in_specs=(
            P(SP, TP),
            P(),
            P(None, SP, TP),
            P(None, SP, TP),
            P(None, SP, TP),
            P(None, TP, SP),
            P(None, TP, None, None),
            P(SP),
        ),
        out_specs=P(SP, TP),
        check_vma=False,
    )
```

```python
import functools

import jax
import jax.numpy as jnp
from jax import lax
from jax.experimental import pallas as pl
from jax.experimental.pallas import tpu as pltpu
from jax.sharding import Mesh
from jax.sharding import PartitionSpec as P


HEAD_DIM = 64
WIN_ROWS = 8
WIN_COLS = 16
LAYERS = 3
GRID_W = 32
SP = ("z", "x")
TP = ("y", "c")
EPS = 1e-06
F32 = jnp.float32
BF16 = jnp.bfloat16
NT = (((1,), (1,)), ((), ()))


def turn(k):
    return [(i, (i + k) % 4) for i in range(4)]


def spread(a, axis):
    return [lax.ppermute(a, axis, turn(k)) for k in (1, 3, 2)]


def in_order(a, three):
    return [a, three[0], three[2], three[1]]


def gather_rows(a, axes):
    return lax.all_to_all(a, axes, 0, 0, tiled=True).reshape(1024, 512)


def after_this(a, done):
    return lax.optimization_barrier((a, done))[0]


def swap(a):
    return lax.ppermute(a, "c", [(0, 1), (1, 0)])


def from_before(a):
    return lax.ppermute(a, SP, [(i, i + 1) for i in range(15)])


def from_after(a):
    return lax.ppermute(a, SP, [(i + 1, i) for i in range(15)])


def behind(axis, k):
    return (lax.axis_index(axis) + (4 - k)) & 3


def ahead(axis, k):
    return (lax.axis_index(axis) + k) & 3


def call(body, outs, *args, scratch=(), **specs):
    return pl.pallas_call(
        body,
        out_shape=outs,
        **specs,
        scratch_shapes=list(scratch),
        compiler_params=pltpu.CompilerParams(vmem_limit_bytes=24 * 1024 * 1024),
    )(*args)


def shaped(*shape, dtype=BF16):
    return jax.ShapeDtypeStruct(shape, dtype)


def fetch(pairs, sems):
    copies = [pltpu.make_async_copy(a, b, sems.at[n]) for n, (a, b) in enumerate(pairs)]
    for copy in copies:
        copy.start()
    for copy in copies:
        copy.wait()


def pack_body(wq, wk, wv, wo, first, parts, sems):
    fetch([(w.at[0], parts.at[n]) for n, w in enumerate((wq, wk, wv, wo))], sems)
    whole = jnp.concatenate([parts[n] for n in range(4)], axis=1)
    for n in range(16):
        first[n] = whole


def many_body(wq, wk, wv, wo, bias, rest, wide, parts, sems):
    pairs = [(w.at[1:3], parts.at[n]) for n, w in enumerate((wq, wk, wv, wo))]
    fetch(pairs, sems)
    for layer in range(2):
        rest[layer] = jnp.concatenate([parts[n, layer] for n in range(4)], axis=1)
    wide[...] = jnp.zeros((8, 256), F32)
    for n in range(2 * LAYERS):
        for lag_row in range(WIN_ROWS):
            at = lag_row * GRID_W
            wide[n : n + 1, at : at + WIN_COLS] = bias[n // 2, n % 2, lag_row : lag_row + 1, :]


def line_body(p0, p1, p2, p3, many, *, layer):
    for k, part in enumerate((p0, p1, p2, p3)):
        at = behind("x", k)
        for n in range(4):
            many[n, at] = part[layer]


def table_body(wide, before, own, after, table):
    own_docs = own[128:144, 0:128].astype(F32)[0:1]
    query_docs = jnp.broadcast_to(own_docs, (128, 128)).T
    key_docs = jnp.concatenate(
        [before[128:144, 0:128].astype(F32)[0:1], own_docs, after[128:144, 0:128].astype(F32)[0:1]], axis=1
    )
    same = jnp.concatenate([query_docs] * 3, axis=1) == key_docs
    r = lax.broadcasted_iota(jnp.int32, (128, 384), 0)
    m = lax.broadcasted_iota(jnp.int32, (128, 384), 1)
    lag = (m >> 5) - (r >> 5)
    off = (m & 31) - (r & 31) + WIN_COLS // 2
    allowed = same & (lag >= 0) & (lag < WIN_ROWS) & (off >= 0) & (off < WIN_COLS)
    for n in range(2 * LAYERS):
        line = jnp.broadcast_to(wide[n : n + 1, :], (GRID_W, 256))
        line = pltpu.roll(line, 256 - WIN_COLS // 2, 1, stride=1, stride_axis=0)
        line = jnp.concatenate([line, jnp.zeros((GRID_W, 128), F32)], axis=1)
        block = jnp.concatenate(
            [line] + [pltpu.roll(line, 32 * q, 1) for q in range(1, 4)], axis=0
        )
        table[n] = jnp.where(allowed, block, -1e30)


def normed_heads(raw):
    values = raw.astype(BF16).astype(F32)
    squares = values * values
    low = lax.broadcasted_iota(jnp.int32, values.shape, 1) < HEAD_DIM
    first = jnp.sum(jnp.where(low, squares, 0.0), axis=1, keepdims=True)
    second = jnp.sum(jnp.where(low, 0.0, squares), axis=1, keepdims=True)
    scale = jnp.where(
        low,
        lax.rsqrt(first * (1.0 / HEAD_DIM) + EPS),
        lax.rsqrt(second * (1.0 / HEAD_DIM) + EPS),
    )
    return (values * scale).astype(BF16)


def finish_heads(acc, q, kv):
    q[...] = normed_heads(acc[:, 0:128])
    kv[:, 0:128] = normed_heads(acc[:, 128:256])
    kv[:, 128:256] = acc[:, 256:384].astype(BF16)


def heads_first_body(own, partner, gain, docs, weights, q, kv):
    c = lax.axis_index("c")
    total = jnp.zeros((128, 128), F32)
    for k in range(4):
        for part in (own, partner):
            values = part[k].astype(F32)
            total = total + values * values
    scale = lax.rsqrt(jnp.sum(total, axis=1, keepdims=True) * (1.0 / 1024) + EPS)
    acc = jnp.zeros((128, 384), F32)
    for k in range(4):
        for part, core in ((own, c), (partner, 1 - c)):
            block = behind("y", k) * 2 + core
            gains = gain[0:1, pl.ds(pl.multiple_of(block * 128, 128), 128)]
            normed = (part[k].astype(F32) * scale * gains).astype(BF16)
            rows = weights[pl.ds(pl.multiple_of(block * 128, 128), 128), 0:384]
            acc = acc + jnp.dot(normed, rows, preferred_element_type=F32)
    finish_heads(acc, q, kv.at[0:128])
    line = (docs[...] + 1).astype(F32).astype(BF16)
    kv[128:144, :] = jnp.broadcast_to(jnp.concatenate([line, line], axis=1), (16, 256))


def heads_pieces_body(x0, x1, x2, x3, gain, weights, q, kv, *, layer):
    pieces = [x[...].astype(F32) for x in (x0, x1, x2, x3)]
    total = sum(p * p for p in pieces)
    scale = lax.rsqrt(jnp.sum(total, axis=1, keepdims=True) * (1.0 / 1024) + EPS)
    acc = jnp.zeros((128, 384), F32)
    for k in range(4):
        block = behind("y", k)
        at = pl.ds(pl.multiple_of(block * 256, 256), 256)
        normed = (pieces[k] * scale * gain[layer : layer + 1, at]).astype(BF16)
        rows = weights[at, 0:384]
        acc = acc + jnp.dot(normed, rows, preferred_element_type=F32)
    finish_heads(acc, q, kv)


def attend(q, keys_values, table):
    queries = q[...]
    low = lax.broadcasted_iota(jnp.int32, (128, 128), 1) < HEAD_DIM
    results = []
    for h in range(2):
        mine = jnp.where(low if h == 0 else ~low, queries, jnp.zeros_like(queries))
        weights, total = [], 0.0
        for b, (keys, _) in enumerate(keys_values):
            scores = lax.dot_general(mine, keys, NT, preferred_element_type=F32)
            scores = scores * HEAD_DIM**-0.5 + table[h, :, b * 128 : (b + 1) * 128]
            grown = jnp.exp(scores)
            weights.append(grown)
            total = total + jnp.sum(grown, axis=1, keepdims=True)
        share = 1.0 / total
        out = 0.0
        for grown, (_, values) in zip(weights, keys_values):
            probs = (grown * share).astype(BF16)
            out = out + jnp.dot(probs, values, preferred_element_type=F32)
        results.append(out)
    return jnp.where(low, results[0], results[1]).astype(BF16)


def attend_scatter_body(q, before, own, after, table, weights, kept, s1, s2, s3, *, layer):
    parts = [(p[0:128, 0:128], p[0:128, 128:256]) for p in (before, own, after)]
    attended = attend(q, parts, table.at[2 * layer : 2 * layer + 2])
    for k, into in enumerate((kept, s1, s2, s3)):
        rows = weights[pl.ds(pl.multiple_of(ahead("y", k) * 256, 256), 256), 384:512]
        share = lax.dot_general(attended, rows, NT, preferred_element_type=F32)
        into[...] = share.astype(into.dtype)


def sum_body(kept, r1, r2, r3, out):
    out[...] = kept[...] + r1[...].astype(F32) + r2[...].astype(F32) + r3[...].astype(F32)


def pair_sum_body(mine, theirs, out):
    out[...] = (mine[...] + theirs[...]).astype(BF16)


def split_body(kept, r1, r2, r3, mine, theirs):
    c = lax.axis_index("c")
    for into, core in ((mine, c), (theirs, 1 - c)):
        at = pl.ds(pl.multiple_of(core * 128, 128), 128)
        into[...] = (
            kept[:, at] + r1[:, at].astype(F32) + r2[:, at].astype(F32) + r3[:, at].astype(F32)
        )


def scattered(body, *args):
    outs = [shaped(128, 256, dtype=F32)] + [shaped(128, 256)] * 3
    kept, s1, s2, s3 = call(body, outs, *args)
    r1 = lax.ppermute(s1, "y", turn(1))
    r3 = lax.ppermute(s3, "y", turn(3))
    r2 = lax.ppermute(s2, "y", turn(2))
    return kept, r1, r2, r3


def local(tokens, norm_gain, w_query, w_key, w_value, w_out, offset_bias, documents):
    hbm = pl.BlockSpec(memory_space=pltpu.HBM)
    held = [
        pltpu.with_memory_space_constraint(a, pltpu.HBM)
        for a in (w_query, w_key, w_value, jnp.swapaxes(w_out, 1, 2))
    ]
    first = call(
        pack_body, shaped(16, 64, 512), *held, in_specs=[hbm] * 4,
        scratch=[pltpu.VMEM((4, 64, 128), BF16), pltpu.SemaphoreType.DMA((4,))],
    )
    weights = gather_rows(first, SP)
    tokens_y = spread(tokens, "y")
    near_y = jnp.stack(in_order(tokens, tokens_y))
    rest, wide = call(
        many_body, [shaped(2, 64, 512), shaped(8, 256, dtype=F32)],
        *held, offset_bias, in_specs=[hbm] * 4 + [pl.BlockSpec()],
        scratch=[pltpu.VMEM((4, 2, 64, 128), BF16), pltpu.SemaphoreType.DMA((4,))],
    )
    third_x = in_order(rest, spread(rest, "x"))
    near_partner = swap(after_this(near_y, wide))

    q, kv = call(
        heads_first_body, [shaped(128, 128), shaped(144, 256)],
        near_y, near_partner, norm_gain, documents.reshape(1, 128), weights,
    )
    many1, many2 = [
        call(functools.partial(line_body, layer=n), shaped(4, 4, 64, 512), *third_x)
        for n in range(2)
    ]
    for layer in range(LAYERS):
        after = from_after(kv)
        before = from_before(kv)
        if layer < 2:
            next_weights = gather_rows(after_this((many1, many2)[layer], kv), "z")
        if layer == 0:
            table = call(table_body, shaped(6, 128, 384, dtype=F32), wide, before, kv, after)
        kept, r1, r2, r3 = scattered(
            functools.partial(attend_scatter_body, layer=layer),
            q, before, kv, after, table, weights,
        )
        if layer == 2:
            break
        if layer == 0:
            kept = after_this(kept, many2)
        half = call(sum_body, shaped(128, 256, dtype=F32), kept, r1, r2, r3)
        stream = call(pair_sum_body, shaped(128, 256), half, swap(half))
        weights = next_weights
        q, kv = call(
            functools.partial(heads_pieces_body, layer=layer + 1),
            [shaped(128, 128), shaped(128, 256)],
            *in_order(stream, spread(stream, "y")), norm_gain, weights,
        )
    mine, theirs = call(split_body, [shaped(128, 128, dtype=F32)] * 2, kept, r1, r2, r3)
    return call(pair_sum_body, shaped(128, 128), mine, swap(theirs))


def solution(mesh):
    torus = Mesh(mesh.devices.reshape(4, 4, 4, 2), ("z", "x", "y", "c"))
    return jax.shard_map(
        local,
        mesh=torus,
        in_specs=(
            P(SP, TP),
            P(),
            P(None, SP, TP),
            P(None, SP, TP),
            P(None, SP, TP),
            P(None, TP, SP),
            P(None, TP, None, None),
            P(SP),
        ),
        out_specs=P(SP, TP),
        check_vma=False,
    )
```

```python
import functools

import jax
import jax.numpy as jnp
from jax import lax
from jax.experimental import pallas as pl
from jax.experimental.pallas import tpu as pltpu
from jax.sharding import Mesh
from jax.sharding import PartitionSpec as P


HEAD_DIM = 64
WIN_ROWS = 8
WIN_COLS = 16
LAYERS = 3
GRID_W = 32
SP = ("z", "x")
TP = ("y", "c")
EPS = 1e-06
F32 = jnp.float32
BF16 = jnp.bfloat16
NT = (((1,), (1,)), ((), ()))


def turn(k):
    return [(i, (i + k) % 4) for i in range(4)]


def spread(a, axis):
    return [lax.ppermute(a, axis, turn(k)) for k in (1, 3, 2)]


def in_order(a, three):
    return [a, three[0], three[2], three[1]]


def gather_rows(a, axes):
    return lax.all_to_all(a, axes, 0, 0, tiled=True).reshape(1024, 512)


def after_this(a, done):
    return lax.optimization_barrier((a, done))[0]


def swap(a):
    return lax.ppermute(a, "c", [(0, 1), (1, 0)])


def from_before(a):
    return lax.ppermute(a, SP, [(i, i + 1) for i in range(15)])


def from_after(a):
    return lax.ppermute(a, SP, [(i + 1, i) for i in range(15)])


def behind(axis, k):
    return (lax.axis_index(axis) + (4 - k)) & 3


def ahead(axis, k):
    return (lax.axis_index(axis) + k) & 3


def call(body, outs, *args, scratch=(), **specs):
    return pl.pallas_call(
        body,
        out_shape=outs,
        **specs,
        scratch_shapes=list(scratch),
        compiler_params=pltpu.CompilerParams(vmem_limit_bytes=24 * 1024 * 1024),
    )(*args)


def shaped(*shape, dtype=BF16):
    return jax.ShapeDtypeStruct(shape, dtype)


def fetch(pairs, sems):
    copies = [pltpu.make_async_copy(a, b, sems.at[n]) for n, (a, b) in enumerate(pairs)]
    for copy in copies:
        copy.start()
    for copy in copies:
        copy.wait()


def pack_body(wq, wk, wv, wo, first, parts, sems):
    fetch([(w.at[0], parts.at[n]) for n, w in enumerate((wq, wk, wv, wo))], sems)
    whole = jnp.concatenate([parts[n] for n in range(4)], axis=1)
    for n in range(16):
        first[n] = whole


def many_body(wq, wk, wv, wo, bias, many, third, wide, parts, sems):
    pairs = [(w.at[1:3], parts.at[n]) for n, w in enumerate((wq, wk, wv, wo))]
    fetch(pairs, sems)
    third[...] = jnp.concatenate([parts[n, 1] for n in range(4)], axis=1)
    whole = jnp.concatenate([parts[n, 0] for n in range(4)], axis=1)
    for n in range(16):
        many[n] = whole
    wide[...] = jnp.zeros((8, 256), F32)
    for n in range(2 * LAYERS):
        for lag_row in range(WIN_ROWS):
            at = lag_row * GRID_W
            wide[n : n + 1, at : at + WIN_COLS] = bias[n // 2, n % 2, lag_row : lag_row + 1, :]


def line_body(p0, p1, p2, p3, many):
    for k, part in enumerate((p0, p1, p2, p3)):
        at = behind("x", k)
        for n in range(4):
            many[n, at] = part[...]


def table_body(wide, before, own, after, table):
    own_docs = own[128:144, 0:128].astype(F32)[0:1]
    query_docs = jnp.broadcast_to(own_docs, (128, 128)).T
    key_docs = jnp.concatenate(
        [before[128:144, 0:128].astype(F32)[0:1], own_docs, after[128:144, 0:128].astype(F32)[0:1]], axis=1
    )
    same = jnp.concatenate([query_docs] * 3, axis=1) == key_docs
    r = lax.broadcasted_iota(jnp.int32, (128, 384), 0)
    m = lax.broadcasted_iota(jnp.int32, (128, 384), 1)
    lag = (m >> 5) - (r >> 5)
    off = (m & 31) - (r & 31) + WIN_COLS // 2
    allowed = same & (lag >= 0) & (lag < WIN_ROWS) & (off >= 0) & (off < WIN_COLS)
    for n in range(2 * LAYERS):
        line = jnp.broadcast_to(wide[n : n + 1, :], (GRID_W, 256))
        line = pltpu.roll(line, 256 - WIN_COLS // 2, 1, stride=1, stride_axis=0)
        line = jnp.concatenate([line, jnp.zeros((GRID_W, 128), F32)], axis=1)
        block = jnp.concatenate(
            [line] + [pltpu.roll(line, 32 * q, 1) for q in range(1, 4)], axis=0
        )
        table[n] = jnp.where(allowed, block, -1e30)


def normed_heads(raw):
    values = raw.astype(BF16).astype(F32)
    squares = values * values
    low = lax.broadcasted_iota(jnp.int32, values.shape, 1) < HEAD_DIM
    first = jnp.sum(jnp.where(low, squares, 0.0), axis=1, keepdims=True)
    second = jnp.sum(jnp.where(low, 0.0, squares), axis=1, keepdims=True)
    scale = jnp.where(
        low,
        lax.rsqrt(first * (1.0 / HEAD_DIM) + EPS),
        lax.rsqrt(second * (1.0 / HEAD_DIM) + EPS),
    )
    return (values * scale).astype(BF16)


def finish_heads(acc, q, kv):
    q[...] = normed_heads(acc[:, 0:128])
    kv[:, 0:128] = normed_heads(acc[:, 128:256])
    kv[:, 128:256] = acc[:, 256:384].astype(BF16)


def heads_first_body(own, partner, gain, docs, weights, q, kv):
    c = lax.axis_index("c")
    total = jnp.zeros((128, 128), F32)
    for k in range(4):
        for part in (own, partner):
            values = part[k].astype(F32)
            total = total + values * values
    scale = lax.rsqrt(jnp.sum(total, axis=1, keepdims=True) * (1.0 / 1024) + EPS)
    acc = jnp.zeros((128, 384), F32)
    for k in range(4):
        for part, core in ((own, c), (partner, 1 - c)):
            block = behind("y", k) * 2 + core
            gains = gain[0:1, pl.ds(pl.multiple_of(block * 128, 128), 128)]
            normed = (part[k].astype(F32) * scale * gains).astype(BF16)
            rows = weights[pl.ds(pl.multiple_of(block * 128, 128), 128), 0:384]
            acc = acc + jnp.dot(normed, rows, preferred_element_type=F32)
    finish_heads(acc, q, kv.at[0:128])
    line = (docs[...] + 1).astype(F32).astype(BF16)
    kv[128:144, :] = jnp.broadcast_to(jnp.concatenate([line, line], axis=1), (16, 256))


def heads_pieces_body(x0, x1, x2, x3, gain, weights, q, kv, *, layer):
    pieces = [x[...].astype(F32) for x in (x0, x1, x2, x3)]
    total = sum(p * p for p in pieces)
    scale = lax.rsqrt(jnp.sum(total, axis=1, keepdims=True) * (1.0 / 1024) + EPS)
    acc = jnp.zeros((128, 384), F32)
    for k in range(4):
        block = behind("y", k)
        at = pl.ds(pl.multiple_of(block * 256, 256), 256)
        normed = (pieces[k] * scale * gain[layer : layer + 1, at]).astype(BF16)
        rows = weights[at, 0:384]
        acc = acc + jnp.dot(normed, rows, preferred_element_type=F32)
    finish_heads(acc, q, kv)


def attend(q, keys_values, table):
    queries = q[...]
    low = lax.broadcasted_iota(jnp.int32, (128, 128), 1) < HEAD_DIM
    results = []
    for h in range(2):
        mine = jnp.where(low if h == 0 else ~low, queries, jnp.zeros_like(queries))
        weights, total = [], 0.0
        for b, (keys, _) in enumerate(keys_values):
            scores = lax.dot_general(mine, keys, NT, preferred_element_type=F32)
            scores = scores * HEAD_DIM**-0.5 + table[h, :, b * 128 : (b + 1) * 128]
            grown = jnp.exp(scores)
            weights.append(grown)
            total = total + jnp.sum(grown, axis=1, keepdims=True)
        share = 1.0 / total
        out = 0.0
        for grown, (_, values) in zip(weights, keys_values):
            probs = (grown * share).astype(BF16)
            out = out + jnp.dot(probs, values, preferred_element_type=F32)
        results.append(out)
    return jnp.where(low, results[0], results[1]).astype(BF16)


def attend_scatter_body(q, before, own, after, table, weights, kept, s1, s2, s3, *, layer):
    parts = [(p[0:128, 0:128], p[0:128, 128:256]) for p in (before, own, after)]
    attended = attend(q, parts, table.at[2 * layer : 2 * layer + 2])
    for k, into in enumerate((kept, s1, s2, s3)):
        rows = weights[pl.ds(pl.multiple_of(ahead("y", k) * 256, 256), 256), 384:512]
        share = lax.dot_general(attended, rows, NT, preferred_element_type=F32)
        into[...] = share.astype(into.dtype)


def sum_body(kept, r1, r2, r3, out):
    out[...] = kept[...] + r1[...].astype(F32) + r2[...].astype(F32) + r3[...].astype(F32)


def pair_sum_body(mine, theirs, out):
    out[...] = (mine[...] + theirs[...]).astype(BF16)


def split_body(kept, r1, r2, r3, mine, theirs):
    c = lax.axis_index("c")
    for into, core in ((mine, c), (theirs, 1 - c)):
        at = pl.ds(pl.multiple_of(core * 128, 128), 128)
        into[...] = (
            kept[:, at] + r1[:, at].astype(F32) + r2[:, at].astype(F32) + r3[:, at].astype(F32)
        )


def scattered(body, *args):
    outs = [shaped(128, 256, dtype=F32)] + [shaped(128, 256)] * 3
    kept, s1, s2, s3 = call(body, outs, *args)
    r1 = lax.ppermute(s1, "y", turn(1))
    r3 = lax.ppermute(s3, "y", turn(3))
    r2 = lax.ppermute(s2, "y", turn(2))
    return kept, r1, r2, r3


def local(tokens, norm_gain, w_query, w_key, w_value, w_out, offset_bias, documents):
    hbm = pl.BlockSpec(memory_space=pltpu.HBM)
    held = [
        pltpu.with_memory_space_constraint(a, pltpu.HBM)
        for a in (w_query, w_key, w_value, jnp.swapaxes(w_out, 1, 2))
    ]
    first = call(
        pack_body, shaped(16, 64, 512), *held, in_specs=[hbm] * 4,
        scratch=[pltpu.VMEM((4, 64, 128), BF16), pltpu.SemaphoreType.DMA((4,))],
    )
    weights = gather_rows(first, SP)
    tokens_y = spread(tokens, "y")
    near_y = jnp.stack(in_order(tokens, tokens_y))
    many1, third, wide = call(
        many_body, [shaped(16, 64, 512), shaped(64, 512), shaped(8, 256, dtype=F32)],
        *held, offset_bias, in_specs=[hbm] * 4 + [pl.BlockSpec()],
        scratch=[pltpu.VMEM((4, 2, 64, 128), BF16), pltpu.SemaphoreType.DMA((4,))],
    )
    third_x = in_order(third, spread(third, "x"))
    near_partner = swap(after_this(near_y, many1))

    q, kv = call(
        heads_first_body, [shaped(128, 128), shaped(144, 256)],
        near_y, near_partner, norm_gain, documents.reshape(1, 128), weights,
    )
    many2 = call(line_body, shaped(4, 4, 64, 512), *third_x)
    for layer in range(LAYERS):
        after = from_after(kv)
        before = from_before(kv)
        if layer < 2:
            many, axes = ((many1, SP), (many2, "z"))[layer]
            next_weights = gather_rows(after_this(many, kv), axes)
        if layer == 0:
            table = call(table_body, shaped(6, 128, 384, dtype=F32), wide, before, kv, after)
        kept, r1, r2, r3 = scattered(
            functools.partial(attend_scatter_body, layer=layer),
            q, before, kv, after, table, weights,
        )
        if layer == 2:
            break
        half = call(sum_body, shaped(128, 256, dtype=F32), kept, r1, r2, r3)
        stream = call(pair_sum_body, shaped(128, 256), half, swap(half))
        weights = next_weights
        pieces = in_order(stream, spread(stream, "y"))
        if layer == 0:
            pieces = after_this(pieces, many2)
        q, kv = call(
            functools.partial(heads_pieces_body, layer=layer + 1),
            [shaped(128, 128), shaped(128, 256)],
            *pieces, norm_gain, weights,
        )
    mine, theirs = call(split_body, [shaped(128, 128, dtype=F32)] * 2, kept, r1, r2, r3)
    return call(pair_sum_body, shaped(128, 128), mine, swap(theirs))


def solution(mesh):
    torus = Mesh(mesh.devices.reshape(4, 4, 4, 2), ("z", "x", "y", "c"))
    return jax.shard_map(
        local,
        mesh=torus,
        in_specs=(
            P(SP, TP),
            P(),
            P(None, SP, TP),
            P(None, SP, TP),
            P(None, SP, TP),
            P(None, TP, SP),
            P(None, TP, None, None),
            P(SP),
        ),
        out_specs=P(SP, TP),
        check_vma=False,
    )
```

```python
import functools

import jax
import jax.numpy as jnp
from jax import lax
from jax.experimental import pallas as pl
from jax.experimental.pallas import tpu as pltpu
from jax.sharding import Mesh
from jax.sharding import PartitionSpec as P


HEAD_DIM = 64
WIN_ROWS = 8
WIN_COLS = 16
LAYERS = 3
GRID_W = 32
SP = ("z", "x")
TP = ("y", "c")
EPS = 1e-06
F32 = jnp.float32
BF16 = jnp.bfloat16
NT = (((1,), (1,)), ((), ()))


def turn(k):
    return [(i, (i + k) % 4) for i in range(4)]


def spread(a, axis):
    return [lax.ppermute(a, axis, turn(k)) for k in (1, 3, 2)]


def in_order(a, three):
    return [a, three[0], three[2], three[1]]


def gather_rows(a, axes):
    return lax.all_to_all(a, axes, 0, 0, tiled=True).reshape(1024, 512)


def after_this(a, done):
    return lax.optimization_barrier((a, done))[0]


def swap(a):
    return lax.ppermute(a, "c", [(0, 1), (1, 0)])


def from_before(a):
    return lax.ppermute(a, SP, [(i, i + 1) for i in range(15)])


def from_after(a):
    return lax.ppermute(a, SP, [(i + 1, i) for i in range(15)])


def behind(axis, k):
    return (lax.axis_index(axis) + (4 - k)) & 3


def ahead(axis, k):
    return (lax.axis_index(axis) + k) & 3


def call(body, outs, *args, scratch=(), **specs):
    return pl.pallas_call(
        body,
        out_shape=outs,
        **specs,
        scratch_shapes=list(scratch),
        compiler_params=pltpu.CompilerParams(vmem_limit_bytes=24 * 1024 * 1024),
    )(*args)


def shaped(*shape, dtype=BF16):
    return jax.ShapeDtypeStruct(shape, dtype)


def fetch(pairs, sems):
    copies = [pltpu.make_async_copy(a, b, sems.at[n]) for n, (a, b) in enumerate(pairs)]
    for copy in copies:
        copy.start()
    for copy in copies:
        copy.wait()


def pack_body(wq, wk, wv, wo, first, parts, sems):
    fetch([(w.at[0], parts.at[n]) for n, w in enumerate((wq, wk, wv, wo))], sems)
    whole = jnp.concatenate([parts[n] for n in range(4)], axis=1)
    for n in range(16):
        first[n] = whole


def many_body(wq, wk, wv, wo, bias, many, third, wide, parts, sems):
    pairs = [(w.at[1:3], parts.at[n]) for n, w in enumerate((wq, wk, wv, wo))]
    fetch(pairs, sems)
    third[...] = jnp.concatenate([parts[n, 1] for n in range(4)], axis=1)
    whole = jnp.concatenate([parts[n, 0] for n in range(4)], axis=1)
    for n in range(16):
        many[n] = whole
    wide[...] = jnp.zeros((8, 256), F32)
    for n in range(2 * LAYERS):
        for lag_row in range(WIN_ROWS):
            at = lag_row * GRID_W
            wide[n : n + 1, at : at + WIN_COLS] = bias[n // 2, n % 2, lag_row : lag_row + 1, :]


def line_body(p0, p1, p2, p3, many):
    for k, part in enumerate((p0, p1, p2, p3)):
        at = behind("x", k)
        for n in range(4):
            many[n, at] = part[...]


def table_body(wide, before, own, after, table):
    own_docs = own[128:144, 0:128].astype(F32)[0:1]
    query_docs = jnp.broadcast_to(own_docs, (128, 128)).T
    key_docs = jnp.concatenate(
        [before[128:144, 0:128].astype(F32)[0:1], own_docs, after[128:144, 0:128].astype(F32)[0:1]], axis=1
    )
    same = jnp.concatenate([query_docs] * 3, axis=1) == key_docs
    r = lax.broadcasted_iota(jnp.int32, (128, 384), 0)
    m = lax.broadcasted_iota(jnp.int32, (128, 384), 1)
    lag = (m >> 5) - (r >> 5)
    off = (m & 31) - (r & 31) + WIN_COLS // 2
    allowed = same & (lag >= 0) & (lag < WIN_ROWS) & (off >= 0) & (off < WIN_COLS)
    for n in range(2 * LAYERS):
        line = jnp.broadcast_to(wide[n : n + 1, :], (GRID_W, 256))
        line = pltpu.roll(line, 256 - WIN_COLS // 2, 1, stride=1, stride_axis=0)
        line = jnp.concatenate([line, jnp.zeros((GRID_W, 128), F32)], axis=1)
        block = jnp.concatenate(
            [line] + [pltpu.roll(line, 32 * q, 1) for q in range(1, 4)], axis=0
        )
        table[n] = jnp.where(allowed, block, -1e30)


def normed_heads(raw):
    values = raw.astype(BF16).astype(F32)
    squares = values * values
    low = lax.broadcasted_iota(jnp.int32, values.shape, 1) < HEAD_DIM
    first = jnp.sum(jnp.where(low, squares, 0.0), axis=1, keepdims=True)
    second = jnp.sum(jnp.where(low, 0.0, squares), axis=1, keepdims=True)
    scale = jnp.where(
        low,
        lax.rsqrt(first * (1.0 / HEAD_DIM) + EPS),
        lax.rsqrt(second * (1.0 / HEAD_DIM) + EPS),
    )
    return (values * scale).astype(BF16)


def finish_heads(acc, q, kv):
    q[...] = normed_heads(acc[:, 0:128])
    kv[:, 0:128] = normed_heads(acc[:, 128:256])
    kv[:, 128:256] = acc[:, 256:384].astype(BF16)


def heads_of(own, partner, gain, weights, layer):
    c = lax.axis_index("c")
    total = jnp.zeros((128, 128), F32)
    for k in range(4):
        for part in (own, partner):
            values = part[k].astype(F32)
            total = total + values * values
    scale = lax.rsqrt(jnp.sum(total, axis=1, keepdims=True) * (1.0 / 1024) + EPS)
    acc = jnp.zeros((128, 384), F32)
    for k in range(4):
        for part, core in ((own, c), (partner, 1 - c)):
            block = behind("y", k) * 2 + core
            gains = gain[layer : layer + 1, pl.ds(pl.multiple_of(block * 128, 128), 128)]
            normed = (part[k].astype(F32) * scale * gains).astype(BF16)
            rows = weights[pl.ds(pl.multiple_of(block * 128, 128), 128), 0:384]
            acc = acc + jnp.dot(normed, rows, preferred_element_type=F32)
    return acc


def heads_next_body(own, partner, gain, weights, q, kv, *, layer):
    finish_heads(heads_of(own, partner, gain, weights, layer), q, kv)


def heads_first_body(own, partner, gain, docs, weights, q, kv):
    finish_heads(heads_of(own, partner, gain, weights, 0), q, kv.at[0:128])
    line = (docs[...] + 1).astype(F32).astype(BF16)
    kv[128:144, :] = jnp.broadcast_to(jnp.concatenate([line, line], axis=1), (16, 256))


def attend(q, keys_values, table):
    queries = q[...]
    low = lax.broadcasted_iota(jnp.int32, (128, 128), 1) < HEAD_DIM
    results = []
    for h in range(2):
        mine = jnp.where(low if h == 0 else ~low, queries, jnp.zeros_like(queries))
        weights, total = [], 0.0
        for b, (keys, _) in enumerate(keys_values):
            scores = lax.dot_general(mine, keys, NT, preferred_element_type=F32)
            scores = scores * HEAD_DIM**-0.5 + table[h, :, b * 128 : (b + 1) * 128]
            grown = jnp.exp(scores)
            weights.append(grown)
            total = total + jnp.sum(grown, axis=1, keepdims=True)
        share = 1.0 / total
        out = 0.0
        for grown, (_, values) in zip(weights, keys_values):
            probs = (grown * share).astype(BF16)
            out = out + jnp.dot(probs, values, preferred_element_type=F32)
        results.append(out)
    return jnp.where(low, results[0], results[1]).astype(BF16)


def attend_halves_body(q, before, own, after, table, weights, mine, theirs, *, layer):
    parts = [(p[0:128, 0:128], p[0:128, 128:256]) for p in (before, own, after)]
    attended = attend(q, parts, table.at[2 * layer : 2 * layer + 2])
    c = lax.axis_index("c")
    for k in range(4):
        for into, core in ((mine, c), (theirs, 1 - c)):
            at = ahead("y", k) * 256 + core * 128
            rows = weights[pl.ds(pl.multiple_of(at, 128), 128), 384:512]
            share = lax.dot_general(attended, rows, NT, preferred_element_type=F32)
            into[k] = share.astype(into.dtype)


def join_body(mine, theirs, kept, s1, s2, s3):
    for k, into in enumerate((kept, s1, s2, s3)):
        into[...] = (mine[k] + theirs[k].astype(F32)).astype(into.dtype)


def total_body(kept, r1, r2, r3, out):
    total = kept[...] + r1[...].astype(F32) + r2[...].astype(F32) + r3[...].astype(F32)
    out[...] = total.astype(BF16)


def turned(s1, s2, s3):
    r1 = lax.ppermute(s1, "y", turn(1))
    r3 = lax.ppermute(s3, "y", turn(3))
    r2 = lax.ppermute(s2, "y", turn(2))
    return r1, r2, r3


def scattered_halves(body, needed, *args):
    outs = [shaped(4, 128, 128, dtype=F32), shaped(4, 128, 128)]
    mine, theirs = call(body, outs, *args)
    if needed is not None:
        mine = after_this(mine, needed)
    outs = [shaped(128, 128, dtype=F32)] + [shaped(128, 128)] * 3
    kept, *sent = call(join_body, outs, mine, swap(theirs))
    return call(total_body, shaped(128, 128), kept, *turned(*sent))


def local(tokens, norm_gain, w_query, w_key, w_value, w_out, offset_bias, documents):
    hbm = pl.BlockSpec(memory_space=pltpu.HBM)
    held = [
        pltpu.with_memory_space_constraint(a, pltpu.HBM)
        for a in (w_query, w_key, w_value, jnp.swapaxes(w_out, 1, 2))
    ]
    first = call(
        pack_body, shaped(16, 64, 512), *held, in_specs=[hbm] * 4,
        scratch=[pltpu.VMEM((4, 64, 128), BF16), pltpu.SemaphoreType.DMA((4,))],
    )
    weights = gather_rows(first, SP)
    tokens_y = spread(tokens, "y")
    near_y = jnp.stack(in_order(tokens, tokens_y))
    many1, third, wide = call(
        many_body, [shaped(16, 64, 512), shaped(64, 512), shaped(8, 256, dtype=F32)],
        *held, offset_bias, in_specs=[hbm] * 4 + [pl.BlockSpec()],
        scratch=[pltpu.VMEM((4, 2, 64, 128), BF16), pltpu.SemaphoreType.DMA((4,))],
    )
    third_x = in_order(third, spread(third, "x"))
    near_partner = swap(after_this(near_y, many1))

    q, kv = call(
        heads_first_body, [shaped(128, 128), shaped(144, 256)],
        near_y, near_partner, norm_gain, documents.reshape(1, 128), weights,
    )
    many2 = call(line_body, shaped(4, 4, 64, 512), *third_x)
    for layer in range(LAYERS):
        after = from_after(kv)
        before = from_before(kv)
        if layer < 2:
            many, axes = ((many1, SP), (many2, "z"))[layer]
            next_weights = gather_rows(after_this(many, kv), axes)
        if layer == 0:
            table = call(
                table_body, shaped(6, 128, 384, dtype=F32), wide, before, kv, after,
            )
        stream = scattered_halves(
            functools.partial(attend_halves_body, layer=layer),
            many2 if layer == 0 else None,
            q, before, kv, after, table, weights,
        )
        if layer == 2:
            return stream
        weights = next_weights
        near_y = jnp.stack(in_order(stream, spread(stream, "y")))
        q, kv = call(
            functools.partial(heads_next_body, layer=layer + 1),
            [shaped(128, 128), shaped(128, 256)],
            near_y, swap(near_y), norm_gain, weights,
        )


def solution(mesh):
    torus = Mesh(mesh.devices.reshape(4, 4, 4, 2), ("z", "x", "y", "c"))
    return jax.shard_map(
        local,
        mesh=torus,
        in_specs=(
            P(SP, TP),
            P(),
            P(None, SP, TP),
            P(None, SP, TP),
            P(None, SP, TP),
            P(None, TP, SP),
            P(None, TP, None, None),
            P(SP),
        ),
        out_specs=P(SP, TP),
        check_vma=False,
    )
```

```python
import functools

import jax
import jax.numpy as jnp
from jax import lax
from jax.experimental import pallas as pl
from jax.experimental.pallas import tpu as pltpu
from jax.sharding import Mesh
from jax.sharding import PartitionSpec as P


HEAD_DIM = 64
WIN_ROWS = 8
WIN_COLS = 16
LAYERS = 3
GRID_W = 32
SP = ("z", "x")
TP = ("y", "c")
EPS = 1e-06
F32 = jnp.float32
BF16 = jnp.bfloat16
NT = (((1,), (1,)), ((), ()))


def turn(k):
    return [(i, (i + k) % 4) for i in range(4)]


def spread(a, axis):
    return [lax.ppermute(a, axis, turn(k)) for k in (1, 3, 2)]


def in_order(a, three):
    return [a, three[0], three[2], three[1]]


def gather_rows(a, axes):
    return lax.all_to_all(a, axes, 0, 0, tiled=True).reshape(1024, 512)


def after_this(a, done):
    return lax.optimization_barrier((a, done))[0]


def swap(a):
    return lax.ppermute(a, "c", [(0, 1), (1, 0)])


def from_before(a):
    return lax.ppermute(a, SP, [(i, i + 1) for i in range(15)])


def from_after(a):
    return lax.ppermute(a, SP, [(i + 1, i) for i in range(15)])


def behind(axis, k):
    return (lax.axis_index(axis) + (4 - k)) & 3


def ahead(axis, k):
    return (lax.axis_index(axis) + k) & 3


def call(body, outs, *args, scratch=(), **specs):
    return pl.pallas_call(
        body,
        out_shape=outs,
        **specs,
        scratch_shapes=list(scratch),
        compiler_params=pltpu.CompilerParams(vmem_limit_bytes=24 * 1024 * 1024),
    )(*args)


def shaped(*shape, dtype=BF16):
    return jax.ShapeDtypeStruct(shape, dtype)


def fetch(pairs, sems):
    copies = [pltpu.make_async_copy(a, b, sems.at[n]) for n, (a, b) in enumerate(pairs)]
    for copy in copies:
        copy.start()
    for copy in copies:
        copy.wait()


def pack_body(wq, wk, wv, wo, first, parts, sems):
    @pl.when(pl.program_id(0) == 0)
    def _():
        fetch([(w.at[0], parts.at[n]) for n, w in enumerate((wq, wk, wv, wo))], sems)

    whole = jnp.concatenate([parts[n] for n in range(4)], axis=1)
    for n in range(4):
        first[n] = whole


def many_body(wq, wk, wv, wo, bias, many, third, wide, parts, sems):
    pairs = [(w.at[1:3], parts.at[n]) for n, w in enumerate((wq, wk, wv, wo))]
    fetch(pairs, sems)
    third[...] = jnp.concatenate([parts[n, 1] for n in range(4)], axis=1)
    whole = jnp.concatenate([parts[n, 0] for n in range(4)], axis=1)
    for n in range(16):
        many[n] = whole
    wide[...] = jnp.zeros((8, 256), F32)
    for n in range(2 * LAYERS):
        for lag_row in range(WIN_ROWS):
            at = lag_row * GRID_W
            wide[n : n + 1, at : at + WIN_COLS] = bias[n // 2, n % 2, lag_row : lag_row + 1, :]


def line_body(p0, p1, p2, p3, many):
    for k, part in enumerate((p0, p1, p2, p3)):
        at = behind("x", k)
        for n in range(4):
            many[n, at] = part[...]


def table_body(wide, before, own, after, table):
    own_docs = own[128:144, 0:128].astype(F32)[0:1]
    query_docs = jnp.broadcast_to(own_docs, (128, 128)).T
    key_docs = jnp.concatenate(
        [before[128:144, 0:128].astype(F32)[0:1], own_docs, after[128:144, 0:128].astype(F32)[0:1]], axis=1
    )
    same = jnp.concatenate([query_docs] * 3, axis=1) == key_docs
    r = lax.broadcasted_iota(jnp.int32, (128, 384), 0)
    m = lax.broadcasted_iota(jnp.int32, (128, 384), 1)
    lag = (m >> 5) - (r >> 5)
    off = (m & 31) - (r & 31) + WIN_COLS // 2
    allowed = same & (lag >= 0) & (lag < WIN_ROWS) & (off >= 0) & (off < WIN_COLS)
    for n in range(2 * LAYERS):
        line = jnp.broadcast_to(wide[n : n + 1, :], (GRID_W, 256))
        line = pltpu.roll(line, 256 - WIN_COLS // 2, 1, stride=1, stride_axis=0)
        line = jnp.concatenate([line, jnp.zeros((GRID_W, 128), F32)], axis=1)
        block = jnp.concatenate(
            [line] + [pltpu.roll(line, 32 * q, 1) for q in range(1, 4)], axis=0
        )
        table[n] = jnp.where(allowed, block, -1e30)


def normed_heads(raw):
    values = raw.astype(BF16).astype(F32)
    squares = values * values
    low = lax.broadcasted_iota(jnp.int32, values.shape, 1) < HEAD_DIM
    first = jnp.sum(jnp.where(low, squares, 0.0), axis=1, keepdims=True)
    second = jnp.sum(jnp.where(low, 0.0, squares), axis=1, keepdims=True)
    scale = jnp.where(
        low,
        lax.rsqrt(first * (1.0 / HEAD_DIM) + EPS),
        lax.rsqrt(second * (1.0 / HEAD_DIM) + EPS),
    )
    return (values * scale).astype(BF16)


def finish_heads(acc, q, kv):
    q[...] = normed_heads(acc[:, 0:128])
    kv[:, 0:128] = normed_heads(acc[:, 128:256])
    kv[:, 128:256] = acc[:, 256:384].astype(BF16)


def heads_first_body(own, partner, gain, docs, weights, q, kv):
    c = lax.axis_index("c")
    total = jnp.zeros((128, 128), F32)
    for k in range(4):
        for part in (own, partner):
            values = part[k].astype(F32)
            total = total + values * values
    scale = lax.rsqrt(jnp.sum(total, axis=1, keepdims=True) * (1.0 / 1024) + EPS)
    acc = jnp.zeros((128, 384), F32)
    for k in range(4):
        for part, core in ((own, c), (partner, 1 - c)):
            block = behind("y", k) * 2 + core
            gains = gain[0:1, pl.ds(pl.multiple_of(block * 128, 128), 128)]
            normed = (part[k].astype(F32) * scale * gains).astype(BF16)
            rows = weights[pl.ds(pl.multiple_of(block * 128, 128), 128), 0:384]
            acc = acc + jnp.dot(normed, rows, preferred_element_type=F32)
    finish_heads(acc, q, kv.at[0:128])
    line = (docs[...] + 1).astype(F32).astype(BF16)
    kv[128:144, :] = jnp.broadcast_to(jnp.concatenate([line, line], axis=1), (16, 256))


def heads_pieces_body(x0, x1, x2, x3, gain, weights, q, kv, *, layer):
    pieces = [x[...].astype(F32) for x in (x0, x1, x2, x3)]
    total = sum(p * p for p in pieces)
    scale = lax.rsqrt(jnp.sum(total, axis=1, keepdims=True) * (1.0 / 1024) + EPS)
    acc = jnp.zeros((128, 384), F32)
    for k in range(4):
        block = behind("y", k)
        at = pl.ds(pl.multiple_of(block * 256, 256), 256)
        normed = (pieces[k] * scale * gain[layer : layer + 1, at]).astype(BF16)
        rows = weights[at, 0:384]
        acc = acc + jnp.dot(normed, rows, preferred_element_type=F32)
    finish_heads(acc, q, kv)


def attend(q, keys_values, table):
    queries = q[...]
    low = lax.broadcasted_iota(jnp.int32, (128, 128), 1) < HEAD_DIM
    results = []
    for h in range(2):
        mine = jnp.where(low if h == 0 else ~low, queries, jnp.zeros_like(queries))
        weights, total = [], 0.0
        for b, (keys, _) in enumerate(keys_values):
            scores = lax.dot_general(mine, keys, NT, preferred_element_type=F32)
            scores = scores * HEAD_DIM**-0.5 + table[h, :, b * 128 : (b + 1) * 128]
            grown = jnp.exp(scores)
            weights.append(grown)
            total = total + jnp.sum(grown, axis=1, keepdims=True)
        share = 1.0 / total
        out = 0.0
        for grown, (_, values) in zip(weights, keys_values):
            probs = (grown * share).astype(BF16)
            out = out + jnp.dot(probs, values, preferred_element_type=F32)
        results.append(out)
    return jnp.where(low, results[0], results[1]).astype(BF16)


def attend_scatter_body(q, before, own, after, table, weights, kept, s1, s2, s3, *, layer):
    parts = [(p[0:128, 0:128], p[0:128, 128:256]) for p in (before, own, after)]
    attended = attend(q, parts, table.at[2 * layer : 2 * layer + 2])
    for k, into in enumerate((kept, s1, s2, s3)):
        rows = weights[pl.ds(pl.multiple_of(ahead("y", k) * 256, 256), 256), 384:512]
        share = lax.dot_general(attended, rows, NT, preferred_element_type=F32)
        into[...] = share.astype(into.dtype)


def attend_halves_body(q, before, own, after, table, weights, mine, theirs, *, layer):
    parts = [(p[0:128, 0:128], p[0:128, 128:256]) for p in (before, own, after)]
    attended = attend(q, parts, table.at[2 * layer : 2 * layer + 2])
    c = lax.axis_index("c")
    for k in range(4):
        for into, core in ((mine, c), (theirs, 1 - c)):
            at = ahead("y", k) * 256 + core * 128
            rows = weights[pl.ds(pl.multiple_of(at, 128), 128), 384:512]
            share = lax.dot_general(attended, rows, NT, preferred_element_type=F32)
            into[k] = share.astype(into.dtype)


def join_body(mine, theirs, kept, s1, s2, s3):
    for k, into in enumerate((kept, s1, s2, s3)):
        into[...] = (mine[k] + theirs[k].astype(F32)).astype(into.dtype)


def total_body(kept, r1, r2, r3, out):
    total = kept[...] + r1[...].astype(F32) + r2[...].astype(F32) + r3[...].astype(F32)
    out[...] = total.astype(BF16)


def sum_body(kept, r1, r2, r3, out):
    out[...] = kept[...] + r1[...].astype(F32) + r2[...].astype(F32) + r3[...].astype(F32)


def pair_sum_body(mine, theirs, out):
    out[...] = (mine[...] + theirs[...]).astype(BF16)


def turned(s1, s2, s3):
    r1 = lax.ppermute(s1, "y", turn(1))
    r3 = lax.ppermute(s3, "y", turn(3))
    r2 = lax.ppermute(s2, "y", turn(2))
    return r1, r2, r3


def scattered(body, *args):
    outs = [shaped(128, 256, dtype=F32)] + [shaped(128, 256)] * 3
    kept, *sent = call(body, outs, *args)
    return kept, *turned(*sent)


def scattered_halves(body, *args):
    outs = [shaped(4, 128, 128, dtype=F32), shaped(4, 128, 128)]
    mine, theirs = call(body, outs, *args)
    outs = [shaped(128, 128, dtype=F32)] + [shaped(128, 128)] * 3
    kept, *sent = call(join_body, outs, mine, swap(theirs))
    return call(total_body, shaped(128, 128), kept, *turned(*sent))


def local(tokens, norm_gain, w_query, w_key, w_value, w_out, offset_bias, documents):
    hbm = pl.BlockSpec(memory_space=pltpu.HBM)
    held = [
        pltpu.with_memory_space_constraint(a, pltpu.HBM)
        for a in (w_query, w_key, w_value, jnp.swapaxes(w_out, 1, 2))
    ]
    first = call(
        pack_body, shaped(16, 64, 512), *held, in_specs=[hbm] * 4,
        grid=(4,), out_specs=pl.BlockSpec((4, 64, 512), lambda n: (n, 0, 0)),
        scratch=[pltpu.VMEM((4, 64, 128), BF16), pltpu.SemaphoreType.DMA((4,))],
    )
    weights = gather_rows(first, SP)
    tokens_y = spread(tokens, "y")
    near_y = jnp.stack(in_order(tokens, tokens_y))
    many1, third, wide = call(
        many_body, [shaped(16, 64, 512), shaped(64, 512), shaped(8, 256, dtype=F32)],
        *held, offset_bias, in_specs=[hbm] * 4 + [pl.BlockSpec()],
        scratch=[pltpu.VMEM((4, 2, 64, 128), BF16), pltpu.SemaphoreType.DMA((4,))],
    )
    third_x = in_order(third, spread(third, "x"))
    near_partner = swap(after_this(near_y, many1))

    q, kv = call(
        heads_first_body, [shaped(128, 128), shaped(144, 256)],
        near_y, near_partner, norm_gain, documents.reshape(1, 128), weights,
    )
    many2 = call(line_body, shaped(4, 4, 64, 512), *third_x)
    for layer in range(LAYERS):
        after = from_after(kv)
        before = from_before(kv)
        if layer < 2:
            many, axes = ((many1, SP), (many2, "z"))[layer]
            next_weights = gather_rows(after_this(many, kv), axes)
        if layer == 0:
            table = call(
                table_body, shaped(6, 128, 384, dtype=F32), wide, before, kv, after,
            )
        args = (q, before, kv, after, table, weights)
        if layer == 2:
            return scattered_halves(
                functools.partial(attend_halves_body, layer=layer), *args
            )
        kept, r1, r2, r3 = scattered(
            functools.partial(attend_scatter_body, layer=layer), *args
        )
        if layer == 0:
            kept = after_this(kept, many2)
        half = call(sum_body, shaped(128, 256, dtype=F32), kept, r1, r2, r3)
        stream = call(pair_sum_body, shaped(128, 256), half, swap(half))
        weights = next_weights
        q, kv = call(
            functools.partial(heads_pieces_body, layer=layer + 1),
            [shaped(128, 128), shaped(128, 256)],
            *in_order(stream, spread(stream, "y")), norm_gain, weights,
        )


def solution(mesh):
    torus = Mesh(mesh.devices.reshape(4, 4, 4, 2), ("z", "x", "y", "c"))
    return jax.shard_map(
        local,
        mesh=torus,
        in_specs=(
            P(SP, TP),
            P(),
            P(None, SP, TP),
            P(None, SP, TP),
            P(None, SP, TP),
            P(None, TP, SP),
            P(None, TP, None, None),
            P(SP),
        ),
        out_specs=P(SP, TP),
        check_vma=False,
    )
```

```python
import functools

import jax
import jax.numpy as jnp
from jax import lax
from jax.experimental import pallas as pl
from jax.experimental.pallas import tpu as pltpu
from jax.sharding import Mesh
from jax.sharding import PartitionSpec as P


HEAD_DIM = 64
WIN_ROWS = 8
WIN_COLS = 16
LAYERS = 3
GRID_W = 32
SP = ("z", "x")
TP = ("y", "c")
EPS = 1e-06
F32 = jnp.float32
BF16 = jnp.bfloat16
NT = (((1,), (1,)), ((), ()))


def turn(k):
    return [(i, (i + k) % 4) for i in range(4)]


def spread(a, axis):
    return [lax.ppermute(a, axis, turn(k)) for k in (1, 3, 2)]


def in_order(a, three):
    return [a, three[0], three[2], three[1]]


def gather_rows(a, axes):
    return lax.all_to_all(a, axes, 0, 0, tiled=True).reshape(1024, 512)


def after_this(a, done):
    return lax.optimization_barrier((a, done))[0]


def swap(a):
    return lax.ppermute(a, "c", [(0, 1), (1, 0)])


def from_before(a):
    return lax.ppermute(a, SP, [(i, i + 1) for i in range(15)])


def from_after(a):
    return lax.ppermute(a, SP, [(i + 1, i) for i in range(15)])


def behind(axis, k):
    return (lax.axis_index(axis) + (4 - k)) & 3


def ahead(axis, k):
    return (lax.axis_index(axis) + k) & 3


def call(body, outs, *args, scratch=(), **specs):
    return pl.pallas_call(
        body,
        out_shape=outs,
        **specs,
        scratch_shapes=list(scratch),
        compiler_params=pltpu.CompilerParams(vmem_limit_bytes=24 * 1024 * 1024),
    )(*args)


def shaped(*shape, dtype=BF16):
    return jax.ShapeDtypeStruct(shape, dtype)


def fetch(pairs, sems):
    copies = [pltpu.make_async_copy(a, b, sems.at[n]) for n, (a, b) in enumerate(pairs)]
    for copy in copies:
        copy.start()
    for copy in copies:
        copy.wait()


def pack_body(wq, wk, wv, wo, first, parts, sems):
    fetch([(w.at[0], parts.at[n]) for n, w in enumerate((wq, wk, wv, wo))], sems)
    whole = jnp.concatenate([parts[n] for n in range(4)], axis=1)
    for n in range(16):
        first[n] = whole


def many_body(wq, wk, wv, wo, bias, many, third, wide, parts, sems):
    pairs = [(w.at[1:3], parts.at[n]) for n, w in enumerate((wq, wk, wv, wo))]
    fetch(pairs, sems)
    third[...] = jnp.concatenate([parts[n, 1] for n in range(4)], axis=1)
    whole = jnp.concatenate([parts[n, 0] for n in range(4)], axis=1)
    for n in range(16):
        many[n] = whole
    wide[...] = jnp.zeros((8, 256), F32)
    for n in range(2 * LAYERS):
        for lag_row in range(WIN_ROWS):
            at = lag_row * GRID_W
            wide[n : n + 1, at : at + WIN_COLS] = bias[n // 2, n % 2, lag_row : lag_row + 1, :]


def line_body(p0, p1, p2, p3, many):
    for k, part in enumerate((p0, p1, p2, p3)):
        at = behind("x", k)
        for n in range(4):
            many[n, at] = part[...]


def table_body(wide, before, own, after, table):
    own_docs = own[128:144, 0:128].astype(F32)[0:1]
    query_docs = jnp.broadcast_to(own_docs, (128, 128)).T
    key_docs = jnp.concatenate(
        [before[128:144, 0:128].astype(F32)[0:1], own_docs, after[128:144, 0:128].astype(F32)[0:1]], axis=1
    )
    same = jnp.concatenate([query_docs] * 3, axis=1) == key_docs
    r = lax.broadcasted_iota(jnp.int32, (128, 384), 0)
    m = lax.broadcasted_iota(jnp.int32, (128, 384), 1)
    lag = (m >> 5) - (r >> 5)
    off = (m & 31) - (r & 31) + WIN_COLS // 2
    allowed = same & (lag >= 0) & (lag < WIN_ROWS) & (off >= 0) & (off < WIN_COLS)
    for n in range(2 * LAYERS):
        line = jnp.broadcast_to(wide[n : n + 1, :], (GRID_W, 256))
        line = pltpu.roll(line, 256 - WIN_COLS // 2, 1, stride=1, stride_axis=0)
        line = jnp.concatenate([line, jnp.zeros((GRID_W, 128), F32)], axis=1)
        block = jnp.concatenate(
            [line] + [pltpu.roll(line, 32 * q, 1) for q in range(1, 4)], axis=0
        )
        table[n] = jnp.where(allowed, block, -1e30)


def normed_heads(raw):
    values = raw.astype(BF16).astype(F32)
    squares = values * values
    low = lax.broadcasted_iota(jnp.int32, values.shape, 1) < HEAD_DIM
    first = jnp.sum(jnp.where(low, squares, 0.0), axis=1, keepdims=True)
    second = jnp.sum(jnp.where(low, 0.0, squares), axis=1, keepdims=True)
    scale = jnp.where(
        low,
        lax.rsqrt(first * (1.0 / HEAD_DIM) + EPS),
        lax.rsqrt(second * (1.0 / HEAD_DIM) + EPS),
    )
    return (values * scale).astype(BF16)


def finish_heads(acc, q, kv):
    q[...] = normed_heads(acc[:, 0:128])
    kv[:, 0:128] = normed_heads(acc[:, 128:256])
    kv[:, 128:256] = acc[:, 256:384].astype(BF16)


def heads_first_body(own, partner, gain, docs, weights, q, kv):
    c = lax.axis_index("c")
    total = jnp.zeros((128, 128), F32)
    for k in range(4):
        for part in (own, partner):
            values = part[k].astype(F32)
            total = total + values * values
    scale = lax.rsqrt(jnp.sum(total, axis=1, keepdims=True) * (1.0 / 1024) + EPS)
    acc = jnp.zeros((128, 384), F32)
    for k in range(4):
        for part, core in ((own, c), (partner, 1 - c)):
            block = behind("y", k) * 2 + core
            gains = gain[0:1, pl.ds(pl.multiple_of(block * 128, 128), 128)]
            normed = (part[k].astype(F32) * scale * gains).astype(BF16)
            rows = weights[pl.ds(pl.multiple_of(block * 128, 128), 128), 0:384]
            acc = acc + jnp.dot(normed, rows, preferred_element_type=F32)
    finish_heads(acc, q, kv.at[0:128])
    line = (docs[...] + 1).astype(F32).astype(BF16)
    kv[128:144, :] = jnp.broadcast_to(jnp.concatenate([line, line], axis=1), (16, 256))


def heads_pieces_body(x0, x1, x2, x3, gain, weights, q, kv, *, layer):
    pieces = [x[...].astype(F32) for x in (x0, x1, x2, x3)]
    total = sum(p * p for p in pieces)
    scale = lax.rsqrt(jnp.sum(total, axis=1, keepdims=True) * (1.0 / 1024) + EPS)
    acc = jnp.zeros((128, 384), F32)
    for k in range(4):
        block = behind("y", k)
        at = pl.ds(pl.multiple_of(block * 256, 256), 256)
        normed = (pieces[k] * scale * gain[layer : layer + 1, at]).astype(BF16)
        rows = weights[at, 0:384]
        acc = acc + jnp.dot(normed, rows, preferred_element_type=F32)
    finish_heads(acc, q, kv)


def attend(q, keys_values, table):
    queries = q[...]
    low = lax.broadcasted_iota(jnp.int32, (128, 128), 1) < HEAD_DIM
    results = []
    for h in range(2):
        mine = jnp.where(low if h == 0 else ~low, queries, jnp.zeros_like(queries))
        weights, total = [], 0.0
        for b, (keys, _) in enumerate(keys_values):
            scores = lax.dot_general(mine, keys, NT, preferred_element_type=F32)
            scores = scores * HEAD_DIM**-0.5 + table[h, :, b * 128 : (b + 1) * 128]
            grown = jnp.exp(scores)
            weights.append(grown)
            total = total + jnp.sum(grown, axis=1, keepdims=True)
        share = 1.0 / total
        out = 0.0
        for grown, (_, values) in zip(weights, keys_values):
            probs = (grown * share).astype(BF16)
            out = out + jnp.dot(probs, values, preferred_element_type=F32)
        results.append(out)
    return jnp.where(low, results[0], results[1]).astype(BF16)


def attend_scatter_body(q, before, own, after, table, weights, kept, s1, s2, s3, *, layer):
    parts = [(p[0:128, 0:128], p[0:128, 128:256]) for p in (before, own, after)]
    attended = attend(q, parts, table.at[2 * layer : 2 * layer + 2])
    for k, into in enumerate((kept, s1, s2, s3)):
        rows = weights[pl.ds(pl.multiple_of(ahead("y", k) * 256, 256), 256), 384:512]
        share = lax.dot_general(attended, rows, NT, preferred_element_type=F32)
        into[...] = share.astype(into.dtype)


def attend_halves_body(q, before, own, after, table, weights, mine, theirs, *, layer):
    parts = [(p[0:128, 0:128], p[0:128, 128:256]) for p in (before, own, after)]
    attended = attend(q, parts, table.at[2 * layer : 2 * layer + 2])
    c = lax.axis_index("c")
    for k in range(4):
        for into, core in ((mine, c), (theirs, 1 - c)):
            at = ahead("y", k) * 256 + core * 128
            rows = weights[pl.ds(pl.multiple_of(at, 128), 128), 384:512]
            share = lax.dot_general(attended, rows, NT, preferred_element_type=F32)
            into[k] = share.astype(into.dtype)


def join_body(mine, theirs, kept, s1, s2, s3):
    for k, into in enumerate((kept, s1, s2, s3)):
        into[...] = (mine[k] + theirs[k].astype(F32)).astype(into.dtype)


def total_body(kept, r1, r2, r3, out):
    total = kept[...] + r1[...].astype(F32) + r2[...].astype(F32) + r3[...].astype(F32)
    out[...] = total.astype(BF16)


def sum_body(kept, r1, r2, r3, out):
    out[...] = kept[...] + r1[...].astype(F32) + r2[...].astype(F32) + r3[...].astype(F32)


def pair_sum_body(mine, theirs, out):
    out[...] = (mine[...] + theirs[...]).astype(BF16)


def turned(s1, s2, s3):
    r1 = lax.ppermute(s1, "y", turn(1))
    r3 = lax.ppermute(s3, "y", turn(3))
    r2 = lax.ppermute(s2, "y", turn(2))
    return r1, r2, r3


def scattered(body, *args):
    outs = [shaped(128, 256, dtype=F32)] + [shaped(128, 256)] * 3
    kept, *sent = call(body, outs, *args)
    return kept, *turned(*sent)


def scattered_halves(body, *args):
    outs = [shaped(4, 128, 128, dtype=F32), shaped(4, 128, 128)]
    mine, theirs = call(body, outs, *args)
    outs = [shaped(128, 128, dtype=F32)] + [shaped(128, 128)] * 3
    kept, *sent = call(join_body, outs, mine, swap(theirs))
    return call(total_body, shaped(128, 128), kept, *turned(*sent))


def local(tokens, norm_gain, w_query, w_key, w_value, w_out, offset_bias, documents):
    hbm = pl.BlockSpec(memory_space=pltpu.HBM)
    held = [
        pltpu.with_memory_space_constraint(a, pltpu.HBM)
        for a in (w_query, w_key, w_value, jnp.swapaxes(w_out, 1, 2))
    ]
    first = call(
        pack_body, shaped(16, 64, 512), *held, in_specs=[hbm] * 4,
        scratch=[pltpu.VMEM((4, 64, 128), BF16), pltpu.SemaphoreType.DMA((4,))],
    )
    weights = gather_rows(first, SP)
    tokens_y = spread(tokens, "y")
    near_y = jnp.stack(in_order(tokens, tokens_y))
    many1, third, wide = call(
        many_body, [shaped(16, 64, 512), shaped(64, 512), shaped(8, 256, dtype=F32)],
        *held, offset_bias, in_specs=[hbm] * 4 + [pl.BlockSpec()],
        scratch=[pltpu.VMEM((4, 2, 64, 128), BF16), pltpu.SemaphoreType.DMA((4,))],
    )
    third_x = in_order(third, spread(third, "x"))
    near_partner = swap(after_this(near_y, many1))

    q, kv = call(
        heads_first_body, [shaped(128, 128), shaped(144, 256)],
        near_y, near_partner, norm_gain, documents.reshape(1, 128), weights,
    )
    many2 = call(line_body, shaped(4, 4, 64, 512), *third_x)
    for layer in range(LAYERS):
        after = from_after(kv)
        before = from_before(kv)
        if layer < 2:
            many, axes = ((many1, SP), (many2, "z"))[layer]
            next_weights = gather_rows(after_this(many, kv), axes)
        if layer == 0:
            table = call(
                table_body, shaped(6, 128, 384, dtype=F32), wide, before, kv, after,
            )
        args = (q, before, kv, after, table, weights)
        if layer == 2:
            return scattered_halves(
                functools.partial(attend_halves_body, layer=layer), *args
            )
        kept, r1, r2, r3 = scattered(
            functools.partial(attend_scatter_body, layer=layer), *args
        )
        if layer == 0:
            kept = after_this(kept, many2)
        half = call(sum_body, shaped(128, 256, dtype=F32), kept, r1, r2, r3)
        stream = call(pair_sum_body, shaped(128, 256), half, swap(half))
        weights = next_weights
        q, kv = call(
            functools.partial(heads_pieces_body, layer=layer + 1),
            [shaped(128, 128), shaped(128, 256)],
            *in_order(stream, spread(stream, "y")), norm_gain, weights,
        )


def solution(mesh):
    torus = Mesh(mesh.devices.reshape(4, 4, 4, 2), ("z", "x", "y", "c"))
    return jax.shard_map(
        local,
        mesh=torus,
        in_specs=(
            P(SP, TP),
            P(),
            P(None, SP, TP),
            P(None, SP, TP),
            P(None, SP, TP),
            P(None, TP, SP),
            P(None, TP, None, None),
            P(SP),
        ),
        out_specs=P(SP, TP),
        check_vma=False,
    )
```
